128 devices in a mesh: sp: 16 (over z, x), dp: 8 (over y, core).
Axes of the slice: x: 4, y: 4, z: 4, core: 2. Of those that a mesh axis runs over, the one named last changes fastest.
Arguments:
- residual_in: bfloat16 [8, 2048, 2048], P('dp', 'sp'), may hold values from -6 to 6
- query_proj: bfloat16 [8, 2048, 2048], P('dp', 'sp'), may hold values from -8 to 8
- key_proj: bfloat16 [8, 2048, 512], P('dp', 'sp'), may hold values from -8 to 8
- value_proj: bfloat16 [8, 2048, 512], P('dp', 'sp'), may hold values from -6 to 6
- query_gain: float32 [128], replicated, may hold values from 0.1 to 7
- key_gain: float32 [128], replicated, may hold values from 0.1 to 7
- out_weight: bfloat16 [2048, 2048], replicated, may hold values from -0.125 to 0.125
- post_gain: float32 [2048], replicated, may hold values from 0.1 to 1.9
- pre_gain: float32 [2048], replicated, may hold values from 0.1 to 1.9
- route_ids: int32 [8, 2048, 2], P('dp', 'sp'), may hold values from 0 to 127, as said below
- group_weight: float32 [8, 2048], P('dp', 'sp'), may hold values from 0.25 to 1
- first_share: float32 [8, 2048], P('dp', 'sp'), may hold values from 0.5 to 1
- gate_weight: bfloat16 [128, 2048, 512], P(('sp', 'dp')), may hold values from -0.125 to 0.125
- up_weight: bfloat16 [128, 2048, 512], P(('sp', 'dp')), may hold values from -0.125 to 0.125
- down_weight: bfloat16 [128, 512, 2048], P(('sp', 'dp')), may hold values from -0.25 to 0.25
Outputs:
- layer_out: bfloat16 [8, 2048, 2048], P('dp', 'sp')
The draws below stay inside these ranges and needn't reach their ends.
Inputs may be any that keep to these rules, and one draw needn't show every extreme that they name: `route_ids`: each token names two different experts of one group of 32 consecutive experts. Among the 128 tokens of one device each group is chosen by exactly 32 tokens, no expert is named by more than 4 of them, and in every draw one expert of each group is named by exactly 4 tokens of every device.
All inputs are finite; a program needn't handle non-finite values.
Results may differ from the reference program's by a relative error of at most 0.009.
The reference program's roundings to bfloat16 on the way count: a program that leaves them out, or rounds other values in their place, can miss the bound.
Values may be sent and summed in bfloat16 or wider, within the bound.
A program may use at most 128 MiB of HBM per device.

```python
import jax
import jax.numpy as jnp
from jax import lax

D = 2048
HEADS = 16
KV_HEADS = 4
HEAD_DIM = 128
FF = 512
GROUPS = 4
GRID_W = 64
TOK_DEV = 128
SEQS = 8
SEQ = 2048
EXPERTS = 128
CAP = 4
N_SP = 16
N_DP = 8


def draw_query_proj(key, part):
    own = jax.random.fold_in(key, 11)
    base = jax.random.truncated_normal(own, -6.0, 6.0, (SEQS, SEQ, HEADS * HEAD_DIM), jnp.float32)
    return base.astype(jnp.bfloat16)


def draw_key_proj(key, part):
    own = jax.random.fold_in(key, 12)
    base = jax.random.truncated_normal(own, -6.0, 6.0, (SEQS, SEQ, KV_HEADS * HEAD_DIM), jnp.float32)
    return base.astype(jnp.bfloat16)


def gain_table(own):
    return 1.0 + 0.18 * jax.random.truncated_normal(own, -5.0, 5.0, (HEAD_DIM,), jnp.float32)


def draw_query_gain(key, part):
    return gain_table(jax.random.fold_in(key, 21))


def draw_key_gain(key, part):
    return gain_table(jax.random.fold_in(key, 22))


def draw_route_ids(key, part):
    per_group = TOK_DEV // GROUPS
    group_width = EXPERTS // GROUPS
    middle = CAP // 2
    hot = jax.random.randint(jax.random.fold_in(key, 31), (GROUPS,), 0, group_width)
    block_count = SEQS * (SEQ // TOK_DEV)

    def one_block(block_key):
        key_tok, key_rest = jax.random.split(block_key)
        order = jax.random.permutation(key_tok, TOK_DEV)
        firsts = []
        seconds = []
        for group_id in range(GROUPS):
            group_key = jax.random.fold_in(key_rest, group_id)
            key_perm, key_shift, key_swap = jax.random.split(group_key, 3)
            shuffled = jax.random.permutation(key_perm, group_width).astype(jnp.int32)
            shifts = jax.random.randint(key_shift, (group_width // 2,), -middle, middle + 1)
            hot_place = jnp.sum(jnp.where(shuffled == hot[group_id], jnp.arange(group_width, dtype=jnp.int32), 0))
            sign_value = 1 - 2 * (hot_place % 2)
            shifts = shifts.at[hot_place // 2].set(middle * sign_value)
            counts = jnp.zeros((group_width,), jnp.int32).at[shuffled[0::2]].set(middle + shifts).at[shuffled[1::2]].set(middle - shifts)
            listed = jnp.repeat(jnp.arange(group_width, dtype=jnp.int32), counts, total_repeat_length=2 * per_group)
            first_pick = listed[:per_group]
            second_pick = listed[per_group:]
            swap_bits = jax.random.randint(key_swap, (per_group,), 0, 2)
            leading = jnp.where(swap_bits == 1, second_pick, first_pick)
            trailing = jnp.where(swap_bits == 1, first_pick, second_pick)
            firsts.append(leading + group_id * group_width)
            seconds.append(trailing + group_id * group_width)
        pairs = jnp.stack([jnp.concatenate(firsts), jnp.concatenate(seconds)], axis=1).astype(jnp.int32)
        return jnp.zeros((TOK_DEV, 2), jnp.int32).at[order].set(pairs)
    blocks_all = jax.vmap(one_block)(jax.random.split(jax.random.fold_in(key, 32), block_count))
    return blocks_all.reshape(SEQS, SEQ, 2)


def level_of(rng, shape, cuts, least, top_value):
    level, own = 1.0, jax.random.fold_in(rng, 6)
    for axis_at, shards_of in cuts:
        steps = jnp.exp(jax.random.uniform(jax.random.fold_in(own, axis_at), (shards_of,), jnp.float32, least / len(cuts), top_value / len(cuts)))
        level = level * jnp.repeat(steps, shape[axis_at] // shards_of).reshape([-1 if axis == axis_at else 1 for axis in range(len(shape))])
    return level


def bell_draw(key, shape, deviation, bound, cuts=(), kind=jnp.bfloat16):
    entries = jax.random.normal(key, shape, jnp.float32) * deviation
    if len(cuts) > 0:
        entries = level_of(key, shape, cuts, -0.22, 0.18) * entries
    return jnp.clip(entries, min=-bound, max=bound).astype(kind)


def setup_inputs(seed: int = 0) -> dict:
    keys = jax.random.split(jax.random.key(seed), 16)
    residual_in = bell_draw(keys[0], (SEQS, SEQ, D), 1.0, 6.0, ((0, 8), (1, 16)))
    query_proj = draw_query_proj(jax.random.fold_in(keys[15], 71), 0)
    key_proj = draw_key_proj(jax.random.fold_in(keys[15], 71), 0)
    value_proj = bell_draw(keys[3], (SEQS, SEQ, KV_HEADS * HEAD_DIM), 1.0, 6.0, ((0, 8), (1, 16)))
    query_gain = draw_query_gain(jax.random.fold_in(keys[15], 71), 0)
    key_gain = draw_key_gain(jax.random.fold_in(keys[15], 71), 0)
    out_weight = bell_draw(keys[6], (D, D), D ** -0.5, 0.125)
    post_gain = jnp.clip(1.0 + 0.18 * jax.random.normal(keys[7], (D,), jnp.float32), 0.1, 1.9)
    pre_gain = jnp.clip(1.0 + 0.18 * jax.random.normal(keys[8], (D,), jnp.float32), 0.1, 1.9)
    route_ids = draw_route_ids(jax.random.fold_in(keys[15], 71), 0)
    group_weight = jnp.clip(0.25 + 0.75 * jax.random.uniform(keys[10], (SEQS, SEQ), jnp.float32) ** level_of(keys[10], (SEQS, SEQ), ((0, 8), (1, 16)), -0.2, 0.2), 0.25, 1.0)
    first_share = jnp.clip(0.5 + 0.5 * jax.random.uniform(keys[11], (SEQS, SEQ), jnp.float32) ** level_of(keys[11], (SEQS, SEQ), ((0, 8), (1, 16)), -0.2, 0.2), 0.5, 1.0)
    gate_weight = bell_draw(keys[12], (EXPERTS, D, FF), D ** -0.5, 0.125, ((0, 128),))
    up_weight = bell_draw(keys[13], (EXPERTS, D, FF), D ** -0.5, 0.125, ((0, 128),))
    down_weight = bell_draw(keys[14], (EXPERTS, FF, D), FF ** -0.5, 0.25, ((0, 128),))
    return {"residual_in": residual_in, "query_proj": query_proj, "key_proj": key_proj, "value_proj": value_proj, "query_gain": query_gain, "key_gain": key_gain, "out_weight": out_weight, "post_gain": post_gain, "pre_gain": pre_gain, "route_ids": route_ids, "group_weight": group_weight, "first_share": first_share, "gate_weight": gate_weight, "up_weight": up_weight, "down_weight": down_weight}


EPSILON = 1e-06

def rotate_heads(raw_heads, gain_vec, positions):
    floats = raw_heads.astype(jnp.float32)
    normed = floats * lax.rsqrt(lax.optimization_barrier(jnp.mean(floats * floats, axis=-1, keepdims=True)) + EPSILON) * gain_vec
    quarter = raw_heads.shape[-1] // 4
    inverse = 10000.0 ** (-jnp.arange(quarter, dtype=jnp.float32) / quarter)
    grid_rows = (positions // GRID_W).astype(jnp.float32)[:, None] * inverse
    grid_cols = (positions % GRID_W).astype(jnp.float32)[:, None] * inverse
    angles = jnp.concatenate([grid_rows, grid_rows, grid_cols, grid_cols], axis=-1)[:, None, :]
    pieces = normed.reshape(normed.shape[:-1] + (2, 2, quarter))
    turned = jnp.stack([-pieces[..., 1, :], pieces[..., 0, :]], axis=-2).reshape(normed.shape)
    return (normed * jnp.cos(angles) + turned * jnp.sin(angles)).astype(jnp.bfloat16)

def attend_blocks(queries, keys_all, values_all):
    count_q, kv_count, group_size, head_width = queries.shape
    block = min(512, count_q)
    blocks = count_q // block
    scale = head_width ** (-0.5)
    zero_index = jnp.zeros((), jnp.int32)

    def one_item(item):
        which = (item // kv_count).astype(jnp.int32)
        head_index = (item % kv_count).astype(jnp.int32)
        start_row = (which * block).astype(jnp.int32)
        q_block = lax.dynamic_slice(queries, (start_row, head_index, zero_index, zero_index), (block, 1, group_size, head_width))[:, 0]
        key_block = lax.dynamic_slice(keys_all, (zero_index, head_index, zero_index), (keys_all.shape[0], 1, head_width))[:, 0]
        value_block = lax.dynamic_slice(values_all, (zero_index, head_index, zero_index), (values_all.shape[0], 1, head_width))[:, 0]
        scores = jnp.einsum('qgd,sd->gqs', q_block.astype(jnp.float32), key_block.astype(jnp.float32)) * scale
        shifted = jnp.exp(scores - lax.optimization_barrier(jnp.max(scores, axis=-1, keepdims=True)))
        weights = (shifted / lax.optimization_barrier(jnp.sum(shifted, axis=-1, keepdims=True))).astype(jnp.bfloat16)
        return jnp.einsum('gqs,sd->qgd', weights.astype(jnp.float32), value_block.astype(jnp.float32)).astype(jnp.bfloat16)
    results = lax.map(one_item, jnp.arange(blocks * kv_count, dtype=jnp.int32))
    results = results.reshape(blocks, kv_count, block, group_size, head_width).transpose(0, 2, 1, 3, 4)
    return results.reshape(count_q, kv_count * group_size * head_width)

def rms_scale(values, gain_vec):
    floats = values.astype(jnp.float32)
    return floats * lax.rsqrt(lax.optimization_barrier(jnp.mean(floats * floats, axis=-1, keepdims=True)) + EPSILON) * gain_vec

def reference(residual_in, query_proj, key_proj, value_proj, query_gain, key_gain, out_weight, post_gain, pre_gain, route_ids, group_weight, first_share, gate_weight, up_weight, down_weight):
    group_size = HEADS // KV_HEADS

    def one_sequence(inputs):
        query_seq, key_seq, value_seq = inputs
        positions = jnp.arange(SEQ, dtype=jnp.int32)
        query_turned = rotate_heads(query_seq.reshape(SEQ, HEADS, HEAD_DIM), query_gain, positions)
        key_turned = rotate_heads(key_seq.reshape(SEQ, KV_HEADS, HEAD_DIM), key_gain, positions)
        return attend_blocks(query_turned.reshape(SEQ, KV_HEADS, group_size, HEAD_DIM), key_turned, value_seq.reshape(SEQ, KV_HEADS, HEAD_DIM))
    attended = lax.map(one_sequence, (query_proj, key_proj, value_proj)).reshape(SEQS * SEQ, D)
    mixed = jnp.dot(attended, out_weight, preferred_element_type=jnp.float32).astype(jnp.bfloat16)
    stream = (residual_in.reshape(SEQS * SEQ, D).astype(jnp.float32) + rms_scale(mixed, post_gain)).astype(jnp.bfloat16)
    normed = rms_scale(stream, pre_gain).astype(jnp.bfloat16)
    chosen = route_ids.reshape(-1).astype(jnp.int32)
    assigns = chosen.shape[0]
    order = jnp.argsort(chosen, stable=True).astype(jnp.int32)
    counts = jax.ops.segment_sum(jnp.ones((assigns,), jnp.int32), chosen, num_segments=EXPERTS).astype(jnp.int32)
    starts = (jnp.cumsum(counts) - counts).astype(jnp.int32)
    most = CAP * N_SP * N_DP
    order_pad = jnp.concatenate([order, jnp.full((most,), assigns, jnp.int32)])
    normed_pad = jnp.concatenate([normed, jnp.zeros((1, D), jnp.bfloat16)], axis=0)

    def per_expert(carry, inputs):
        index, gate_one, up_one, down_one = inputs
        picked = lax.dynamic_slice(order_pad, (starts[index].astype(jnp.int32),), (most,))
        valid = jnp.arange(most, dtype=jnp.int32) < counts[index]
        picked = jnp.where(valid, picked, assigns).astype(jnp.int32)
        rows_in = normed_pad[picked // 2]
        gated = jnp.dot(rows_in, gate_one, preferred_element_type=jnp.float32)
        lifted = jnp.dot(rows_in, up_one, preferred_element_type=jnp.float32)
        hidden = (jax.nn.silu(gated) * lifted).astype(jnp.bfloat16)
        produced = jnp.dot(hidden, down_one, preferred_element_type=jnp.float32).astype(jnp.bfloat16)
        return (carry.at[picked].set(produced), None)
    outputs, _ = lax.scan(per_expert, jnp.zeros((assigns + 1, D), jnp.bfloat16), (jnp.arange(EXPERTS, dtype=jnp.int32), gate_weight, up_weight, down_weight))
    results = outputs[:assigns].astype(jnp.float32).reshape(SEQS * SEQ, 2, D)
    share = first_share.reshape(-1)
    weight_pair = group_weight.reshape(-1)[:, None] * jnp.stack([share, 1.0 - share], axis=1)
    combined = lax.optimization_barrier(jnp.sum(weight_pair[:, :, None] * results, axis=1))
    return (stream.astype(jnp.float32) + combined).astype(jnp.bfloat16).reshape(SEQS, SEQ, D)
```

```python
import functools

import jax
import jax.numpy as jnp
import numpy as np
from jax import lax
from jax.experimental import pallas as pl
from jax.experimental.pallas import tpu as pltpu
from jax.sharding import PartitionSpec as P

HEADS = 16
KV_HEADS = 4
HEAD_DIM = 128
GRID_W = 64
RING = 4
EPSILON = 1e-06
MESH = pl.DeviceIdType.MESH
F32 = jnp.float32
BF16 = jnp.bfloat16


def angle_tables():
    quarter = HEAD_DIM // 4
    inverse = (np.float32(10000.0) ** (-np.arange(quarter, dtype=np.float32) / quarter)).astype(
        np.float32
    )
    places = np.concatenate([np.arange(32), np.arange(GRID_W)]).astype(np.float32)
    angles = places[:, None] * np.tile(inverse, 4)[None, :]
    return np.stack([np.cos(angles), np.sin(angles)]).astype(np.float32)


def position():
    s = lax.axis_index("sp")
    d = lax.axis_index("dp")
    return s // RING, s % RING, d // 2, d % 2


def at(z, x, y, c):
    return (
        ((z + 2 * RING) % RING) * RING + (x + 2 * RING) % RING,
        ((y + 2 * RING) % RING) * 2 + c,
    )


def turn(heads, gain, cos, sin):
    normed = (
        heads * lax.rsqrt(jnp.mean(heads * heads, axis=-1, keepdims=True) + EPSILON) * gain
    )
    lane = lax.broadcasted_iota(jnp.int32, normed.shape, 1)
    turned = jnp.where(
        (lane // 32) % 2 == 0, -pltpu.roll(normed, 96, 1), pltpu.roll(normed, 32, 1)
    )
    return (normed * cos + turned * sin).astype(BF16)


def attention_kernel(
    q_hbm, k_hbm, v_hbm, w_hbm, res_hbm, table_ref, qg_ref, kg_ref, postg_ref, preg_ref,
    stream_ref, normed_ref,
    kv, qt, q_raw, k_raw, v_raw, w, res, top, total, acc, att, mixed,
    local_sem, send_sem, recv_sem,
):
    z, x, y, c = position()
    right, left = at(z, x + 1, y, c), at(z, x - 1, y, c)
    up, down = at(z + 1, x, y, c), at(z - 1, x, y, c)

    loads = []
    for i, (src, dst) in enumerate(
        [(k_hbm, k_raw), (v_hbm, v_raw), (q_hbm, q_raw), (res_hbm, res), (w_hbm, w)]
    ):
        load = pltpu.make_async_copy(src, dst, local_sem.at[i])
        load.start()
        loads.append(load)

    barrier = pltpu.get_barrier_semaphore()
    for peer in (right, left, up, down):
        pl.semaphore_signal(barrier, inc=1, device_id=peer, device_id_type=MESH)

    lane = lax.broadcasted_iota(jnp.int32, (GRID_W, HEAD_DIM), 1)

    def table(which):
        halves = []
        for part in range(2):
            row = table_ref[which, pl.ds(2 * (z * RING + x) + part, 1), :]
            halves.append(jnp.where(lane < 64, row, table_ref[which, 32 : 32 + GRID_W, :]))
        return jnp.concatenate(halves, axis=0)

    cos, sin = table(0), table(1)
    loads[0].wait()
    for h in range(KV_HEADS):
        raw = k_raw[:, h * 128 : (h + 1) * 128].astype(F32)
        kv[h // 2, 0, 0, :, (h % 2) * 128 : (h % 2 + 1) * 128] = turn(raw, kg_ref[...], cos, sin)
    loads[1].wait()
    for half in range(2):
        kv[half, 0, 0, :, 256:512] = v_raw[:, half * 256 : (half + 1) * 256]
    pl.semaphore_wait(barrier, 4)

    messages = {}
    first = {0: (right, left), 1: (up, down)}
    second = {0: (up, down), 1: (right, left)}

    def message(name, src, dst, peer):
        i = len(messages)
        messages[name] = pltpu.make_async_remote_copy(
            src_ref=src,
            dst_ref=dst,
            send_sem=send_sem.at[i],
            recv_sem=recv_sem.at[i],
            device_id=peer,
            device_id_type=MESH,
        )

    low, high = pl.ds(0, 64), pl.ds(64, 64)
    for p in range(2):
        plus, minus = first[p]
        message(("own+", p), kv.at[p, 0, 0], kv.at[p, 0, 3], plus)
        message(("own-", p), kv.at[p, 0, 0], kv.at[p, 0, 1], minus)
        message(("relay+", p), kv.at[p, 0, 3, low], kv.at[p, 0, 2, low], plus)
        message(("relay-", p), kv.at[p, 0, 1, high], kv.at[p, 0, 2, high], minus)
        plus, minus = second[p]
        for r in range(4):
            message(("far+", p, r), kv.at[p, 0, r], kv.at[p, 3, r], plus)
            message(("far-", p, r), kv.at[p, 0, r], kv.at[p, 1, r], minus)
            message(("last+", p, r), kv.at[p, 3, r, low], kv.at[p, 2, r, low], plus)
            message(("last-", p, r), kv.at[p, 1, r, high], kv.at[p, 2, r, high], minus)

    def start(kind, *key):
        for sign in "+-":
            messages[(kind + sign,) + key].start()

    def arrived(kind, *key):
        for sign in "+-":
            messages[(kind + sign,) + key].wait_recv()

    start("own", 0)
    start("own", 1)
    start("far", 0, 0)
    start("far", 1, 0)

    loads[2].wait()
    for h in range(HEADS):
        raw = q_raw[:, h * 128 : (h + 1) * 128].astype(F32)
        qt[h // 4, (h % 4) * 128 : (h % 4 + 1) * 128, :] = turn(raw, qg_ref[...], cos, sin)

    for p in range(2):
        arrived("own", p)
        start("relay", p)
        start("far", p, 3)
        start("far", p, 1)
    for p in range(2):
        arrived("far", p, 0)
        start("last", p, 0)
    for p in range(2):
        arrived("relay", p)
        start("far", p, 2)

    scale = float(np.log2(np.e) / np.sqrt(HEAD_DIM))

    def attend(r, opening):
        def one(g, carry):
            p, h = g // 2, g % 2
            keys = kv[p, r, :, :, pl.ds(pl.multiple_of(h * 128, 128), 128)].reshape(512, 128)
            values = kv[p, r, :, :, pl.ds(pl.multiple_of(256 + h * 128, 128), 128)].reshape(
                512, 128
            )
            scores = lax.dot_general(
                qt[g], keys, (((1,), (1,)), ((), ())), preferred_element_type=F32
            )
            peak = jnp.max(scores, axis=-1, keepdims=True)
            if not opening:
                before = top[g]
                peak = jnp.maximum(peak, before)
            weights = jnp.exp2((scores - peak) * scale)
            summed = jnp.sum(weights, axis=-1, keepdims=True)
            out = jnp.dot(weights.astype(BF16), values, preferred_element_type=F32)
            if not opening:
                shrink = jnp.exp2((before - peak) * scale)
                summed += total[g] * shrink
                out += acc[g] * shrink
            top[g] = peak
            total[g] = summed
            acc[g] = out
            return carry

        lax.fori_loop(0, KV_HEADS, one, 0)

    attend(0, True)
    for r in (3, 1):
        for p in range(2):
            arrived("far", p, r)
            start("last", p, r)
    for p in range(2):
        arrived("far", p, 2)
        start("last", p, 2)
    attend(3, False)
    attend(1, False)
    for p in range(2):
        for r in range(4):
            arrived("last", p, r)
    attend(2, False)

    for h in range(HEADS):
        rows = slice((h % 4) * 128, (h % 4 + 1) * 128)
        att[:, h * 128 : (h + 1) * 128] = (acc[h // 4, rows, :] / total[h // 4, rows, :]).astype(
            BF16
        )
    loads[3].wait()
    loads[4].wait()

    def project(n, carry):
        cols = pl.ds(pl.multiple_of(n * 512, 512), 512)
        mixed[:, cols] = jnp.dot(att[...], w[:, cols], preferred_element_type=F32).astype(BF16)
        return carry

    lax.fori_loop(0, 4, project, 0)

    def norm(n, carry):
        rows = pl.ds(pl.multiple_of(n * 16, 16), 16)
        m = mixed[rows, :].astype(F32)
        m = m * lax.rsqrt(jnp.mean(m * m, axis=-1, keepdims=True) + EPSILON) * postg_ref[...]
        stream = (res[rows, :].astype(F32) + m).astype(BF16)
        stream_ref[rows, :] = stream
        s = stream.astype(F32)
        s = s * lax.rsqrt(jnp.mean(s * s, axis=-1, keepdims=True) + EPSILON) * preg_ref[...]
        normed_ref[rows, :] = s.astype(BF16)
        return carry

    lax.fori_loop(0, 8, norm, 0)
    for m in messages.values():
        m.wait_send()


def attention(q, k, v, w, res, query_gain, key_gain, post_gain, pre_gain):
    hbm = pl.BlockSpec(memory_space=pl.ANY)
    vmem = pl.BlockSpec(memory_space=pltpu.VMEM)
    tokens, width = q.shape
    return pl.pallas_call(
        attention_kernel,
        out_shape=[jax.ShapeDtypeStruct((tokens, width), BF16)] * 2,
        in_specs=[hbm] * 5 + [vmem] * 5,
        out_specs=[vmem] * 2,
        scratch_shapes=[
            pltpu.VMEM((2, 4, 4, 128, 512), BF16),
            pltpu.VMEM((4, 512, 128), BF16),
            pltpu.VMEM((tokens, width), BF16),
            pltpu.VMEM((tokens, 512), BF16),
            pltpu.VMEM((tokens, 512), BF16),
            pltpu.VMEM((width, width), BF16),
            pltpu.VMEM((tokens, width), BF16),
            pltpu.VMEM((4, 512, 1), F32),
            pltpu.VMEM((4, 512, 1), F32),
            pltpu.VMEM((4, 512, 128), F32),
            pltpu.VMEM((tokens, width), BF16),
            pltpu.VMEM((tokens, width), BF16),
            pltpu.SemaphoreType.DMA((5,)),
            pltpu.SemaphoreType.DMA((40,)),
            pltpu.SemaphoreType.DMA((40,)),
        ],
        compiler_params=pltpu.CompilerParams(
            collective_id=0, has_side_effects=True, vmem_limit_bytes=60 * 1024 * 1024
        ),
        name="attention",
    )(
        q, k, v, w, res, jnp.asarray(angle_tables()), query_gain.reshape(1, -1),
        key_gain.reshape(1, -1), post_gain.reshape(1, -1), pre_gain.reshape(1, -1),
    )


def expert_ffn(arrived, gate_weight, up_weight, down_weight):
    gated = jnp.einsum("nesd,edf->nesf", arrived, gate_weight, preferred_element_type=jnp.float32)
    lifted = jnp.einsum("nesd,edf->nesf", arrived, up_weight, preferred_element_type=jnp.float32)
    hidden = (jax.nn.silu(gated) * lifted).astype(jnp.bfloat16)
    return jnp.einsum(
        "nesf,efd->nesd", hidden, down_weight, preferred_element_type=jnp.float32
    ).astype(jnp.bfloat16)


def local(
    residual_in,
    query_proj,
    key_proj,
    value_proj,
    query_gain,
    key_gain,
    out_weight,
    post_gain,
    pre_gain,
    route_ids,
    group_weight,
    first_share,
    gate_weight,
    up_weight,
    down_weight,
):
    sp_count = lax.axis_size("sp")
    dp_count = lax.axis_size("dp")
    tokens = query_proj.shape[1]
    stream, normed = attention(
        query_proj[0], key_proj[0], value_proj[0], out_weight, residual_in[0],
        query_gain, key_gain, post_gain, pre_gain,
    )
    model_width = normed.shape[1]
    local_experts = gate_weight.shape[0]
    expert_count = local_experts * sp_count * dp_count
    capacity = 4 * tokens // expert_count
    chosen = route_ids.reshape(2 * tokens)
    onehot = (chosen[:, None] == jnp.arange(expert_count, dtype=jnp.int32)[None, :]).astype(
        jnp.int32
    )
    earlier = jnp.cumsum(onehot, axis=0) - onehot
    slot_rank = jnp.sum(earlier * onehot, axis=1)
    slot_index = chosen * capacity + slot_rank
    source_row = (
        jnp.full((expert_count * capacity,), tokens, jnp.int32)
        .at[slot_index]
        .set(jnp.arange(2 * tokens, dtype=jnp.int32) // 2)
    )
    padded = jnp.concatenate([normed, jnp.zeros((1, model_width), jnp.bfloat16)], axis=0)
    outgoing = padded[source_row]
    shaped = outgoing.reshape(sp_count * dp_count, local_experts, capacity, model_width)
    answered = expert_ffn(
        lax.all_to_all(shaped, ("sp", "dp"), split_axis=0, concat_axis=0, tiled=True),
        gate_weight,
        up_weight,
        down_weight,
    )
    returned = lax.all_to_all(answered, ("sp", "dp"), split_axis=0, concat_axis=0, tiled=True)
    results = (
        returned.reshape(expert_count * capacity, model_width)[slot_index]
        .astype(jnp.float32)
        .reshape(tokens, 2, model_width)
    )
    share = first_share[0]
    weight_pair = group_weight[0][:, None] * jnp.stack([share, 1.0 - share], axis=1)
    combined = jnp.sum(weight_pair[:, :, None] * results, axis=1)
    return (
        (stream.astype(jnp.float32) + combined).astype(jnp.bfloat16).reshape(1, tokens, model_width)
    )


def solution(mesh):
    placed = (
        P("dp", "sp", None),
        P("dp", "sp", None),
        P("dp", "sp", None),
        P("dp", "sp", None),
        P(),
        P(),
        P(),
        P(),
        P(),
        P("dp", "sp", None),
        P("dp", "sp"),
        P("dp", "sp"),
        P(("sp", "dp"), None, None),
        P(("sp", "dp"), None, None),
        P(("sp", "dp"), None, None),
    )
    return jax.shard_map(
        local, mesh=mesh, in_specs=placed, out_specs=P("dp", "sp", None), check_vma=False
    )
```

```python
import jax
import jax.numpy as jnp
import numpy as np
from jax import lax
from jax.experimental import pallas as pl
from jax.experimental.pallas import tpu as pltpu
from jax.sharding import PartitionSpec as P

HEADS = 16
KV_HEADS = 4
HEAD_DIM = 128
GRID_W = 64
RING = 4
EPSILON = 1e-06
MESH = pl.DeviceIdType.MESH
F32 = jnp.float32
BF16 = jnp.bfloat16


def angle_tables():
    quarter = HEAD_DIM // 4
    inverse = (np.float32(10000.0) ** (-np.arange(quarter, dtype=np.float32) / quarter)).astype(
        np.float32
    )
    places = np.concatenate([np.arange(32), np.arange(GRID_W)]).astype(np.float32)
    angles = places[:, None] * np.tile(inverse, 4)[None, :]
    return np.stack([np.cos(angles), np.sin(angles)]).astype(np.float32)


def position():
    s = lax.axis_index("sp")
    d = lax.axis_index("dp")
    return s // RING, s % RING, d // 2, d % 2


def at(z, x, y, c):
    return (
        ((z + 2 * RING) % RING) * RING + (x + 2 * RING) % RING,
        ((y + 2 * RING) % RING) * 2 + c,
    )


def turn(heads, gain, cos, sin):
    normed = (
        heads * lax.rsqrt(jnp.mean(heads * heads, axis=-1, keepdims=True) + EPSILON) * gain
    )
    lane = lax.broadcasted_iota(jnp.int32, normed.shape, 1)
    turned = jnp.where(
        (lane // 32) % 2 == 0, -pltpu.roll(normed, 96, 1), pltpu.roll(normed, 32, 1)
    )
    return (normed * cos + turned * sin).astype(BF16)


def attention_kernel(
    q_hbm, k_hbm, v_hbm, w_hbm, res_hbm, table_ref, qg_ref, kg_ref, postg_ref, preg_ref,
    stream_ref, normed_ref,
    kv, qt, q_raw, k_raw, v_raw, w, res, top, total, acc, att, mixed,
    local_sem, send_sem, recv_sem,
):
    z, x, y, c = position()
    right, left = at(z, x + 1, y, c), at(z, x - 1, y, c)
    up, down = at(z + 1, x, y, c), at(z - 1, x, y, c)

    loads = []
    for i, (src, dst) in enumerate(
        [(k_hbm, k_raw), (v_hbm, v_raw), (q_hbm, q_raw), (res_hbm, res), (w_hbm, w)]
    ):
        load = pltpu.make_async_copy(src, dst, local_sem.at[i])
        load.start()
        loads.append(load)

    barrier = pltpu.get_barrier_semaphore()
    for peer in (right, left, up, down):
        pl.semaphore_signal(barrier, inc=1, device_id=peer, device_id_type=MESH)

    lane = lax.broadcasted_iota(jnp.int32, (GRID_W, HEAD_DIM), 1)

    def table(which):
        halves = []
        for part in range(2):
            row = table_ref[which, pl.ds(2 * (z * RING + x) + part, 1), :]
            halves.append(jnp.where(lane < 64, row, table_ref[which, 32 : 32 + GRID_W, :]))
        return jnp.concatenate(halves, axis=0)

    cos, sin = table(0), table(1)
    loads[0].wait()
    for h in range(KV_HEADS):
        raw = k_raw[:, h * 128 : (h + 1) * 128].astype(F32)
        kv[h // 2, 0, 0, :, (h % 2) * 128 : (h % 2 + 1) * 128] = turn(raw, kg_ref[...], cos, sin)
    loads[1].wait()
    for half in range(2):
        kv[half, 0, 0, :, 256:512] = v_raw[:, half * 256 : (half + 1) * 256]
    pl.semaphore_wait(barrier, 4)

    messages = {}
    first = {0: (right, left), 1: (up, down)}
    second = {0: (up, down), 1: (right, left)}

    def message(name, src, dst, peer):
        i = len(messages)
        messages[name] = pltpu.make_async_remote_copy(
            src_ref=src,
            dst_ref=dst,
            send_sem=send_sem.at[i],
            recv_sem=recv_sem.at[i],
            device_id=peer,
            device_id_type=MESH,
        )

    low, high = pl.ds(0, 64), pl.ds(64, 64)
    for p in range(2):
        plus, minus = first[p]
        message(("own+", p), kv.at[p, 0, 0], kv.at[p, 0, 3], plus)
        message(("own-", p), kv.at[p, 0, 0], kv.at[p, 0, 1], minus)
        message(("relay+", p), kv.at[p, 0, 3, low], kv.at[p, 0, 2, low], plus)
        message(("relay-", p), kv.at[p, 0, 1, high], kv.at[p, 0, 2, high], minus)
        plus, minus = second[p]
        for r in range(4):
            message(("far+", p, r), kv.at[p, 0, r], kv.at[p, 3, r], plus)
            message(("far-", p, r), kv.at[p, 0, r], kv.at[p, 1, r], minus)
            message(("last+", p, r), kv.at[p, 3, r, low], kv.at[p, 2, r, low], plus)
            message(("last-", p, r), kv.at[p, 1, r, high], kv.at[p, 2, r, high], minus)

    def start(kind, *key):
        for sign in "+-":
            messages[(kind + sign,) + key].start()

    def arrived(kind, *key):
        for sign in "+-":
            messages[(kind + sign,) + key].wait_recv()

    start("own", 0)
    start("own", 1)
    start("far", 0, 0)
    start("far", 1, 0)

    loads[2].wait()
    for h in range(HEADS):
        raw = q_raw[:, h * 128 : (h + 1) * 128].astype(F32)
        qt[h // 4, (h % 4) * 128 : (h % 4 + 1) * 128, :] = turn(raw, qg_ref[...], cos, sin)

    for p in range(2):
        arrived("own", p)
        start("relay", p)
        start("far", p, 3)
        start("far", p, 1)
    for p in range(2):
        arrived("far", p, 0)
        start("last", p, 0)
    for p in range(2):
        arrived("relay", p)
        start("far", p, 2)

    scale = float(np.log2(np.e) / np.sqrt(HEAD_DIM))

    def attend(r, opening):
        def one(g, carry):
            p, h = g // 2, g % 2
            keys = kv[p, r, :, :, pl.ds(pl.multiple_of(h * 128, 128), 128)].reshape(512, 128)
            values = kv[p, r, :, :, pl.ds(pl.multiple_of(256 + h * 128, 128), 128)].reshape(
                512, 128
            )
            scores = lax.dot_general(
                qt[g], keys, (((1,), (1,)), ((), ())), preferred_element_type=F32
            )
            peak = jnp.max(scores, axis=-1, keepdims=True)
            if not opening:
                before = top[g]
                peak = jnp.maximum(peak, before)
            weights = jnp.exp2((scores - peak) * scale)
            summed = jnp.sum(weights, axis=-1, keepdims=True)
            out = jnp.dot(weights.astype(BF16), values, preferred_element_type=F32)
            if not opening:
                shrink = jnp.exp2((before - peak) * scale)
                summed += total[g] * shrink
                out += acc[g] * shrink
            top[g] = peak
            total[g] = summed
            acc[g] = out
            return carry

        lax.fori_loop(0, KV_HEADS, one, 0)

    attend(0, True)
    for r in (3, 1):
        for p in range(2):
            arrived("far", p, r)
            start("last", p, r)
    for p in range(2):
        arrived("far", p, 2)
        start("last", p, 2)
    attend(3, False)
    attend(1, False)
    for p in range(2):
        for r in range(4):
            arrived("last", p, r)
    attend(2, False)

    for h in range(HEADS):
        rows = slice((h % 4) * 128, (h % 4 + 1) * 128)
        att[:, h * 128 : (h + 1) * 128] = (acc[h // 4, rows, :] / total[h // 4, rows, :]).astype(
            BF16
        )
    loads[3].wait()
    loads[4].wait()

    def project(n, carry):
        cols = pl.ds(pl.multiple_of(n * 512, 512), 512)
        mixed[:, cols] = jnp.dot(att[...], w[:, cols], preferred_element_type=F32).astype(BF16)
        return carry

    lax.fori_loop(0, 4, project, 0)

    def norm(n, carry):
        rows = pl.ds(pl.multiple_of(n * 16, 16), 16)
        m = mixed[rows, :].astype(F32)
        m = m * lax.rsqrt(jnp.mean(m * m, axis=-1, keepdims=True) + EPSILON) * postg_ref[...]
        stream = (res[rows, :].astype(F32) + m).astype(BF16)
        stream_ref[rows, :] = stream
        s = stream.astype(F32)
        s = s * lax.rsqrt(jnp.mean(s * s, axis=-1, keepdims=True) + EPSILON) * preg_ref[...]
        normed_ref[rows, :] = s.astype(BF16)
        return carry

    lax.fori_loop(0, 8, norm, 0)
    for m in messages.values():
        m.wait_send()


def attention(q, k, v, w, res, query_gain, key_gain, post_gain, pre_gain):
    hbm = pl.BlockSpec(memory_space=pl.ANY)
    vmem = pl.BlockSpec(memory_space=pltpu.VMEM)
    tokens, width = q.shape
    return pl.pallas_call(
        attention_kernel,
        out_shape=[jax.ShapeDtypeStruct((tokens, width), BF16)] * 2,
        in_specs=[hbm] * 5 + [vmem] * 5,
        out_specs=[vmem] * 2,
        scratch_shapes=[
            pltpu.VMEM((2, 4, 4, 128, 512), BF16),
            pltpu.VMEM((4, 512, 128), BF16),
            pltpu.VMEM((tokens, width), BF16),
            pltpu.VMEM((tokens, 512), BF16),
            pltpu.VMEM((tokens, 512), BF16),
            pltpu.VMEM((width, width), BF16),
            pltpu.VMEM((tokens, width), BF16),
            pltpu.VMEM((4, 512, 1), F32),
            pltpu.VMEM((4, 512, 1), F32),
            pltpu.VMEM((4, 512, 128), F32),
            pltpu.VMEM((tokens, width), BF16),
            pltpu.VMEM((tokens, width), BF16),
            pltpu.SemaphoreType.DMA((5,)),
            pltpu.SemaphoreType.DMA((40,)),
            pltpu.SemaphoreType.DMA((40,)),
        ],
        compiler_params=pltpu.CompilerParams(
            collective_id=0, has_side_effects=True, vmem_limit_bytes=60 * 1024 * 1024
        ),
        name="attention",
    )(
        q, k, v, w, res, jnp.asarray(angle_tables()), query_gain.reshape(1, -1),
        key_gain.reshape(1, -1), post_gain.reshape(1, -1), pre_gain.reshape(1, -1),
    )


class Exchange:
    def __init__(self, send_sem, recv_sem):
        self.send_sem, self.recv_sem, self.copies = send_sem, recv_sem, {}

    def start(self, name, src, dst, peer):
        i = len(self.copies)
        copy = pltpu.make_async_remote_copy(
            src_ref=src,
            dst_ref=dst,
            send_sem=self.send_sem.at[i],
            recv_sem=self.recv_sem.at[i],
            device_id=peer,
            device_id_type=MESH,
        )
        assert name not in self.copies
        self.copies[name] = copy
        copy.start()

    def arrived(self, name):
        self.copies[name].wait_recv()

    def finish(self):
        for copy in self.copies.values():
            copy.wait_send()


CHUNKS = 2


def flat(ref, cols, lead):
    block = ref[lead + (slice(None),) * (len(ref.shape) - len(lead) - 1) + (cols,)]
    return block.reshape(-1, block.shape[-1])


def expert_kernel(
    normed_ref, ids_ref, gw_ref, fs_ref, stream_hbm, gate_hbm, up_hbm, down_hbm,
    out_ref,
    stream, gate, up, down, meta,
    zs, rows, zrel, xs, xr, xrel, yr, yrel, gates, lifts, hidden,
    made, back, backrel, ret, retrel, comb, zret, zretrel,
    spread, pick1, pick2, home,
    local_sem, send_sem, recv_sem,
):
    z, x, y, c = position()
    width = normed_ref.shape[1]
    step = width // CHUNKS
    ring = {
        "z": (at(z + 1, x, y, c), at(z - 1, x, y, c)),
        "x": (at(z, x + 1, y, c), at(z, x - 1, y, c)),
        "y": (at(z, x, y + 1, c), at(z, x, y - 1, c)),
        "yc": (at(z, x, y + 1, 1 - c), at(z, x, y - 1, 1 - c)),
    }
    across, twin = at(z + 2, x, y, c), at(z, x, y, 1 - c)

    loads = []
    for i, (src, dst) in enumerate(
        [(gate_hbm.at[0], gate), (up_hbm.at[0], up), (down_hbm.at[0], down), (stream_hbm, stream)]
    ):
        load = pltpu.make_async_copy(src, dst, local_sem.at[i])
        load.start()
        loads.append(load)

    barrier = pltpu.get_barrier_semaphore()
    peers = [p for pair in ring.values() for p in pair] + [across, twin]
    for peer in peers:
        pl.semaphore_signal(barrier, inc=1, device_id=peer, device_id_type=MESH)

    ex = Exchange(send_sem, recv_sem)

    def iota(shape, dim):
        return lax.broadcasted_iota(jnp.int32, shape, dim)

    eye = iota((128, 128), 0) == iota((128, 128), 1)
    earlier = (iota((128, 128), 0) < iota((128, 128), 1)).astype(F32)

    def lay(column):
        return jnp.sum(jnp.where(eye, column, 0.0), axis=0, keepdims=True)

    def stand(row):
        return jnp.sum(jnp.where(eye, row, 0.0), axis=1, keepdims=True)

    def counted(members):
        return jnp.dot(members, earlier, preferred_element_type=F32)

    ids = ids_ref[...].astype(F32)
    meta[0, 0:1, :] = lay(ids[:, 0:1])
    meta[0, 1:2, :] = lay(ids[:, 1:2])
    meta[0, 2:3, :] = gw_ref[...]
    meta[0, 3:4, :] = fs_ref[...]
    meta[0, 4:8, :] = jnp.zeros((4, 128), F32)

    pl.semaphore_wait(barrier, len(peers))
    ex.start("meta+", meta.at[0], meta.at[3], ring["z"][0])
    ex.start("meta-", meta.at[0], meta.at[1], ring["z"][1])
    ex.start("meta2", meta.at[0], meta.at[2], across)

    relative = ((meta[0, 0:1, :].astype(jnp.int32) >> 5) - z + 4) & 3
    members = (iota((8, 128), 0) == relative).astype(F32)
    rank = jnp.sum(members * counted(members), axis=0, keepdims=True)
    target = relative.astype(F32) * 32.0 + rank
    pack = (iota((128, 128), 0).astype(F32) == target).astype(BF16)
    home[...] = (iota((128, 128), 1).astype(F32) == stand(target)).astype(BF16)

    def chunk(i):
        return pl.ds(i * step, step)

    def halves(ref, key, cols):
        return ref.at[key + (pl.ds(0, 16), cols)], ref.at[key + (pl.ds(16, 16), cols)]

    def ring_send(tag, axis, i, opposite, relays, direct):
        plus, minus = ring[axis]
        ex.start((tag, "out+", i), opposite[0], relays[0], plus)
        ex.start((tag, "out-", i), opposite[1], relays[1], minus)
        ex.start((tag, "+", i), direct[0][0], direct[0][1], plus)
        ex.start((tag, "-", i), direct[1][0], direct[1][1], minus)

    def ring_forward(tag, axis, i, relays, finals):
        plus, minus = ring[axis]
        ex.arrived((tag, "out+", i))
        ex.start((tag, "on+", i), relays[0], finals[0], plus)
        ex.arrived((tag, "out-", i))
        ex.start((tag, "on-", i), relays[1], finals[1], minus)

    def z_out(i, src, dst, relay):
        cols = chunk(i)
        relays = relay.at[0, :, cols], relay.at[1, :, cols]
        ring_send(
            ("z", id_of(src)), "z", i, halves(src, (2,), cols), relays,
            (
                (src.at[1, :, cols], dst.at[3, :, cols]),
                (src.at[3, :, cols], dst.at[1, :, cols]),
            ),
        )

    def id_of(ref):
        return "d" if ref is zs else "r"

    def z_on(i, src, dst, relay):
        cols = chunk(i)
        relays = relay.at[0, :, cols], relay.at[1, :, cols]
        ring_forward(("z", id_of(src)), "z", i, relays, halves(dst, (2,), cols))

    def z_in(i, src):
        for sign in ("+", "-", "on+", "on-"):
            ex.arrived((("z", id_of(src)), sign, i))

    for i in range(CHUNKS):
        cols = chunk(i)
        packed = jnp.dot(pack, normed_ref[:, cols], preferred_element_type=F32).astype(BF16)
        zs[:, :, cols] = packed.reshape(4, 32, step)
        rows[0, :, cols] = packed[0:32]
        z_out(i, zs, rows, zrel)

    for name in ("meta+", "meta-", "meta2"):
        ex.arrived(name)
    stacks = [[], [], [], []]
    for r in range(4):
        first = meta[r, 0:1, :]
        inside = (first.astype(jnp.int32) >> 5) == z
        members = jnp.broadcast_to(inside.astype(F32), (8, 128))
        rank = counted(members)[0:1]
        places = jnp.where(inside, rank, -1.0)
        taken = iota((32, 128), 0).astype(F32) == places
        for which in range(4):
            stacks[which].append(
                jnp.sum(
                    jnp.where(taken, meta[r, which : which + 1, :], 0.0), axis=1, keepdims=True
                )
            )
    first, second, group_share, first_share = [jnp.concatenate(s, axis=0) for s in stacks]

    def relative_expert(column):
        e = lay(column).astype(jnp.int32) & 31
        return ((((e >> 3) - x + 4) & 3) << 3) + (((((e >> 1) & 3) - y + 4) & 3) << 1) + (
            (e & 1) ^ c
        )

    rel1, rel2 = relative_expert(first), relative_expert(second)
    named1 = (iota((32, 128), 0) == rel1).astype(F32)
    named2 = (iota((32, 128), 0) == rel2).astype(F32)
    ahead = counted(named1 + named2)
    slot1 = rel1.astype(F32) * 16.0 + jnp.sum(named1 * ahead, axis=0, keepdims=True)
    slot2 = rel2.astype(F32) * 16.0 + jnp.sum(named2 * ahead, axis=0, keepdims=True)
    places = iota((512, 128), 0).astype(F32)
    spread[...] = ((places == slot1) | (places == slot2)).astype(BF16)
    places = iota((128, 512), 1).astype(F32)
    pick1[...] = (places == stand(slot1)).astype(BF16)
    pick2[...] = (places == stand(slot2)).astype(BF16)
    weight1 = group_share * first_share
    weight2 = group_share * (1.0 - first_share)

    def x_parts(i, relay, dst):
        cols = chunk(i)
        relays = relay.at[0, :, :, :, cols], relay.at[1, :, :, :, cols]
        finals = dst.at[2, pl.ds(0, 2), :, :, cols], dst.at[2, pl.ds(2, 2), :, :, cols]
        return relays, finals

    def x_out(tag, i, src, dst, relay):
        cols = chunk(i)
        relays, _ = x_parts(i, relay, dst)
        ring_send(
            (tag, "x"), "x", i,
            (src.at[2, pl.ds(0, 2), :, :, cols], src.at[2, pl.ds(2, 2), :, :, cols]), relays,
            (
                (src.at[1, :, :, :, cols], dst.at[3, :, :, :, cols]),
                (src.at[3, :, :, :, cols], dst.at[1, :, :, :, cols]),
            ),
        )

    def x_on(tag, i, dst, relay):
        relays, finals = x_parts(i, relay, dst)
        ring_forward((tag, "x"), "x", i, relays, finals)

    def y_out(tag, i, r, src, dst, relay):
        name = (tag, "y", r)
        ring_send(
            name, "y", i, (src(2, 0), src(2, 1)), (relay.at[0, r, :, chunk(i)], relay.at[1, r, :, chunk(i)]),
            ((src(1, 0), dst(3, 0)), (src(3, 0), dst(1, 0))),
        )
        ex.start((name, "c+", i), src(1, 1), dst(3, 1), ring["yc"][0])
        ex.start((name, "c-", i), src(3, 1), dst(1, 1), ring["yc"][1])
        ex.start((name, "twin", i), src(0, 1), dst(0, 1), twin)

    def y_on(tag, i, r, dst, relay):
        name = (tag, "y", r)
        ex.arrived((name, "out+", i))
        ex.start((name, "on+", i), relay.at[0, r, :, chunk(i)], dst(2, 0), ring["y"][0])
        ex.arrived((name, "out-", i))
        ex.start((name, "on-", i), relay.at[1, r, :, chunk(i)], dst(2, 1), ring["yc"][1])

    def y_in(tag, i, r):
        for sign in ("+", "-", "c+", "c-", "twin", "on+", "on-"):
            ex.arrived(((tag, "y", r), sign, i))

    def block(ref, r, cols):
        return lambda ry, rc: ref.at[r, ry, rc, :, cols]

    def to_expert(i, r):
        cols = chunk(i)
        source = xs if r == 0 else xr
        y_out("d", i, r, block(source, r, cols), block(yr, r, cols), yrel)
        yr[r, 0, 0, :, cols] = source[r, 0, 0, :, cols]

    for i in range(CHUNKS):
        cols = chunk(i)
        z_on(i, zs, rows, zrel)
        z_in(i, zs)
        slots = jnp.dot(
            spread[...], rows[:, :, cols].reshape(128, step), preferred_element_type=F32
        )
        xs[:, :, :, :, cols] = slots.astype(BF16).reshape(4, 4, 2, 16, step)
        x_out("d", i, xs, xr, xrel)
        to_expert(i, 0)
        x_on("d", i, xr, xrel)

    loads[0].wait()
    loads[1].wait()
    for i in range(CHUNKS):
        cols = chunk(i)
        y_on("d", i, 0, block(yr, 0, cols), yrel)
        ex.arrived((("d", "x"), "+", i))
        to_expert(i, 3)
        ex.arrived((("d", "x"), "-", i))
        to_expert(i, 1)
        y_on("d", i, 3, block(yr, 3, cols), yrel)
        y_on("d", i, 1, block(yr, 1, cols), yrel)
        ex.arrived((("d", "x"), "on+", i))
        ex.arrived((("d", "x"), "on-", i))
        to_expert(i, 2)
        y_on("d", i, 2, block(yr, 2, cols), yrel)
        for r in range(4):
            y_in("d", i, r)
        arrived = yr[:, :, :, :, cols].reshape(512, step)
        for total, weight in ((gates, gate), (lifts, up)):
            product = jnp.dot(arrived, weight[cols, :], preferred_element_type=F32)
            total[...] = product if i == 0 else total[...] + product

    g = gates[...]
    hidden[...] = (g / (1.0 + jnp.exp(-g)) * lifts[...]).astype(BF16)
    loads[2].wait()

    def landing(r, cols):
        return block(ret if r == 0 else back, r, cols)

    def x_back_parts(i):
        cols = chunk(i)
        relays = retrel.at[0, :, :, :, cols], retrel.at[1, :, :, :, cols]
        finals = ret.at[2, pl.ds(0, 2), :, :, cols], ret.at[2, pl.ds(2, 2), :, :, cols]
        return relays, finals

    for i in range(CHUNKS):
        cols = chunk(i)
        produced = jnp.dot(hidden[...], down[:, cols], preferred_element_type=F32)
        made[:, :, :, :, cols] = produced.astype(BF16).reshape(4, 4, 2, 16, step)
        for r in (2, 3, 1, 0):
            y_out("r", i, r, block(made, r, cols), landing(r, cols), backrel)
            (ret if r == 0 else back)[r, 0, 0, :, cols] = made[r, 0, 0, :, cols]

    for i in range(CHUNKS):
        cols = chunk(i)
        relays, finals = x_back_parts(i)
        plus, minus = ring["x"]
        for r in (2, 3, 1, 0):
            y_on("r", i, r, landing(r, cols), backrel)
        y_in("r", i, 2)
        ex.start(("r", "xout+", i), back.at[2, pl.ds(0, 2), :, :, cols], relays[0], plus)
        ex.start(("r", "xout-", i), back.at[2, pl.ds(2, 2), :, :, cols], relays[1], minus)
        y_in("r", i, 3)
        ex.start(("r", "x-", i), back.at[3, :, :, :, cols], ret.at[1, :, :, :, cols], minus)
        y_in("r", i, 1)
        ex.start(("r", "x+", i), back.at[1, :, :, :, cols], ret.at[3, :, :, :, cols], plus)
        ex.arrived(("r", "xout+", i))
        ex.start(("r", "xon+", i), relays[0], finals[0], plus)
        ex.arrived(("r", "xout-", i))
        ex.start(("r", "xon-", i), relays[1], finals[1], minus)
        y_in("r", i, 0)

    for i in range(CHUNKS):
        cols = chunk(i)
        for sign in ("x+", "x-", "xon+", "xon-"):
            ex.arrived(("r", sign, i))
        returned = ret[:, :, :, :, cols].reshape(512, step)
        one = jnp.dot(pick1[...], returned, preferred_element_type=F32)
        two = jnp.dot(pick2[...], returned, preferred_element_type=F32)
        mixed = (weight1 * one + weight2 * two).astype(BF16)
        comb[:, :, cols] = mixed.reshape(4, 32, step)
        zret[0, :, cols] = mixed[0:32]
        z_out(i, comb, zret, zretrel)

    loads[3].wait()
    for i in range(CHUNKS):
        cols = chunk(i)
        z_on(i, comb, zret, zretrel)
        z_in(i, comb)
        added = jnp.dot(
            home[...], zret[:, :, cols].reshape(128, step), preferred_element_type=F32
        )
        out_ref[:, cols] = (stream[:, cols].astype(F32) + added).astype(BF16)
    ex.finish()


def expert_layer(normed, ids, group_weight, first_share, stream, gate, up, down):
    hbm = pl.BlockSpec(memory_space=pl.ANY)
    vmem = pl.BlockSpec(memory_space=pltpu.VMEM)
    tokens, width = normed.shape
    _, _, ff = gate.shape
    slots = (4, 4, 2, 16, width)
    copies = 3 + 96 * CHUNKS
    return pl.pallas_call(
        expert_kernel,
        out_shape=jax.ShapeDtypeStruct((tokens, width), BF16),
        in_specs=[vmem] * 4 + [hbm] * 4,
        out_specs=vmem,
        scratch_shapes=[
            pltpu.VMEM((tokens, width), BF16),
            pltpu.VMEM((width, ff), BF16),
            pltpu.VMEM((width, ff), BF16),
            pltpu.VMEM((ff, width), BF16),
            pltpu.VMEM((4, 8, 128), F32),
            pltpu.VMEM((4, 32, width), BF16),
            pltpu.VMEM((4, 32, width), BF16),
            pltpu.VMEM((2, 16, width), BF16),
            pltpu.VMEM(slots, BF16),
            pltpu.VMEM(slots, BF16),
            pltpu.VMEM((2, 2, 2, 16, width), BF16),
            pltpu.VMEM(slots, BF16),
            pltpu.VMEM((2, 4, 16, width), BF16),
            pltpu.VMEM((512, ff), F32),
            pltpu.VMEM((512, ff), F32),
            pltpu.VMEM((512, ff), BF16),
            pltpu.VMEM(slots, BF16),
            pltpu.VMEM(slots, BF16),
            pltpu.VMEM((2, 4, 16, width), BF16),
            pltpu.VMEM(slots, BF16),
            pltpu.VMEM((2, 2, 2, 16, width), BF16),
            pltpu.VMEM((4, 32, width), BF16),
            pltpu.VMEM((4, 32, width), BF16),
            pltpu.VMEM((2, 16, width), BF16),
            pltpu.VMEM((512, 128), BF16),
            pltpu.VMEM((128, 512), BF16),
            pltpu.VMEM((128, 512), BF16),
            pltpu.VMEM((128, 128), BF16),
            pltpu.SemaphoreType.DMA((4,)),
            pltpu.SemaphoreType.DMA((copies,)),
            pltpu.SemaphoreType.DMA((copies,)),
        ],
        compiler_params=pltpu.CompilerParams(
            collective_id=1, has_side_effects=True, vmem_limit_bytes=60 * 1024 * 1024
        ),
        name="experts",
    )(normed, ids, group_weight, first_share, stream, gate, up, down)


def local(
    residual_in,
    query_proj,
    key_proj,
    value_proj,
    query_gain,
    key_gain,
    out_weight,
    post_gain,
    pre_gain,
    route_ids,
    group_weight,
    first_share,
    gate_weight,
    up_weight,
    down_weight,
):
    stream, normed = attention(
        query_proj[0], key_proj[0], value_proj[0], out_weight, residual_in[0],
        query_gain, key_gain, post_gain, pre_gain,
    )
    out = expert_layer(
        normed, route_ids[0], group_weight, first_share, stream,
        gate_weight, up_weight, down_weight,
    )
    return out[None]


def solution(mesh):
    placed = (
        P("dp", "sp", None),
        P("dp", "sp", None),
        P("dp", "sp", None),
        P("dp", "sp", None),
        P(),
        P(),
        P(),
        P(),
        P(),
        P("dp", "sp", None),
        P("dp", "sp"),
        P("dp", "sp"),
        P(("sp", "dp"), None, None),
        P(("sp", "dp"), None, None),
        P(("sp", "dp"), None, None),
    )
    return jax.shard_map(
        local, mesh=mesh, in_specs=placed, out_specs=P("dp", "sp", None), check_vma=False
    )
```

```python
import jax
import jax.numpy as jnp
import numpy as np
from jax import lax
from jax.experimental import pallas as pl
from jax.experimental.pallas import tpu as pltpu
from jax.sharding import PartitionSpec as P

HEADS = 16
KV_HEADS = 4
HEAD_DIM = 128
GRID_W = 64
RING = 4
EPSILON = 1e-06
MESH = pl.DeviceIdType.MESH


class Phase:
    def __init__(self):
        self.scope = None

    def __call__(self, name=None):
        if self.scope is not None:
            self.scope.__exit__(None, None, None)
        self.scope = None
        if name is not None:
            self.scope = jax.named_scope(name)
            self.scope.__enter__()


F32 = jnp.float32
BF16 = jnp.bfloat16


def angle_tables():
    quarter = HEAD_DIM // 4
    inverse = (np.float32(10000.0) ** (-np.arange(quarter, dtype=np.float32) / quarter)).astype(
        np.float32
    )
    places = np.concatenate([np.arange(32), np.arange(GRID_W)]).astype(np.float32)
    angles = places[:, None] * np.tile(inverse, 4)[None, :]
    return np.stack([np.cos(angles), np.sin(angles)]).astype(np.float32)


def position():
    s = lax.axis_index("sp")
    d = lax.axis_index("dp")
    return s // RING, s % RING, d // 2, d % 2


def at(z, x, y, c):
    return (
        ((z + 2 * RING) % RING) * RING + (x + 2 * RING) % RING,
        ((y + 2 * RING) % RING) * 2 + c,
    )


def turn(heads, gain, cos, sin):
    normed = (
        heads * lax.rsqrt(jnp.mean(heads * heads, axis=-1, keepdims=True) + EPSILON) * gain
    )
    lane = lax.broadcasted_iota(jnp.int32, normed.shape, 1)
    turned = jnp.where(
        (lane // 32) % 2 == 0, -pltpu.roll(normed, 96, 1), pltpu.roll(normed, 32, 1)
    )
    return (normed * cos + turned * sin).astype(BF16)


class Exchange:
    def __init__(self, send_sem, recv_sem):
        self.send_sem, self.recv_sem, self.copies = send_sem, recv_sem, {}

    def start(self, name, src, dst, peer):
        i = len(self.copies)
        copy = pltpu.make_async_remote_copy(
            src_ref=src,
            dst_ref=dst,
            send_sem=self.send_sem.at[i],
            recv_sem=self.recv_sem.at[i],
            device_id=peer,
            device_id_type=MESH,
        )
        assert name not in self.copies
        self.copies[name] = copy
        copy.start()

    def arrived(self, *names):
        for name in names:
            self.copies[name].wait_recv()

    def finish(self):
        for copy in self.copies.values():
            copy.wait_send()


ROUNDS = 2
COPIES = 40 + 3 + ROUNDS * (2 * 84 + 2 * 6)


def iota(shape, dim):
    return lax.broadcasted_iota(jnp.int32, shape, dim)


def layer_kernel(
    q_hbm, k_hbm, v_hbm, w_hbm, res_hbm, gate_hbm, up_hbm, down_hbm,
    table_ref, qg_ref, kg_ref, postg_ref, preg_ref, ids_ref, gw_ref, fs_ref,
    out_ref,
    kv, qt, q_raw, k_raw, v_raw, w, res, top, total, acc, att, mixed, normed,
    gate, up, down, meta,
    zs, rows, zrel, xs, xr, xrel, yr, yrel, gates, lifts, hidden,
    made, back, backrel, ret, retrel, comb, zret, zretrel,
    spread, pick1, pick2, home,
    local_sem, send_sem, recv_sem,
):
    z, x, y, c = position()
    width = q_raw.shape[1]
    phase = Phase()
    phase("turn")
    loads = {}
    for i, (name, src, dst) in enumerate(
        [
            ("k", k_hbm, k_raw), ("v", v_hbm, v_raw), ("q", q_hbm, q_raw), ("res", res_hbm, res),
            ("w", w_hbm, w), ("gate", gate_hbm.at[0], gate), ("up", up_hbm.at[0], up),
            ("down", down_hbm.at[0], down),
        ]
    ):
        loads[name] = pltpu.make_async_copy(src, dst, local_sem.at[i])
        loads[name].start()

    ring = {
        "z": (at(z + 1, x, y, c), at(z - 1, x, y, c)),
        "x": (at(z, x + 1, y, c), at(z, x - 1, y, c)),
        "y": (at(z, x, y + 1, c), at(z, x, y - 1, c)),
        "yc": (at(z, x, y + 1, 1 - c), at(z, x, y - 1, 1 - c)),
    }
    across, twin = at(z + 2, x, y, c), at(z, x, y, 1 - c)
    barrier = pltpu.get_barrier_semaphore()
    peers = [p for pair in ring.values() for p in pair] + [across, twin]
    for peer in peers:
        pl.semaphore_signal(barrier, inc=1, device_id=peer, device_id_type=MESH)
    ex = Exchange(send_sem, recv_sem)

    lane = iota((GRID_W, HEAD_DIM), 1)

    def table(which):
        halves = []
        for part in range(2):
            row = table_ref[which, pl.ds(2 * (z * RING + x) + part, 1), :]
            halves.append(jnp.where(lane < 64, row, table_ref[which, 32 : 32 + GRID_W, :]))
        return jnp.concatenate(halves, axis=0)

    cos, sin = table(0), table(1)
    meta[0, 0:2, :] = ids_ref[...].astype(F32)
    meta[0, 2:3, :] = gw_ref[...]
    meta[0, 3:4, :] = fs_ref[...]
    meta[0, 4:8, :] = jnp.zeros((4, 128), F32)
    loads["k"].wait()
    for h in range(KV_HEADS):
        raw = k_raw[:, h * 128 : (h + 1) * 128].astype(F32)
        kv[h // 2, 0, 0, :, (h % 2) * 128 : (h % 2 + 1) * 128] = turn(raw, kg_ref[...], cos, sin)
    loads["v"].wait()
    for half in range(2):
        kv[half, 0, 0, :, 256:512] = v_raw[:, half * 256 : (half + 1) * 256]
    phase("barrier")
    pl.semaphore_wait(barrier, len(peers))

    phase("start")
    first = ("x", "z")
    second = ("z", "x")
    low, high = pl.ds(0, 64), pl.ds(64, 64)

    def both(p, kind, r=0):
        names = ((kind, p, r, "+"), (kind, p, r, "-"))
        if kind == "own":
            peer = ring[first[p]]
            pairs = (kv.at[p, 0, 0], kv.at[p, 0, 3]), (kv.at[p, 0, 0], kv.at[p, 0, 1])
        elif kind == "relay":
            peer = ring[first[p]]
            pairs = (
                (kv.at[p, 0, 3, low], kv.at[p, 0, 2, low]),
                (kv.at[p, 0, 1, high], kv.at[p, 0, 2, high]),
            )
        elif kind == "far":
            peer = ring[second[p]]
            pairs = (kv.at[p, 0, r], kv.at[p, 3, r]), (kv.at[p, 0, r], kv.at[p, 1, r])
        else:
            peer = ring[second[p]]
            pairs = (
                (kv.at[p, 3, r, low], kv.at[p, 2, r, low]),
                (kv.at[p, 1, r, high], kv.at[p, 2, r, high]),
            )
        for name, (src, dst), to in zip(names, pairs, peer):
            ex.start(name, src, dst, to)

    def got(p, kind, r=0):
        ex.arrived((kind, p, r, "+"), (kind, p, r, "-"))

    for p in range(2):
        both(p, "own")
    for p in range(2):
        both(p, "far", 0)
    ex.start("meta+", meta.at[0], meta.at[3], ring["z"][0])
    ex.start("meta-", meta.at[0], meta.at[1], ring["z"][1])
    ex.start("meta2", meta.at[0], meta.at[2], across)

    phase("qturn")
    loads["q"].wait()
    for h in range(HEADS):
        raw = q_raw[:, h * 128 : (h + 1) * 128].astype(F32)
        qt[h // 4, (h % 4) * 128 : (h % 4 + 1) * 128, :] = turn(raw, qg_ref[...], cos, sin)

    phase("own")
    for p in range(2):
        got(p, "own")
        both(p, "relay")
    for r in (3, 1):
        for p in range(2):
            both(p, "far", r)

    phase("tables")
    eye = iota((128, 128), 0) == iota((128, 128), 1)
    earlier = (iota((128, 128), 0) < iota((128, 128), 1)).astype(F32)

    def lay(column):
        return jnp.sum(jnp.where(eye, column, 0.0), axis=0, keepdims=True)

    def stand(row):
        return jnp.sum(jnp.where(eye, row, 0.0), axis=1, keepdims=True)

    def counted(members):
        return jnp.dot(members, earlier, preferred_element_type=F32)

    relative = ((meta[0, 0:1, :].astype(jnp.int32) >> 5) - z + 4) & 3
    members = (iota((8, 128), 0) == relative).astype(F32)
    rank = jnp.sum(members * counted(members), axis=0, keepdims=True)
    target = relative.astype(F32) * 32.0 + rank
    pack = (iota((128, 128), 0).astype(F32) == target).astype(BF16)
    home[...] = (iota((128, 128), 1).astype(F32) == stand(target)).astype(BF16)

    phase("relay")
    for p in range(2):
        got(p, "relay")
        both(p, "far", 2)
    for p in range(2):
        got(p, "far", 0)
        both(p, "last", 0)

    phase("tables2")
    ex.arrived("meta+", "meta-", "meta2")
    stacks = [[], [], [], []]
    for r in range(4):
        inside = (meta[r, 0:1, :].astype(jnp.int32) >> 5) == z
        members = jnp.broadcast_to(inside.astype(F32), (8, 128))
        places = jnp.where(inside, counted(members)[0:1], -1.0)
        taken = iota((32, 128), 0).astype(F32) == places
        for which in range(4):
            stacks[which].append(
                jnp.sum(
                    jnp.where(taken, meta[r, which : which + 1, :], 0.0), axis=1, keepdims=True
                )
            )
    expert1, expert2, group_share, first_share = [jnp.concatenate(s, axis=0) for s in stacks]

    def relative_expert(column):
        e = lay(column).astype(jnp.int32) & 31
        return (
            ((((e >> 3) - x + 4) & 3) << 3)
            + (((((e >> 1) & 3) - y + 4) & 3) << 1)
            + ((e & 1) ^ c)
        )

    rel1, rel2 = relative_expert(expert1), relative_expert(expert2)
    named1 = (iota((32, 128), 0) == rel1).astype(F32)
    named2 = (iota((32, 128), 0) == rel2).astype(F32)
    ahead = counted(named1 + named2)
    slot1 = rel1.astype(F32) * 16.0 + jnp.sum(named1 * ahead, axis=0, keepdims=True)
    slot2 = rel2.astype(F32) * 16.0 + jnp.sum(named2 * ahead, axis=0, keepdims=True)
    places = iota((512, 128), 0).astype(F32)
    spread[...] = ((places == slot1) | (places == slot2)).astype(BF16)
    places = iota((128, 512), 1).astype(F32)
    pick1[...] = (places == stand(slot1)).astype(BF16)
    pick2[...] = (places == stand(slot2)).astype(BF16)
    weight1 = group_share * first_share
    weight2 = group_share * (1.0 - first_share)

    scale = float(np.log2(np.e) / np.sqrt(HEAD_DIM))

    def attend(r, opening):
        def one(g, carry):
            p, h = g // 2, g % 2
            keys = kv[p, r, :, :, pl.ds(pl.multiple_of(h * 128, 128), 128)].reshape(512, 128)
            values = kv[p, r, :, :, pl.ds(pl.multiple_of(256 + h * 128, 128), 128)].reshape(
                512, 128
            )
            scores = lax.dot_general(
                keys, qt[g], (((1,), (1,)), ((), ())), preferred_element_type=F32
            )
            peak = jnp.max(scores, axis=0, keepdims=True)
            if not opening:
                before = top[g]
                peak = jnp.maximum(peak, before)
            weights = jnp.exp2((scores - peak) * scale)
            summed = jnp.sum(weights, axis=0, keepdims=True)
            out = lax.dot_general(
                values, weights.astype(BF16), (((0,), (0,)), ((), ())),
                preferred_element_type=F32,
            )
            if not opening:
                shrink = jnp.exp2((before - peak) * scale)
                summed += total[g] * shrink
                out += acc[g] * shrink
            top[g] = peak
            total[g] = summed
            acc[g] = out
            return carry

        lax.fori_loop(0, KV_HEADS, one, 0)

    phase("att0")
    attend(0, True)
    phase("far31")
    for r in (3, 1):
        for p in range(2):
            got(p, "far", r)
            both(p, "last", r)
    phase("far2")
    for p in range(2):
        got(p, "far", 2)
        both(p, "last", 2)
    phase("att3")
    attend(3, False)
    phase("att1")
    attend(1, False)
    phase("last")
    for r in (0, 3, 1, 2):
        for p in range(2):
            got(p, "last", r)
    phase("att2")
    attend(2, False)

    phase("div")
    for g in range(KV_HEADS):
        scaled = acc[g] / total[g]
        for h in range(4):
            head = g * 4 + h
            att[:, head * 128 : (head + 1) * 128] = (
                scaled[:, h * 128 : (h + 1) * 128].T.astype(BF16)
            )
    loads["res"].wait()
    loads["w"].wait()
    phase("proj")

    def project(n, carry):
        cols = pl.ds(pl.multiple_of(n * 512, 512), 512)
        mixed[:, cols] = jnp.dot(att[...], w[:, cols], preferred_element_type=F32).astype(BF16)
        return carry

    lax.fori_loop(0, 4, project, 0)
    phase("norm")

    def norm(n, carry):
        at_rows = pl.ds(pl.multiple_of(n * 32, 32), 32)
        m = mixed[at_rows, :].astype(F32)
        m = m * lax.rsqrt(jnp.mean(m * m, axis=-1, keepdims=True) + EPSILON) * postg_ref[...]
        stream = (res[at_rows, :].astype(F32) + m).astype(BF16)
        res[at_rows, :] = stream
        s = stream.astype(F32)
        s = s * lax.rsqrt(jnp.mean(s * s, axis=-1, keepdims=True) + EPSILON) * preg_ref[...]
        normed[at_rows, :] = s.astype(BF16)
        return carry

    lax.fori_loop(0, 4, norm, 0)

    span = width // ROUNDS
    step = span // 2

    def span_of(i):
        return pl.ds(i * span, span)

    def z_parts(tag, i, src, dst, relay):
        cols = span_of(i)
        top_rows, low_rows = pl.ds(0, 16), pl.ds(16, 16)
        relays = relay.at[0, :, cols], relay.at[1, :, cols]
        opposite = src.at[2, top_rows, cols], src.at[2, low_rows, cols]
        finals = dst.at[2, top_rows, cols], dst.at[2, low_rows, cols]
        return cols, relays, opposite, finals

    def z_out(tag, i, src, dst, relay):
        cols, relays, opposite, _ = z_parts(tag, i, src, dst, relay)
        ex.start((tag, "z", "out+", i), opposite[0], relays[0], ring["z"][0])
        ex.start((tag, "z", "out-", i), opposite[1], relays[1], ring["z"][1])

    def z_direct(tag, i, src, dst):
        cols = span_of(i)
        ex.start((tag, "z", "+", i), src.at[1, :, cols], dst.at[3, :, cols], ring["z"][0])
        ex.start((tag, "z", "-", i), src.at[3, :, cols], dst.at[1, :, cols], ring["z"][1])

    def z_on(tag, i, src, dst, relay):
        _, relays, _, finals = z_parts(tag, i, src, dst, relay)
        for sign, relayed, final, to in zip("+-", relays, finals, ring["z"]):
            ex.arrived((tag, "z", "out" + sign, i))
            ex.start((tag, "z", "on" + sign, i), relayed, final, to)

    def z_in(tag, i):
        ex.arrived(*[(tag, "z", kind, i) for kind in ("+", "-", "on+", "on-")])

    def swap(tag, i, src, mid, dst, x_relay, y_relay):
        a, b = pl.ds(i * span, step), pl.ds(i * span + step, step)

        def block(ref, r, cols):
            return lambda ry, rc: ref.at[r, ry, rc, :, cols]

        def x_relays(cols):
            return x_relay.at[0, :, :, :, cols], x_relay.at[1, :, :, :, cols]

        def x_split(ref, cols):
            return ref.at[2, pl.ds(0, 2), :, :, cols], ref.at[2, pl.ds(2, 2), :, :, cols]

        def x_out(w, ref, cols):
            for sign, part, relayed, to in zip("+-", x_split(ref, cols), x_relays(cols), ring["x"]):
                ex.start((tag, w, "x", "out" + sign, i), part, relayed, to)

        def x_plus(w, ref, to, cols):
            ex.start(
                (tag, w, "x", "+", i), ref.at[1, :, :, :, cols], to.at[3, :, :, :, cols],
                ring["x"][0],
            )

        def x_minus(w, ref, to, cols):
            ex.start(
                (tag, w, "x", "-", i), ref.at[3, :, :, :, cols], to.at[1, :, :, :, cols],
                ring["x"][1],
            )

        def x_on(w, to_ref, cols):
            finals = x_split(to_ref, cols)
            for sign, relayed, final, to in zip("+-", x_relays(cols), finals, ring["x"]):
                ex.arrived((tag, w, "x", "out" + sign, i))
                ex.start((tag, w, "x", "on" + sign, i), relayed, final, to)

        def y_names(w, r, kinds):
            return [(tag, w, "y", r, kind, i) for kind in kinds]

        def y_relays(r, cols):
            return y_relay.at[0, r, :, cols], y_relay.at[1, r, :, cols]

        def y_out(w, r, ref, cols):
            part = block(ref, r, cols)
            names = y_names(w, r, ("out+", "out-"))
            for rc, relayed in enumerate(y_relays(r, cols)):
                ex.start(names[rc], part(2, rc), relayed, ring["y"][rc])

        def y_direct(w, r, ref, to_ref, cols):
            part, final = block(ref, r, cols), block(to_ref, r, cols)
            names = y_names(w, r, ("+", "-", "c+", "c-", "twin"))
            ex.start(names[0], part(1, 0), final(3, 0), ring["y"][0])
            ex.start(names[1], part(3, 0), final(1, 0), ring["y"][1])
            ex.start(names[2], part(1, 1), final(3, 1), ring["yc"][0])
            ex.start(names[3], part(3, 1), final(1, 1), ring["yc"][1])
            ex.start(names[4], part(0, 1), final(0, 1), twin)
            to_ref[r, 0, 0, :, cols] = ref[r, 0, 0, :, cols]

        def y_on(w, r, to_ref, cols):
            final = block(to_ref, r, cols)
            outs, ons = y_names(w, r, ("out+", "out-")), y_names(w, r, ("on+", "on-"))
            ex.arrived(outs[0])
            ex.start(ons[0], y_relays(r, cols)[0], final(2, 0), ring["y"][0])
            ex.arrived(outs[1])
            ex.start(ons[1], y_relays(r, cols)[1], final(2, 1), ring["yc"][1])

        def y_in(w, r):
            ex.arrived(*y_names(w, r, ("+", "-", "c+", "c-", "twin", "on+", "on-")))

        def landing(r):
            return dst if r == 0 else mid

        def origin(r):
            return src if r == 0 else mid

        x_out("a", src, a)
        y_out("b", 2, src, b)
        y_out("b", 3, src, b)
        y_out("b", 1, src, b)
        x_plus("a", src, mid, a)
        x_minus("a", src, mid, a)
        y_direct("b", 2, src, mid, b)
        y_direct("b", 3, src, mid, b)
        y_direct("b", 1, src, mid, b)
        y_out("a", 0, src, a)
        y_out("b", 0, src, b)
        yield
        y_on("b", 2, mid, b)
        y_on("b", 3, mid, b)
        y_on("b", 1, mid, b)
        y_direct("a", 0, src, dst, a)
        y_direct("b", 0, src, dst, b)
        x_on("a", mid, a)
        yield
        y_on("a", 0, dst, a)
        y_on("b", 0, dst, b)
        y_in("b", 2)
        x_out("b", mid, b)
        ex.arrived((tag, "a", "x", "+", i))
        y_out("a", 3, mid, a)
        y_direct("a", 3, mid, dst, a)
        ex.arrived((tag, "a", "x", "-", i))
        y_out("a", 1, mid, a)
        y_direct("a", 1, mid, dst, a)
        y_in("b", 3)
        x_minus("b", mid, dst, b)
        y_in("b", 1)
        x_plus("b", mid, dst, b)
        yield
        ex.arrived((tag, "a", "x", "on+", i), (tag, "a", "x", "on-", i))
        y_out("a", 2, mid, a)
        y_direct("a", 2, mid, dst, a)
        y_on("a", 3, dst, a)
        y_on("a", 1, dst, a)
        x_on("b", dst, b)
        yield
        y_on("a", 2, dst, a)
        yield
        for r in range(4):
            y_in("a", r)
        y_in("b", 0)
        ex.arrived(*[(tag, "b", "x", kind, i) for kind in ("+", "-", "on+", "on-")])

    def run(steps, count):
        for _ in range(count):
            next(steps, None)

    phase("pack")
    for i in range(ROUNDS):
        cols = span_of(i)
        packed = jnp.dot(pack, normed[:, cols], preferred_element_type=F32).astype(BF16)
        zs[:, :, cols] = packed.reshape(4, 32, span)
        rows[0, :, cols] = packed[0:32]
        z_out("d", i, zs, rows, zrel)
        if i == 0:
            z_direct("d", 0, zs, rows)

    def slots(i):
        cols = span_of(i)
        z_in("d", i)
        phase("slots%d" % i)
        spaced = jnp.dot(
            spread[...], rows[:, :, cols].reshape(128, span), preferred_element_type=F32
        )
        xs[:, :, :, :, cols] = spaced.astype(BF16).reshape(4, 4, 2, 16, span)

    def lift(i):
        cols = span_of(i)
        arrived = yr[:, :, :, :, cols].reshape(512, span)
        for sums, weight in ((gates, gate), (lifts, up)):
            product = jnp.dot(arrived, weight[cols, :], preferred_element_type=F32)
            sums[...] = product if i == 0 else sums[...] + product

    def lower(i):
        cols = span_of(i)
        produced = jnp.dot(hidden[...], down[:, cols], preferred_element_type=F32)
        made[:, :, :, :, cols] = produced.astype(BF16).reshape(4, 4, 2, 16, span)

    def combine(i):
        cols = span_of(i)
        returned = ret[:, :, :, :, cols].reshape(512, span)
        one = jnp.dot(pick1[...], returned, preferred_element_type=F32)
        two = jnp.dot(pick2[...], returned, preferred_element_type=F32)
        summed = (weight1 * one + weight2 * two).astype(BF16)
        comb[:, :, cols] = summed.reshape(4, 32, span)
        zret[0, :, cols] = summed[0:32]
        z_out("r", i, comb, zret, zretrel)
        z_direct("r", i, comb, zret)

    there = [swap("d", i, xs, xr, yr, xrel, yrel) for i in range(ROUNDS)]
    phase("zon0")
    z_on("d", 0, zs, rows, zrel)
    z_direct("d", 1, zs, rows)
    phase("zin0")
    slots(0)
    phase("d0_start")
    run(there[0], 1)
    phase("d0_b")
    run(there[0], 1)
    phase("zon1")
    z_on("d", 1, zs, rows, zrel)
    phase("d0_c")
    run(there[0], 1)
    phase("zin1")
    slots(1)
    phase("d0_d")
    run(there[0], 1)
    phase("d1_start")
    run(there[1], 1)
    phase("d0_e")
    run(there[0], 1)
    phase("d1_b")
    run(there[1], 1)
    phase("d0_in")
    run(there[0], 1)
    phase("lift0")
    loads["gate"].wait()
    loads["up"].wait()
    lift(0)
    for n in "cdef":
        phase("d1_" + n)
        run(there[1], 1)
    phase("lift1")
    lift(1)
    phase("silu")
    g = gates[...]
    hidden[...] = (g / (1.0 + jnp.exp(-g)) * lifts[...]).astype(BF16)
    loads["down"].wait()

    home_way = [swap("r", i, made, back, ret, retrel, backrel) for i in range(ROUNDS)]
    phase("lower0")
    lower(0)
    phase("r0_start")
    run(home_way[0], 1)
    phase("lower1")
    lower(1)
    for n in "bcd":
        phase("r0_" + n)
        run(home_way[0], 1)
    phase("r1_start")
    run(home_way[1], 1)
    phase("r0_e")
    run(home_way[0], 1)
    phase("r1_b")
    run(home_way[1], 1)
    phase("r0_in")
    run(home_way[0], 1)
    phase("combine0")
    combine(0)
    for n in "cd":
        phase("r1_" + n)
        run(home_way[1], 1)
    phase("zon0r")
    z_on("r", 0, comb, zret, zretrel)
    for n in "ef":
        phase("r1_" + n)
        run(home_way[1], 1)
    phase("combine1")
    combine(1)

    def arrive(i):
        cols = span_of(i)
        z_in("r", i)
        added = jnp.dot(
            home[...], zret[:, :, cols].reshape(128, span), preferred_element_type=F32
        )
        out_ref[:, cols] = (res[:, cols].astype(F32) + added).astype(BF16)

    phase("out0")
    arrive(0)
    phase("zon1r")
    z_on("r", 1, comb, zret, zretrel)
    phase("out1")
    arrive(1)
    phase("sent")
    ex.finish()
    phase()


def layer(
    q, k, v, w, res, gate, up, down, query_gain, key_gain, post_gain, pre_gain, ids, gw, fs
):
    hbm = pl.BlockSpec(memory_space=pl.ANY)
    vmem = pl.BlockSpec(memory_space=pltpu.VMEM)
    tokens, width = q.shape
    _, _, ff = gate.shape
    slots = pltpu.VMEM((4, 4, 2, 16, width), BF16)
    x_relay = pltpu.VMEM((2, 2, 2, 16, width), BF16)
    y_relay = pltpu.VMEM((2, 4, 16, width), BF16)
    z_block = pltpu.VMEM((4, 32, width), BF16)
    z_relay = pltpu.VMEM((2, 16, width), BF16)
    rows = pltpu.VMEM((tokens, width), BF16)
    return pl.pallas_call(
        layer_kernel,
        out_shape=jax.ShapeDtypeStruct((tokens, width), BF16),
        in_specs=[hbm] * 8 + [vmem] * 8,
        out_specs=vmem,
        scratch_shapes=[
            pltpu.VMEM((2, 4, 4, 128, 512), BF16),
            pltpu.VMEM((4, 512, 128), BF16),
            rows,
            pltpu.VMEM((tokens, 512), BF16),
            pltpu.VMEM((tokens, 512), BF16),
            pltpu.VMEM((width, width), BF16),
            rows,
            pltpu.VMEM((4, 1, 512), F32),
            pltpu.VMEM((4, 1, 512), F32),
            pltpu.VMEM((4, 128, 512), F32),
            rows,
            rows,
            rows,
            pltpu.VMEM((width, ff), BF16),
            pltpu.VMEM((width, ff), BF16),
            pltpu.VMEM((ff, width), BF16),
            pltpu.VMEM((4, 8, 128), F32),
            z_block, z_block, z_relay,
            slots, slots, x_relay, slots, y_relay,
            pltpu.VMEM((512, ff), F32),
            pltpu.VMEM((512, ff), F32),
            pltpu.VMEM((512, ff), BF16),
            slots, slots, y_relay, slots, x_relay,
            z_block, z_block, z_relay,
            pltpu.VMEM((512, 128), BF16),
            pltpu.VMEM((128, 512), BF16),
            pltpu.VMEM((128, 512), BF16),
            pltpu.VMEM((128, 128), BF16),
            pltpu.SemaphoreType.DMA((8,)),
            pltpu.SemaphoreType.DMA((COPIES,)),
            pltpu.SemaphoreType.DMA((COPIES,)),
        ],
        compiler_params=pltpu.CompilerParams(
            collective_id=0, has_side_effects=True, vmem_limit_bytes=62 * 1024 * 1024
        ),
        name="layer",
    )(
        q, k, v, w, res, gate, up, down, jnp.asarray(angle_tables()), query_gain.reshape(1, -1),
        key_gain.reshape(1, -1), post_gain.reshape(1, -1), pre_gain.reshape(1, -1), ids, gw, fs,
    )


def local(
    residual_in,
    query_proj,
    key_proj,
    value_proj,
    query_gain,
    key_gain,
    out_weight,
    post_gain,
    pre_gain,
    route_ids,
    group_weight,
    first_share,
    gate_weight,
    up_weight,
    down_weight,
):
    out = layer(
        query_proj[0], key_proj[0], value_proj[0], out_weight, residual_in[0],
        gate_weight, up_weight, down_weight, query_gain, key_gain, post_gain, pre_gain,
        route_ids[0].T, group_weight, first_share,
    )
    return out[None]


def solution(mesh):
    placed = (
        P("dp", "sp", None),
        P("dp", "sp", None),
        P("dp", "sp", None),
        P("dp", "sp", None),
        P(),
        P(),
        P(),
        P(),
        P(),
        P("dp", "sp", None),
        P("dp", "sp"),
        P("dp", "sp"),
        P(("sp", "dp"), None, None),
        P(("sp", "dp"), None, None),
        P(("sp", "dp"), None, None),
    )
    return jax.shard_map(
        local, mesh=mesh, in_specs=placed, out_specs=P("dp", "sp", None), check_vma=False
    )
```

```python
import jax
import jax.numpy as jnp
import numpy as np
from jax import lax
from jax.experimental import pallas as pl
from jax.experimental.pallas import tpu as pltpu
from jax.sharding import PartitionSpec as P

HEADS = 16
KV_HEADS = 4
HEAD_DIM = 128
GRID_W = 64
RING = 4
EPSILON = 1e-06
MESH = pl.DeviceIdType.MESH


class Phase:
    def __init__(self):
        self.scope = None

    def __call__(self, name=None):
        if self.scope is not None:
            self.scope.__exit__(None, None, None)
        self.scope = None
        if name is not None:
            self.scope = jax.named_scope(name)
            self.scope.__enter__()


F32 = jnp.float32
BF16 = jnp.bfloat16


def angle_tables():
    quarter = HEAD_DIM // 4
    inverse = (np.float32(10000.0) ** (-np.arange(quarter, dtype=np.float32) / quarter)).astype(
        np.float32
    )
    places = np.concatenate([np.arange(32), np.arange(GRID_W)]).astype(np.float32)
    angles = places[:, None] * np.tile(inverse, 4)[None, :]
    return np.stack([np.cos(angles), np.sin(angles)]).astype(np.float32)


def position():
    s = lax.axis_index("sp")
    d = lax.axis_index("dp")
    return s // RING, s % RING, d // 2, d % 2


def at(z, x, y, c):
    return (
        ((z + 2 * RING) % RING) * RING + (x + 2 * RING) % RING,
        ((y + 2 * RING) % RING) * 2 + c,
    )


def turn(heads, gain, cos, sin):
    normed = (
        heads * lax.rsqrt(jnp.mean(heads * heads, axis=-1, keepdims=True) + EPSILON) * gain
    )
    lane = lax.broadcasted_iota(jnp.int32, normed.shape, 1)
    turned = jnp.where(
        (lane // 32) % 2 == 0, -pltpu.roll(normed, 96, 1), pltpu.roll(normed, 32, 1)
    )
    return (normed * cos + turned * sin).astype(BF16)


class Exchange:
    def __init__(self, send_sem, recv_sem):
        self.send_sem, self.recv_sem, self.copies = send_sem, recv_sem, {}
        self.unsent = []

    def start(self, name, src, dst, peer):
        i = len(self.copies)
        copy = pltpu.make_async_remote_copy(
            src_ref=src,
            dst_ref=dst,
            send_sem=self.send_sem.at[i],
            recv_sem=self.recv_sem.at[i],
            device_id=peer,
            device_id_type=MESH,
        )
        assert name not in self.copies
        self.copies[name] = copy
        self.unsent.append(copy)
        copy.start()

    def arrived(self, *names):
        for name in names:
            self.copies[name].wait_recv()

    def settle(self, count):
        done = len(self.copies) - len(self.unsent)
        for copy in self.unsent[: count - done]:
            copy.wait_send()
        self.unsent = self.unsent[count - done :]


ROUNDS = 2
COPIES = 40 + 3 + ROUNDS * 2 * (62 + 3)


def iota(shape, dim):
    return lax.broadcasted_iota(jnp.int32, shape, dim)


def layer_kernel(
    q_hbm, k_hbm, v_hbm, w_hbm, res_hbm, gate_hbm, up_hbm, down_hbm,
    table_ref, qg_ref, kg_ref, postg_ref, preg_ref, ids_ref, gw_ref, fs_ref,
    out_ref,
    kv, qt, q_raw, k_raw, v_raw, w, res, top, total, acc, att, mixed, normed,
    gate, up, down, meta,
    zs, rows, xs, xr, yr, gates, lifts, hidden, made, back, ret, comb, zret,
    spread, pick1, pick2, home,
    local_sem, send_sem, recv_sem,
):
    z, x, y, c = position()
    width = q_raw.shape[1]
    phase = Phase()
    phase("turn")
    loads = {}
    for i, (name, src, dst) in enumerate(
        [
            ("k", k_hbm, k_raw), ("v", v_hbm, v_raw), ("q", q_hbm, q_raw), ("res", res_hbm, res),
            ("w", w_hbm, w), ("gate", gate_hbm.at[0], gate), ("up", up_hbm.at[0], up),
            ("down", down_hbm.at[0], down),
        ]
    ):
        loads[name] = pltpu.make_async_copy(src, dst, local_sem.at[i])
        loads[name].start()

    to_z = {s: at(z + s, x, y, c) for s in (1, 2, 3)}
    to_x = {s: at(z, x + s, y, c) for s in (1, 2, 3)}
    to_y = {(s, o): at(z, x, y + s, c if o == 0 else 1 - c) for s in range(4) for o in (0, 1)}
    del to_y[0, 0]
    ring = {"z": (to_z[1], to_z[3]), "x": (to_x[1], to_x[3])}
    barrier = pltpu.get_barrier_semaphore()
    peers = [*to_z.values(), *to_x.values(), *to_y.values()]
    for peer in peers:
        pl.semaphore_signal(barrier, inc=1, device_id=peer, device_id_type=MESH)
    ex = Exchange(send_sem, recv_sem)

    lane = iota((GRID_W, HEAD_DIM), 1)

    def table(which):
        halves = []
        for part in range(2):
            row = table_ref[which, pl.ds(2 * (z * RING + x) + part, 1), :]
            halves.append(jnp.where(lane < 64, row, table_ref[which, 32 : 32 + GRID_W, :]))
        return jnp.concatenate(halves, axis=0)

    cos, sin = table(0), table(1)
    meta[0, 0:2, :] = ids_ref[...].astype(F32)
    meta[0, 2:3, :] = gw_ref[...]
    meta[0, 3:4, :] = fs_ref[...]
    meta[0, 4:8, :] = jnp.zeros((4, 128), F32)
    loads["k"].wait()
    for h in range(KV_HEADS):
        raw = k_raw[:, h * 128 : (h + 1) * 128].astype(F32)
        kv[h // 2, 0, 0, :, (h % 2) * 128 : (h % 2 + 1) * 128] = turn(raw, kg_ref[...], cos, sin)
    loads["v"].wait()
    for half in range(2):
        kv[half, 0, 0, :, 256:512] = v_raw[:, half * 256 : (half + 1) * 256]
    phase("barrier")
    pl.semaphore_wait(barrier, len(peers))

    phase("start")
    first = ("x", "z")
    second = ("z", "x")
    low, high = pl.ds(0, 64), pl.ds(64, 64)

    def both(p, kind, r=0):
        names = ((kind, p, r, "+"), (kind, p, r, "-"))
        if kind == "own":
            peer = ring[first[p]]
            pairs = (kv.at[p, 0, 0], kv.at[p, 0, 3]), (kv.at[p, 0, 0], kv.at[p, 0, 1])
        elif kind == "relay":
            peer = ring[first[p]]
            pairs = (
                (kv.at[p, 0, 3, low], kv.at[p, 0, 2, low]),
                (kv.at[p, 0, 1, high], kv.at[p, 0, 2, high]),
            )
        elif kind == "far":
            peer = ring[second[p]]
            pairs = (kv.at[p, 0, r], kv.at[p, 3, r]), (kv.at[p, 0, r], kv.at[p, 1, r])
        else:
            peer = ring[second[p]]
            pairs = (
                (kv.at[p, 3, r, low], kv.at[p, 2, r, low]),
                (kv.at[p, 1, r, high], kv.at[p, 2, r, high]),
            )
        for name, (src, dst), to in zip(names, pairs, peer):
            ex.start(name, src, dst, to)

    def got(p, kind, r=0):
        ex.arrived((kind, p, r, "+"), (kind, p, r, "-"))

    for p in range(2):
        both(p, "own")
    for p in range(2):
        both(p, "far", 0)
    ex.start("meta+", meta.at[0], meta.at[3], ring["z"][0])
    ex.start("meta-", meta.at[0], meta.at[1], ring["z"][1])
    ex.start("meta2", meta.at[0], meta.at[2], to_z[2])

    phase("qturn")
    loads["q"].wait()
    for h in range(HEADS):
        raw = q_raw[:, h * 128 : (h + 1) * 128].astype(F32)
        qt[h // 4, (h % 4) * 128 : (h % 4 + 1) * 128, :] = turn(raw, qg_ref[...], cos, sin)

    phase("own")
    for p in range(2):
        got(p, "own")
        both(p, "relay")
    for r in (3, 1):
        for p in range(2):
            both(p, "far", r)

    phase("tables")
    eye = iota((128, 128), 0) == iota((128, 128), 1)
    earlier = (iota((128, 128), 0) < iota((128, 128), 1)).astype(F32)

    def lay(column):
        return jnp.sum(jnp.where(eye, column, 0.0), axis=0, keepdims=True)

    def stand(row):
        return jnp.sum(jnp.where(eye, row, 0.0), axis=1, keepdims=True)

    def counted(members):
        return jnp.dot(members, earlier, preferred_element_type=F32)

    relative = ((meta[0, 0:1, :].astype(jnp.int32) >> 5) - z + 4) & 3
    members = (iota((8, 128), 0) == relative).astype(F32)
    rank = jnp.sum(members * counted(members), axis=0, keepdims=True)
    target = relative.astype(F32) * 32.0 + rank
    pack = (iota((128, 128), 0).astype(F32) == target).astype(BF16)
    home[...] = (iota((128, 128), 1).astype(F32) == stand(target)).astype(BF16)

    phase("relay")
    for p in range(2):
        got(p, "relay")
        both(p, "far", 2)
    for p in range(2):
        got(p, "far", 0)
        both(p, "last", 0)

    phase("tables2")
    ex.arrived("meta+", "meta-", "meta2")
    stacks = [[], [], [], []]
    for r in range(4):
        inside = (meta[r, 0:1, :].astype(jnp.int32) >> 5) == z
        members = jnp.broadcast_to(inside.astype(F32), (8, 128))
        places = jnp.where(inside, counted(members)[0:1], -1.0)
        taken = iota((32, 128), 0).astype(F32) == places
        for which in range(4):
            stacks[which].append(
                jnp.sum(
                    jnp.where(taken, meta[r, which : which + 1, :], 0.0), axis=1, keepdims=True
                )
            )
    expert1, expert2, group_share, first_share = [jnp.concatenate(s, axis=0) for s in stacks]

    def relative_expert(column):
        e = lay(column).astype(jnp.int32) & 31
        return (
            ((((e >> 3) - x + 4) & 3) << 3)
            + (((((e >> 1) & 3) - y + 4) & 3) << 1)
            + ((e & 1) ^ c)
        )

    rel1, rel2 = relative_expert(expert1), relative_expert(expert2)
    named1 = (iota((32, 128), 0) == rel1).astype(F32)
    named2 = (iota((32, 128), 0) == rel2).astype(F32)
    ahead = counted(named1 + named2)
    slot1 = rel1.astype(F32) * 16.0 + jnp.sum(named1 * ahead, axis=0, keepdims=True)
    slot2 = rel2.astype(F32) * 16.0 + jnp.sum(named2 * ahead, axis=0, keepdims=True)
    places = iota((512, 128), 0).astype(F32)
    spread[...] = ((places == slot1) | (places == slot2)).astype(BF16)
    places = iota((128, 512), 1).astype(F32)
    pick1[...] = (places == stand(slot1)).astype(BF16)
    pick2[...] = (places == stand(slot2)).astype(BF16)
    weight1 = group_share * first_share
    weight2 = group_share * (1.0 - first_share)

    scale = float(np.log2(np.e) / np.sqrt(HEAD_DIM))

    def attend(blocks, opening=False):
        def one(g, carry):
            p, h = g // 2, g % 2

            def part(offset):
                cols = pl.ds(pl.multiple_of(offset + h * 128, 128), 128)
                return jnp.concatenate([kv[p, a, b, :, cols] for a, b in blocks], axis=0)

            keys, values = part(0), part(256)
            scores = lax.dot_general(
                keys, qt[g], (((1,), (1,)), ((), ())), preferred_element_type=F32
            )
            peak = jnp.max(scores, axis=0, keepdims=True)
            if not opening:
                before = top[g]
                peak = jnp.maximum(peak, before)
            weights = jnp.exp2((scores - peak) * scale)
            summed = jnp.sum(weights, axis=0, keepdims=True)
            out = lax.dot_general(
                values, weights.astype(BF16), (((0,), (0,)), ((), ())),
                preferred_element_type=F32,
            )
            if not opening:
                shrink = jnp.exp2((before - peak) * scale)
                summed += total[g] * shrink
                out += acc[g] * shrink
            top[g] = peak
            total[g] = summed
            acc[g] = out
            return carry

        lax.fori_loop(0, KV_HEADS, one, 0, unroll=2)

    phase("att0")
    attend([(0, 0), (0, 1), (0, 2), (0, 3)], opening=True)

    def step_on(r, kind):
        for p in range(2):
            got(p, kind, r)
            if kind == "far":
                both(p, "last", r)

    phase("far3")
    step_on(3, "far")
    phase("att1")
    attend([(3, 0), (3, 3), (1, 0), (1, 3)])
    phase("far1")
    step_on(1, "far")
    phase("far2")
    step_on(2, "far")
    phase("att2")
    attend([(3, 1), (1, 1), (3, 2), (1, 2)])
    phase("last03")
    step_on(0, "last")
    step_on(3, "last")
    phase("att3")
    attend([(2, 0), (2, 3)])
    phase("last12")
    step_on(1, "last")
    step_on(2, "last")
    phase("att4")
    attend([(2, 1), (2, 2)])

    phase("div")
    for g in range(KV_HEADS):
        scaled = acc[g] / total[g]
        for h in range(4):
            head = g * 4 + h
            att[:, head * 128 : (head + 1) * 128] = (
                scaled[:, h * 128 : (h + 1) * 128].T.astype(BF16)
            )
    loads["res"].wait()
    loads["w"].wait()
    phase("proj")

    def project(n, carry):
        cols = pl.ds(pl.multiple_of(n * 512, 512), 512)
        mixed[:, cols] = jnp.dot(att[...], w[:, cols], preferred_element_type=F32).astype(BF16)
        return carry

    lax.fori_loop(0, 4, project, 0, unroll=2)
    phase("norm")

    def norm(n, carry):
        at_rows = pl.ds(pl.multiple_of(n * 32, 32), 32)
        m = mixed[at_rows, :].astype(F32)
        m = m * lax.rsqrt(jnp.mean(m * m, axis=-1, keepdims=True) + EPSILON) * postg_ref[...]
        stream = (res[at_rows, :].astype(F32) + m).astype(BF16)
        res[at_rows, :] = stream
        s = stream.astype(F32)
        s = s * lax.rsqrt(jnp.mean(s * s, axis=-1, keepdims=True) + EPSILON) * preg_ref[...]
        normed[at_rows, :] = s.astype(BF16)
        return carry

    lax.fori_loop(0, 4, norm, 0)

    span = width // ROUNDS
    step = span // 2

    def span_of(i):
        return pl.ds(i * span, span)

    def z_out(tag, i, src, dst):
        cols = span_of(i)
        for r in (2, 1, 3):
            ex.start((tag, "z", r, i), src.at[r, :, cols], dst.at[4 - r, :, cols], to_z[r])

    def z_in(tag, i):
        ex.arrived(*[(tag, "z", r, i) for r in (2, 1, 3)])

    def swap(tag, i, src, mid, dst):
        a, b = pl.ds(i * span, step), pl.ds(i * span + step, step)

        def x_out(w, r, ref, to_ref, cols):
            ex.start(
                (tag, w, "x", r, i), ref.at[r, :, :, :, cols], to_ref.at[4 - r, :, :, :, cols],
                to_x[r],
            )

        def x_in(w, r):
            ex.arrived((tag, w, "x", 4 - r, i))

        sides = [(2, 0), (2, 1), (1, 0), (3, 0), (1, 1), (3, 1), (0, 1)]

        def y_out(w, r, ref, to_ref, cols):
            for ry, rc in sides:
                ex.start(
                    (tag, w, "y", r, ry, rc, i), ref.at[r, ry, rc, :, cols],
                    to_ref.at[r, (4 - ry) % 4, rc, :, cols], to_y[ry, rc],
                )
            to_ref[r, 0, 0, :, cols] = ref[r, 0, 0, :, cols]

        def y_in(w, r):
            ex.arrived(*[(tag, w, "y", r, ry, rc, i) for ry, rc in sides])

        for r in (2, 1, 3):
            x_out("a", r, src, mid, a)
        for r in (2, 3, 1):
            y_out("b", r, src, mid, b)
        y_out("a", 0, src, dst, a)
        y_out("b", 0, src, dst, b)
        yield
        y_in("b", 2)
        x_out("b", 2, mid, dst, b)
        y_in("b", 3)
        x_out("b", 3, mid, dst, b)
        x_in("a", 2)
        y_out("a", 2, mid, dst, a)
        y_in("b", 1)
        x_out("b", 1, mid, dst, b)
        x_in("a", 3)
        y_out("a", 3, mid, dst, a)
        x_in("a", 1)
        y_out("a", 1, mid, dst, a)
        yield
        y_in("a", 0)
        y_in("b", 0)
        y_in("a", 2)
        x_in("b", 2)
        yield
        y_in("a", 3)
        x_in("b", 3)
        yield
        y_in("a", 1)
        x_in("b", 1)

    def run(steps, count):
        for _ in range(count):
            next(steps, None)

    phase("pack")
    for i in range(ROUNDS):
        cols = span_of(i)
        packed = jnp.dot(pack, normed[:, cols], preferred_element_type=F32).astype(BF16)
        zs[:, :, cols] = packed.reshape(4, 32, span)
        rows[0, :, cols] = packed[0:32]
        z_out("d", i, zs, rows)

    def slots(i):
        cols = span_of(i)
        z_in("d", i)
        phase("slots%d" % i)
        spaced = jnp.dot(
            spread[...], rows[:, :, cols].reshape(128, span), preferred_element_type=F32
        )
        xs[:, :, :, :, cols] = spaced.astype(BF16).reshape(4, 4, 2, 16, span)

    def lift(i, at_r, count):
        cols, at_rows = span_of(i), pl.ds(at_r * 128, count * 128)
        arrived = yr[at_r : at_r + count, :, :, :, cols].reshape(count * 128, span)
        for sums, weight in ((gates, gate), (lifts, up)):
            product = jnp.dot(arrived, weight[cols, :], preferred_element_type=F32)
            sums[at_rows, :] = product if i == 0 else sums[at_rows, :] + product

    def lower(i):
        cols = span_of(i)
        produced = jnp.dot(hidden[...], down[:, cols], preferred_element_type=F32)
        made[:, :, :, :, cols] = produced.astype(BF16).reshape(4, 4, 2, 16, span)

    def combine(i):
        cols = span_of(i)
        returned = ret[:, :, :, :, cols].reshape(512, span)
        one = jnp.dot(pick1[...], returned, preferred_element_type=F32)
        two = jnp.dot(pick2[...], returned, preferred_element_type=F32)
        summed = (weight1 * one + weight2 * two).astype(BF16)
        comb[:, :, cols] = summed.reshape(4, 32, span)
        zret[0, :, cols] = summed[0:32]
        z_out("r", i, comb, zret)

    there = [swap("d", i, xs, xr, yr) for i in range(ROUNDS)]
    phase("zin0")
    slots(0)
    phase("d_start0")
    run(there[0], 1)
    ex.settle(43)
    loads["gate"].wait()
    loads["up"].wait()
    for i in range(ROUNDS):
        if i + 1 < ROUNDS:
            phase("zin%d" % (i + 1))
            slots(i + 1)
        phase("d_mid%d" % i)
        run(there[i], 1)
        if i + 1 < ROUNDS:
            phase("d_start%d" % (i + 1))
            run(there[i + 1], 1)
            phase("d_in%d" % i)
            run(there[i], 3)
            phase("lift%d" % i)
            lift(i, 0, 4)
            continue
        ex.settle(43 + 3 * ROUNDS + 62 * i)
        phase("d_in%d" % i)
        run(there[i], 1)
        phase("lift%d" % i)
        lift(i, 0, 1)
        lift(i, 2, 1)
        phase("d_in%d" % i)
        run(there[i], 1)
        phase("lift%d" % i)
        lift(i, 3, 1)
        phase("d_in%d" % i)
        run(there[i], 1)
        phase("lift%d" % i)
        lift(i, 1, 1)
    phase("silu")
    g = gates[...]
    hidden[...] = (g / (1.0 + jnp.exp(-g)) * lifts[...]).astype(BF16)
    loads["down"].wait()

    home_way = [swap("r", i, made, back, ret) for i in range(ROUNDS)]
    phase("lower0")
    lower(0)
    phase("r_start0")
    run(home_way[0], 1)
    for i in range(ROUNDS):
        if i + 1 < ROUNDS:
            phase("lower%d" % (i + 1))
            lower(i + 1)
        phase("r_mid%d" % i)
        run(home_way[i], 1)
        if i + 1 < ROUNDS:
            phase("r_start%d" % (i + 1))
            run(home_way[i + 1], 1)
        ex.settle(43 + 3 * ROUNDS + 62 * ROUNDS)
        phase("r_in%d" % i)
        run(home_way[i], 3)
        if i + 1 == ROUNDS:
            ex.settle(len(ex.copies) - 31)
        phase("combine%d" % i)
        combine(i)

    def arrive(i):
        cols = span_of(i)
        z_in("r", i)
        added = jnp.dot(
            home[...], zret[:, :, cols].reshape(128, span), preferred_element_type=F32
        )
        out_ref[:, cols] = (res[:, cols].astype(F32) + added).astype(BF16)

    for i in range(ROUNDS):
        phase("out%d" % i)
        arrive(i)
    phase("sent")
    ex.settle(COPIES)
    phase()


def layer(
    q, k, v, w, res, gate, up, down, query_gain, key_gain, post_gain, pre_gain, ids, gw, fs
):
    hbm = pl.BlockSpec(memory_space=pl.ANY)
    vmem = pl.BlockSpec(memory_space=pltpu.VMEM)
    tokens, width = q.shape
    _, _, ff = gate.shape
    slots = pltpu.VMEM((4, 4, 2, 16, width), BF16)
    z_block = pltpu.VMEM((4, 32, width), BF16)
    rows = pltpu.VMEM((tokens, width), BF16)
    return pl.pallas_call(
        layer_kernel,
        out_shape=jax.ShapeDtypeStruct((tokens, width), BF16),
        in_specs=[hbm] * 8 + [vmem] * 8,
        out_specs=vmem,
        scratch_shapes=[
            pltpu.VMEM((2, 4, 4, 128, 512), BF16),
            pltpu.VMEM((4, 512, 128), BF16),
            rows,
            pltpu.VMEM((tokens, 512), BF16),
            pltpu.VMEM((tokens, 512), BF16),
            pltpu.VMEM((width, width), BF16),
            rows,
            pltpu.VMEM((4, 1, 512), F32),
            pltpu.VMEM((4, 1, 512), F32),
            pltpu.VMEM((4, 128, 512), F32),
            rows,
            rows,
            rows,
            pltpu.VMEM((width, ff), BF16),
            pltpu.VMEM((width, ff), BF16),
            pltpu.VMEM((ff, width), BF16),
            pltpu.VMEM((4, 8, 128), F32),
            z_block, z_block, slots, slots, slots,
            pltpu.VMEM((512, ff), F32),
            pltpu.VMEM((512, ff), F32),
            pltpu.VMEM((512, ff), BF16),
            slots, slots, slots, z_block, z_block,
            pltpu.VMEM((512, 128), BF16),
            pltpu.VMEM((128, 512), BF16),
            pltpu.VMEM((128, 512), BF16),
            pltpu.VMEM((128, 128), BF16),
            pltpu.SemaphoreType.DMA((8,)),
            pltpu.SemaphoreType.DMA((COPIES,)),
            pltpu.SemaphoreType.DMA((COPIES,)),
        ],
        compiler_params=pltpu.CompilerParams(
            collective_id=0, has_side_effects=True, vmem_limit_bytes=62 * 1024 * 1024
        ),
        name="layer",
    )(
        q, k, v, w, res, gate, up, down, jnp.asarray(angle_tables()), query_gain.reshape(1, -1),
        key_gain.reshape(1, -1), post_gain.reshape(1, -1), pre_gain.reshape(1, -1), ids, gw, fs,
    )


def local(
    residual_in,
    query_proj,
    key_proj,
    value_proj,
    query_gain,
    key_gain,
    out_weight,
    post_gain,
    pre_gain,
    route_ids,
    group_weight,
    first_share,
    gate_weight,
    up_weight,
    down_weight,
):
    out = layer(
        query_proj[0], key_proj[0], value_proj[0], out_weight, residual_in[0],
        gate_weight, up_weight, down_weight, query_gain, key_gain, post_gain, pre_gain,
        route_ids[0].T, group_weight, first_share,
    )
    return out[None]


def solution(mesh):
    placed = (
        P("dp", "sp", None),
        P("dp", "sp", None),
        P("dp", "sp", None),
        P("dp", "sp", None),
        P(),
        P(),
        P(),
        P(),
        P(),
        P("dp", "sp", None),
        P("dp", "sp"),
        P("dp", "sp"),
        P(("sp", "dp"), None, None),
        P(("sp", "dp"), None, None),
        P(("sp", "dp"), None, None),
    )
    return jax.shard_map(
        local, mesh=mesh, in_specs=placed, out_specs=P("dp", "sp", None), check_vma=False
    )
```

```python
import jax
import jax.numpy as jnp
import numpy as np
from jax import lax
from jax.experimental import pallas as pl
from jax.experimental.pallas import tpu as pltpu
from jax.sharding import PartitionSpec as P

HEADS = 16
KV_HEADS = 4
HEAD_DIM = 128
GRID_W = 64
RING = 4
EPSILON = 1e-06
MESH = pl.DeviceIdType.MESH


class Phase:
    def __init__(self):
        self.scope = None

    def __call__(self, name=None):
        if self.scope is not None:
            self.scope.__exit__(None, None, None)
        self.scope = None
        if name is not None:
            self.scope = jax.named_scope(name)
            self.scope.__enter__()


F32 = jnp.float32
BF16 = jnp.bfloat16


def angle_tables():
    quarter = HEAD_DIM // 4
    inverse = (np.float32(10000.0) ** (-np.arange(quarter, dtype=np.float32) / quarter)).astype(
        np.float32
    )
    places = np.concatenate([np.arange(32), np.arange(GRID_W)]).astype(np.float32)
    angles = places[:, None] * np.tile(inverse, 4)[None, :]
    return np.stack([np.cos(angles), np.sin(angles)]).astype(np.float32)


def position():
    s = lax.axis_index("sp")
    d = lax.axis_index("dp")
    return s // RING, s % RING, d // 2, d % 2


def at(z, x, y, c):
    return (
        ((z + 2 * RING) % RING) * RING + (x + 2 * RING) % RING,
        ((y + 2 * RING) % RING) * 2 + c,
    )


def turn(heads, gain, cos, sin):
    normed = (
        heads * lax.rsqrt(jnp.mean(heads * heads, axis=-1, keepdims=True) + EPSILON) * gain
    )
    lane = lax.broadcasted_iota(jnp.int32, normed.shape, 1)
    turned = jnp.where(
        (lane // 32) % 2 == 0, -pltpu.roll(normed, 96, 1), pltpu.roll(normed, 32, 1)
    )
    return (normed * cos + turned * sin).astype(BF16)


class Exchange:
    def __init__(self, send_sem, recv_sem):
        self.send_sem, self.recv_sem, self.copies = send_sem, recv_sem, {}
        self.unsent = []

    def start(self, name, src, dst, peer):
        i = len(self.copies)
        copy = pltpu.make_async_remote_copy(
            src_ref=src,
            dst_ref=dst,
            send_sem=self.send_sem.at[i],
            recv_sem=self.recv_sem.at[i],
            device_id=peer,
            device_id_type=MESH,
        )
        assert name not in self.copies
        self.copies[name] = copy
        self.unsent.append(copy)
        copy.start()

    def arrived(self, *names):
        for name in names:
            self.copies[name].wait_recv()

    def settle(self, count):
        done = len(self.copies) - len(self.unsent)
        for copy in self.unsent[: count - done]:
            copy.wait_send()
        self.unsent = self.unsent[count - done :]


SPANS = {"d": (512, 1024, 512), "r": (1024, 512, 512)}
ROUNDS = 3
COPIES = 40 + 3 + ROUNDS * 2 * (62 + 3)


def iota(shape, dim):
    return lax.broadcasted_iota(jnp.int32, shape, dim)


def layer_kernel(
    q_hbm, k_hbm, v_hbm, w_hbm, res_hbm, gate_hbm, up_hbm, down_hbm,
    table_hbm, qg_hbm, kg_hbm, postg_hbm, preg_hbm, ids_hbm, gw_hbm, fs_hbm,
    out_ref,
    table_ref, qg_ref, kg_ref, postg_ref, preg_ref, ids_ref, gw_ref, fs_ref,
    kv, qt, q_raw, k_raw, v_raw, w, res, top, total, acc, att, mixed, normed,
    gate, up, down, meta,
    zs, rows, xs, xr, yr, gates, lifts, hidden, made, back, ret, comb, zret,
    spread, pick1, pick2, home,
    local_sem, send_sem, recv_sem,
):
    z, x, y, c = position()
    width = q_raw.shape[1]
    phase = Phase()
    phase("turn")
    loads = {}
    for i, (name, src, dst) in enumerate(
        [
            ("table", table_hbm, table_ref), ("k", k_hbm, k_raw), ("kg", kg_hbm, kg_ref),
            ("v", v_hbm, v_raw), ("ids", ids_hbm, ids_ref), ("gw", gw_hbm, gw_ref),
            ("fs", fs_hbm, fs_ref), ("qg", qg_hbm, qg_ref), ("q", q_hbm, q_raw),
            ("postg", postg_hbm, postg_ref), ("preg", preg_hbm, preg_ref), ("res", res_hbm, res),
            ("w", w_hbm, w), ("gate", gate_hbm.at[0], gate), ("up", up_hbm.at[0], up),
            ("down", down_hbm.at[0], down),
        ]
    ):
        loads[name] = pltpu.make_async_copy(src, dst, local_sem.at[i])
        loads[name].start()

    to_z = {s: at(z + s, x, y, c) for s in (1, 2, 3)}
    to_x = {s: at(z, x + s, y, c) for s in (1, 2, 3)}
    to_y = {(s, o): at(z, x, y + s, c if o == 0 else 1 - c) for s in range(4) for o in (0, 1)}
    del to_y[0, 0]
    ring = {"z": (to_z[1], to_z[3]), "x": (to_x[1], to_x[3])}
    barrier = pltpu.get_barrier_semaphore()
    peers = [*to_z.values(), *to_x.values(), *to_y.values()]
    for peer in peers:
        pl.semaphore_signal(barrier, inc=1, device_id=peer, device_id_type=MESH)
    ex = Exchange(send_sem, recv_sem)

    lane = iota((GRID_W, HEAD_DIM), 1)

    def table(which):
        halves = []
        for part in range(2):
            row = table_ref[which, pl.ds(2 * (z * RING + x) + part, 1), :]
            halves.append(jnp.where(lane < 64, row, table_ref[which, 32 : 32 + GRID_W, :]))
        return jnp.concatenate(halves, axis=0)

    loads["table"].wait()
    cos, sin = table(0), table(1)
    for name in ("ids", "gw", "fs"):
        loads[name].wait()
    meta[0, 0:2, :] = ids_ref[...].astype(F32)
    meta[0, 2:3, :] = gw_ref[...]
    meta[0, 3:4, :] = fs_ref[...]
    meta[0, 4:8, :] = jnp.zeros((4, 128), F32)
    loads["k"].wait()
    loads["kg"].wait()
    for h in range(KV_HEADS):
        raw = k_raw[:, h * 128 : (h + 1) * 128].astype(F32)
        kv[h // 2, 0, 0, :, (h % 2) * 128 : (h % 2 + 1) * 128] = turn(raw, kg_ref[...], cos, sin)
    loads["v"].wait()
    for half in range(2):
        kv[half, 0, 0, :, 256:512] = v_raw[:, half * 256 : (half + 1) * 256]
    phase("barrier")
    pl.semaphore_wait(barrier, len(peers))

    phase("start")
    first = ("x", "z")
    second = ("z", "x")
    low, high = pl.ds(0, 64), pl.ds(64, 64)

    def both(p, kind, r=0):
        names = ((kind, p, r, "+"), (kind, p, r, "-"))
        if kind == "own":
            peer = ring[first[p]]
            pairs = (kv.at[p, 0, 0], kv.at[p, 0, 3]), (kv.at[p, 0, 0], kv.at[p, 0, 1])
        elif kind == "relay":
            peer = ring[first[p]]
            pairs = (
                (kv.at[p, 0, 3, low], kv.at[p, 0, 2, low]),
                (kv.at[p, 0, 1, high], kv.at[p, 0, 2, high]),
            )
        elif kind == "far":
            peer = ring[second[p]]
            pairs = (kv.at[p, 0, r], kv.at[p, 3, r]), (kv.at[p, 0, r], kv.at[p, 1, r])
        else:
            peer = ring[second[p]]
            pairs = (
                (kv.at[p, 3, r, low], kv.at[p, 2, r, low]),
                (kv.at[p, 1, r, high], kv.at[p, 2, r, high]),
            )
        for name, (src, dst), to in zip(names, pairs, peer):
            ex.start(name, src, dst, to)

    def got(p, kind, r=0):
        ex.arrived((kind, p, r, "+"), (kind, p, r, "-"))

    for p in range(2):
        both(p, "own")
    for p in range(2):
        both(p, "far", 0)
    ex.start("meta+", meta.at[0], meta.at[3], ring["z"][0])
    ex.start("meta-", meta.at[0], meta.at[1], ring["z"][1])
    ex.start("meta2", meta.at[0], meta.at[2], to_z[2])

    phase("qturn")
    loads["q"].wait()
    loads["qg"].wait()
    for h in range(HEADS):
        raw = q_raw[:, h * 128 : (h + 1) * 128].astype(F32)
        qt[h // 4, (h % 4) * 128 : (h % 4 + 1) * 128, :] = turn(raw, qg_ref[...], cos, sin)

    phase("own")
    for p in range(2):
        got(p, "own")
        both(p, "relay")
    for r in (3, 1):
        for p in range(2):
            both(p, "far", r)

    phase("tables")
    eye = iota((128, 128), 0) == iota((128, 128), 1)
    earlier = (iota((128, 128), 0) < iota((128, 128), 1)).astype(F32)

    def lay(column):
        return jnp.sum(jnp.where(eye, column, 0.0), axis=0, keepdims=True)

    def stand(row):
        return jnp.sum(jnp.where(eye, row, 0.0), axis=1, keepdims=True)

    def counted(members):
        return jnp.dot(members, earlier, preferred_element_type=F32)

    relative = ((meta[0, 0:1, :].astype(jnp.int32) >> 5) - z + 4) & 3
    members = (iota((8, 128), 0) == relative).astype(F32)
    rank = jnp.sum(members * counted(members), axis=0, keepdims=True)
    target = relative.astype(F32) * 32.0 + rank
    pack = (iota((128, 128), 0).astype(F32) == target).astype(BF16)
    home[...] = (iota((128, 128), 1).astype(F32) == stand(target)).astype(BF16)

    phase("relay")
    for p in range(2):
        got(p, "relay")
        both(p, "far", 2)
    for p in range(2):
        got(p, "far", 0)
        both(p, "last", 0)

    phase("tables2")
    ex.arrived("meta+", "meta-", "meta2")
    stacks = [[], [], [], []]
    for r in range(4):
        inside = (meta[r, 0:1, :].astype(jnp.int32) >> 5) == z
        members = jnp.broadcast_to(inside.astype(F32), (8, 128))
        places = jnp.where(inside, counted(members)[0:1], -1.0)
        taken = iota((32, 128), 0).astype(F32) == places
        for which in range(4):
            stacks[which].append(
                jnp.sum(
                    jnp.where(taken, meta[r, which : which + 1, :], 0.0), axis=1, keepdims=True
                )
            )
    expert1, expert2, group_share, first_share = [jnp.concatenate(s, axis=0) for s in stacks]

    def relative_expert(column):
        e = lay(column).astype(jnp.int32) & 31
        return (
            ((((e >> 3) - x + 4) & 3) << 3)
            + (((((e >> 1) & 3) - y + 4) & 3) << 1)
            + ((e & 1) ^ c)
        )

    rel1, rel2 = relative_expert(expert1), relative_expert(expert2)
    named1 = (iota((32, 128), 0) == rel1).astype(F32)
    named2 = (iota((32, 128), 0) == rel2).astype(F32)
    ahead = counted(named1 + named2)
    slot1 = rel1.astype(F32) * 16.0 + jnp.sum(named1 * ahead, axis=0, keepdims=True)
    slot2 = rel2.astype(F32) * 16.0 + jnp.sum(named2 * ahead, axis=0, keepdims=True)
    places = iota((512, 128), 0).astype(F32)
    spread[...] = ((places == slot1) | (places == slot2)).astype(BF16)
    places = iota((128, 512), 1).astype(F32)
    pick1[...] = (places == stand(slot1)).astype(BF16)
    pick2[...] = (places == stand(slot2)).astype(BF16)
    weight1 = group_share * first_share
    weight2 = group_share * (1.0 - first_share)

    scale = float(np.log2(np.e) / np.sqrt(HEAD_DIM))

    def attend(blocks, opening=False):
        def one(g, carry):
            p, h = g // 2, g % 2

            def part(offset):
                cols = pl.ds(pl.multiple_of(offset + h * 128, 128), 128)
                return jnp.concatenate([kv[p, a, b, :, cols] for a, b in blocks], axis=0)

            keys, values = part(0), part(256)
            scores = lax.dot_general(
                keys, qt[g], (((1,), (1,)), ((), ())), preferred_element_type=F32
            )
            peak = jnp.max(scores, axis=0, keepdims=True)
            if not opening:
                before = top[g]
                peak = jnp.maximum(peak, before)
            weights = jnp.exp2((scores - peak) * scale)
            summed = jnp.sum(weights, axis=0, keepdims=True)
            out = lax.dot_general(
                values, weights.astype(BF16), (((0,), (0,)), ((), ())),
                preferred_element_type=F32,
            )
            if not opening:
                shrink = jnp.exp2((before - peak) * scale)
                summed += total[g] * shrink
                out += acc[g] * shrink
            top[g] = peak
            total[g] = summed
            acc[g] = out
            return carry

        lax.fori_loop(0, KV_HEADS, one, 0, unroll=len(blocks) < 4 or 2)

    phase("att0")
    attend([(0, 0), (0, 1), (0, 2), (0, 3)], opening=True)

    def step_on(r, kind):
        for p in range(2):
            got(p, kind, r)
            if kind == "far":
                both(p, "last", r)

    phase("far3")
    step_on(3, "far")
    phase("att1")
    attend([(3, 0), (3, 3), (1, 0), (1, 3)])
    phase("far1")
    step_on(1, "far")
    phase("far2")
    step_on(2, "far")
    phase("att2")
    attend([(3, 1), (1, 1), (3, 2), (1, 2)])
    phase("last03")
    step_on(0, "last")
    step_on(3, "last")
    phase("att3")
    attend([(2, 0), (2, 3)])
    phase("last12")
    step_on(1, "last")
    phase("att4")
    attend([(2, 1)])
    phase("last2")
    step_on(2, "last")
    phase("att5")
    attend([(2, 2)])

    phase("div")
    for g in range(KV_HEADS):
        scaled = acc[g] / total[g]
        for h in range(4):
            head = g * 4 + h
            att[:, head * 128 : (head + 1) * 128] = (
                scaled[:, h * 128 : (h + 1) * 128].T.astype(BF16)
            )
    for name in ("postg", "preg", "res"):
        loads[name].wait()
    loads["w"].wait()
    phase("proj")

    def project(n, carry):
        cols = pl.ds(pl.multiple_of(n * 512, 512), 512)
        mixed[:, cols] = jnp.dot(att[...], w[:, cols], preferred_element_type=F32).astype(BF16)
        return carry

    lax.fori_loop(0, 4, project, 0, unroll=True)
    phase("norm")

    def norm(n, carry):
        at_rows = pl.ds(pl.multiple_of(n * 32, 32), 32)
        m = mixed[at_rows, :].astype(F32)
        m = m * lax.rsqrt(jnp.mean(m * m, axis=-1, keepdims=True) + EPSILON) * postg_ref[...]
        stream = (res[at_rows, :].astype(F32) + m).astype(BF16)
        res[at_rows, :] = stream
        s = stream.astype(F32)
        s = s * lax.rsqrt(jnp.mean(s * s, axis=-1, keepdims=True) + EPSILON) * preg_ref[...]
        normed[at_rows, :] = s.astype(BF16)
        return carry

    lax.fori_loop(0, 4, norm, 0, unroll=2)

    def begin_of(tag, i):
        return sum(SPANS[tag][:i])

    def span_of(tag, i):
        return pl.ds(begin_of(tag, i), SPANS[tag][i])

    def z_out(tag, i, src, dst):
        cols = span_of(tag, i)
        for r in (2, 1, 3):
            ex.start((tag, "z", r, i), src.at[r, :, cols], dst.at[4 - r, :, cols], to_z[r])

    def z_in(tag, i):
        ex.arrived(*[(tag, "z", r, i) for r in (2, 1, 3)])

    def swap(tag, i, src, mid, dst):
        step = SPANS[tag][i] // 2
        a, b = pl.ds(begin_of(tag, i), step), pl.ds(begin_of(tag, i) + step, step)

        def x_out(w, r, ref, to_ref, cols):
            ex.start(
                (tag, w, "x", r, i), ref.at[r, :, :, :, cols], to_ref.at[4 - r, :, :, :, cols],
                to_x[r],
            )

        def x_in(w, r):
            ex.arrived((tag, w, "x", 4 - r, i))

        sides = [(2, 0), (2, 1), (1, 0), (3, 0), (1, 1), (3, 1), (0, 1)]

        def y_out(w, r, ref, to_ref, cols):
            for ry, rc in sides:
                ex.start(
                    (tag, w, "y", r, ry, rc, i), ref.at[r, ry, rc, :, cols],
                    to_ref.at[r, (4 - ry) % 4, rc, :, cols], to_y[ry, rc],
                )
            to_ref[r, 0, 0, :, cols] = ref[r, 0, 0, :, cols]

        def y_in(w, r):
            ex.arrived(*[(tag, w, "y", r, ry, rc, i) for ry, rc in sides])

        for r in (2, 1, 3):
            x_out("a", r, src, mid, a)
        yield
        for r in (2, 3, 1):
            y_out("b", r, src, mid, b)
        y_out("a", 0, src, dst, a)
        y_out("b", 0, src, dst, b)
        yield
        y_in("b", 2)
        x_out("b", 2, mid, dst, b)
        y_in("b", 3)
        x_out("b", 3, mid, dst, b)
        x_in("a", 2)
        y_out("a", 2, mid, dst, a)
        y_in("b", 1)
        x_out("b", 1, mid, dst, b)
        x_in("a", 3)
        y_out("a", 3, mid, dst, a)
        x_in("a", 1)
        y_out("a", 1, mid, dst, a)
        yield
        y_in("a", 0)
        y_in("b", 0)
        y_in("a", 2)
        x_in("b", 2)
        yield
        y_in("a", 3)
        x_in("b", 3)
        yield
        y_in("a", 1)
        x_in("b", 1)

    def run(steps, count):
        for _ in range(count):
            next(steps, None)

    phase("pack")
    for i in range(ROUNDS):
        cols = span_of("d", i)
        packed = jnp.dot(pack, normed[:, cols], preferred_element_type=F32).astype(BF16)
        zs[:, :, cols] = packed.reshape(4, 32, SPANS["d"][i])
        rows[0, :, cols] = packed[0:32]
        z_out("d", i, zs, rows)

    def slots(i):
        cols = span_of("d", i)
        z_in("d", i)
        phase("slots%d" % i)
        spaced = jnp.dot(
            spread[...], rows[:, :, cols].reshape(128, SPANS["d"][i]), preferred_element_type=F32
        )
        xs[:, :, :, :, cols] = spaced.astype(BF16).reshape(4, 4, 2, 16, SPANS["d"][i])

    def lift(i, at_r, count):
        cols, at_rows = span_of("d", i), pl.ds(at_r * 128, count * 128)
        arrived = yr[at_r : at_r + count, :, :, :, cols].reshape(count * 128, SPANS["d"][i])
        for sums, weight in ((gates, gate), (lifts, up)):
            product = jnp.dot(arrived, weight[cols, :], preferred_element_type=F32)
            sums[at_rows, :] = product if i == 0 else sums[at_rows, :] + product

    def lower(i, half):
        step = SPANS["r"][i] // 2
        cols = pl.ds(begin_of("r", i) + half * step, step)
        produced = jnp.dot(hidden[...], down[:, cols], preferred_element_type=F32)
        made[:, :, :, :, cols] = produced.astype(BF16).reshape(4, 4, 2, 16, step)

    def combine(i):
        cols = span_of("r", i)
        returned = ret[:, :, :, :, cols].reshape(512, SPANS["r"][i])
        one = jnp.dot(pick1[...], returned, preferred_element_type=F32)
        two = jnp.dot(pick2[...], returned, preferred_element_type=F32)
        summed = (weight1 * one + weight2 * two).astype(BF16)
        comb[:, :, cols] = summed.reshape(4, 32, SPANS["r"][i])
        zret[0, :, cols] = summed[0:32]
        z_out("r", i, comb, zret)

    there = [swap("d", i, xs, xr, yr) for i in range(ROUNDS)]
    def begin(i):
        phase("zin%d" % i)
        slots(i)
        phase("d_start%d" % i)
        run(there[i], 2)

    def middle(i):
        phase("d_mid%d" % i)
        run(there[i], 1)

    begin(0)
    ex.settle(43)
    begin(1)
    middle(0)
    begin(2)
    middle(1)
    phase("d_in0")
    run(there[0], 3)
    phase("lift0")
    loads["gate"].wait()
    loads["up"].wait()
    lift(0, 0, 4)
    middle(2)
    ex.settle(43 + 3 * ROUNDS + 62)
    for i in (1, 2):
        for pieces in (((0, 1), (2, 1)), ((3, 1),), ((1, 1),)):
            phase("d_in%d" % i)
            run(there[i], 1)
            phase("lift%d" % i)
            for piece in pieces:
                lift(i, *piece)
    phase("silu")
    g = gates[...]
    hidden[...] = (g / (1.0 + jnp.exp(-g)) * lifts[...]).astype(BF16)
    loads["down"].wait()

    home_way = [swap("r", i, made, back, ret) for i in range(ROUNDS)]
    def begin(i):
        for half in range(2):
            phase("lower%d" % i)
            lower(i, half)
            phase("r_start%d" % i)
            run(home_way[i], 1)

    def middle(i):
        phase("r_mid%d" % i)
        run(home_way[i], 1)

    def end(i):
        phase("r_in%d" % i)
        run(home_way[i], 3)
        phase("combine%d" % i)
        combine(i)

    begin(0)
    begin(1)
    middle(0)
    begin(2)
    middle(1)
    ex.settle(43 + 3 * ROUNDS + 62 * ROUNDS)
    end(0)
    middle(2)
    end(1)
    ex.settle(len(ex.copies) - 40)
    end(2)

    def arrive(i):
        cols = span_of("r", i)
        z_in("r", i)
        added = jnp.dot(
            home[...], zret[:, :, cols].reshape(128, SPANS["r"][i]), preferred_element_type=F32
        )
        out_ref[:, cols] = (res[:, cols].astype(F32) + added).astype(BF16)

    for i in range(ROUNDS):
        phase("out%d" % i)
        arrive(i)
    phase("sent")
    ex.settle(COPIES)
    phase()


def layer(
    q, k, v, w, res, gate, up, down, query_gain, key_gain, post_gain, pre_gain, ids, gw, fs
):
    hbm = pl.BlockSpec(memory_space=pltpu.HBM)
    vmem = pl.BlockSpec(memory_space=pltpu.VMEM)
    tokens, width = q.shape
    _, _, ff = gate.shape
    slots = pltpu.VMEM((4, 4, 2, 16, width), BF16)
    z_block = pltpu.VMEM((4, 32, width), BF16)
    rows = pltpu.VMEM((tokens, width), BF16)
    return pl.pallas_call(
        layer_kernel,
        out_shape=pltpu.VMEM((tokens, width), BF16),
        in_specs=[hbm] * 16,
        out_specs=vmem,
        scratch_shapes=[
            pltpu.VMEM((2, 32 + GRID_W, HEAD_DIM), F32),
            pltpu.VMEM((1, HEAD_DIM), F32),
            pltpu.VMEM((1, HEAD_DIM), F32),
            pltpu.VMEM((1, width), F32),
            pltpu.VMEM((1, width), F32),
            pltpu.VMEM((2, tokens), jnp.int32),
            pltpu.VMEM((1, tokens), F32),
            pltpu.VMEM((1, tokens), F32),
            pltpu.VMEM((2, 4, 4, 128, 512), BF16),
            pltpu.VMEM((4, 512, 128), BF16),
            rows,
            pltpu.VMEM((tokens, 512), BF16),
            pltpu.VMEM((tokens, 512), BF16),
            pltpu.VMEM((width, width), BF16),
            rows,
            pltpu.VMEM((4, 1, 512), F32),
            pltpu.VMEM((4, 1, 512), F32),
            pltpu.VMEM((4, 128, 512), F32),
            rows,
            rows,
            rows,
            pltpu.VMEM((width, ff), BF16),
            pltpu.VMEM((width, ff), BF16),
            pltpu.VMEM((ff, width), BF16),
            pltpu.VMEM((4, 8, 128), F32),
            z_block, z_block, slots, slots, slots,
            pltpu.VMEM((512, ff), F32),
            pltpu.VMEM((512, ff), F32),
            pltpu.VMEM((512, ff), BF16),
            slots, slots, slots, z_block, z_block,
            pltpu.VMEM((512, 128), BF16),
            pltpu.VMEM((128, 512), BF16),
            pltpu.VMEM((128, 512), BF16),
            pltpu.VMEM((128, 128), BF16),
            pltpu.SemaphoreType.DMA((16,)),
            pltpu.SemaphoreType.DMA((COPIES,)),
            pltpu.SemaphoreType.DMA((COPIES,)),
        ],
        compiler_params=pltpu.CompilerParams(
            collective_id=0, has_side_effects=True, vmem_limit_bytes=60 * 1024 * 1024
        ),
        name="layer",
    )(
        q, k, v, w, res, gate, up, down, jnp.asarray(angle_tables()), query_gain.reshape(1, -1),
        key_gain.reshape(1, -1), post_gain.reshape(1, -1), pre_gain.reshape(1, -1), ids, gw, fs,
    )


def local(
    residual_in,
    query_proj,
    key_proj,
    value_proj,
    query_gain,
    key_gain,
    out_weight,
    post_gain,
    pre_gain,
    route_ids,
    group_weight,
    first_share,
    gate_weight,
    up_weight,
    down_weight,
):
    out = layer(
        query_proj[0], key_proj[0], value_proj[0], out_weight, residual_in[0],
        gate_weight, up_weight, down_weight, query_gain, key_gain, post_gain, pre_gain,
        route_ids[0].T, group_weight, first_share,
    )
    return out[None]


def solution(mesh):
    placed = (
        P("dp", "sp", None),
        P("dp", "sp", None),
        P("dp", "sp", None),
        P("dp", "sp", None),
        P(),
        P(),
        P(),
        P(),
        P(),
        P("dp", "sp", None),
        P("dp", "sp"),
        P("dp", "sp"),
        P(("sp", "dp"), None, None),
        P(("sp", "dp"), None, None),
        P(("sp", "dp"), None, None),
    )
    return jax.shard_map(
        local, mesh=mesh, in_specs=placed, out_specs=P("dp", "sp", None), check_vma=False
    )
```

```python
import jax
import jax.numpy as jnp
import numpy as np
from jax import lax
from jax.experimental import pallas as pl
from jax.experimental.pallas import tpu as pltpu
from jax.sharding import PartitionSpec as P

HEADS = 16
KV_HEADS = 4
HEAD_DIM = 128
GRID_W = 64
RING = 4
EPSILON = 1e-06
MESH = pl.DeviceIdType.MESH


class Phase:
    def __init__(self):
        self.scope = None

    def __call__(self, name=None):
        if self.scope is not None:
            self.scope.__exit__(None, None, None)
        self.scope = None
        if name is not None:
            self.scope = jax.named_scope(name)
            self.scope.__enter__()


F32 = jnp.float32
BF16 = jnp.bfloat16


def angle_tables():
    quarter = HEAD_DIM // 4
    inverse = (np.float32(10000.0) ** (-np.arange(quarter, dtype=np.float32) / quarter)).astype(
        np.float32
    )
    places = np.concatenate([np.arange(32), np.arange(GRID_W)]).astype(np.float32)
    angles = places[:, None] * np.tile(inverse, 4)[None, :]
    return np.stack([np.cos(angles), np.sin(angles)]).astype(np.float32)


def position():
    s = lax.axis_index("sp")
    d = lax.axis_index("dp")
    return s // RING, s % RING, d // 2, d % 2


def at(z, x, y, c):
    return (
        ((z + 2 * RING) % RING) * RING + (x + 2 * RING) % RING,
        ((y + 2 * RING) % RING) * 2 + c,
    )


def turn(heads, gain, cos, sin):
    normed = (
        heads * lax.rsqrt(jnp.mean(heads * heads, axis=-1, keepdims=True) + EPSILON) * gain
    )
    lane = lax.broadcasted_iota(jnp.int32, normed.shape, 1)
    turned = jnp.where(
        (lane // 32) % 2 == 0, -pltpu.roll(normed, 96, 1), pltpu.roll(normed, 32, 1)
    )
    return (normed * cos + turned * sin).astype(BF16)


class Exchange:
    def __init__(self, send_sem, recv_sem):
        self.send_sem, self.recv_sem = send_sem, recv_sem
        self.sent_at, self.got_at = {}, {}

    def start(self, sent, got, src, dst, peer):
        pltpu.make_async_remote_copy(
            src_ref=src,
            dst_ref=dst,
            send_sem=self.send_sem.at[self.sent_at.setdefault(sent, len(self.sent_at))],
            recv_sem=self.recv_sem.at[self.got_at.setdefault(got, len(self.got_at))],
            device_id=peer,
            device_id_type=MESH,
        ).start()

    def arrived(self, got, like):
        pltpu.make_async_copy(like, like, self.recv_sem.at[self.got_at[got]]).wait()

    def settle(self, sent, like):
        pltpu.make_async_copy(like, like, self.send_sem.at[self.sent_at[sent]]).wait()


SPANS = {"d": (256, 512, 768, 512), "r": (512, 768, 512, 256)}
ROUNDS = 4
SENT = 5 + 4 * ROUNDS
GOT = 21 + 2 * 8 * ROUNDS


def iota(shape, dim):
    return lax.broadcasted_iota(jnp.int32, shape, dim)


def layer_kernel(
    q_hbm, k_hbm, v_hbm, w_hbm, res_hbm, gate_hbm, up_hbm, down_hbm,
    table_hbm, qg_hbm, kg_hbm, postg_hbm, preg_hbm, ids_hbm, gw_hbm, fs_hbm,
    out_ref,
    table_ref, qg_ref, kg_ref, postg_ref, preg_ref, ids_ref, gw_ref, fs_ref,
    kv, qt, q_raw, k_raw, v_raw, w, res, top, total, acc, att, mixed, normed,
    gate, up, down, meta,
    zs, rows, xs, xr, yr, gates, lifts, hidden, made, back, ret, comb, zret,
    spread, pick1, pick2, home, tally,
    local_sem, send_sem, recv_sem,
):
    z, x, y, c = position()
    width = q_raw.shape[1]
    phase = Phase()
    phase("turn")
    to_z = {s: at(z + s, x, y, c) for s in (1, 2, 3)}
    to_x = {s: at(z, x + s, y, c) for s in (1, 2, 3)}
    to_y = {(s, o): at(z, x, y + s, c if o == 0 else 1 - c) for s in range(4) for o in (0, 1)}
    del to_y[0, 0]
    ring = {"z": (to_z[1], to_z[3]), "x": (to_x[1], to_x[3])}
    barrier = pltpu.get_barrier_semaphore()
    peers = [*to_z.values(), *to_x.values(), *to_y.values()]
    for peer in peers:
        pl.semaphore_signal(barrier, inc=1, device_id=peer, device_id_type=MESH)
    loads = {}
    for i, (name, src, dst) in enumerate(
        [
            ("table", table_hbm, table_ref), ("k", k_hbm, k_raw), ("kg", kg_hbm, kg_ref),
            ("v", v_hbm, v_raw), ("ids", ids_hbm, ids_ref), ("gw", gw_hbm, gw_ref),
            ("fs", fs_hbm, fs_ref), ("qg", qg_hbm, qg_ref), ("q", q_hbm, q_raw),
            ("postg", postg_hbm, postg_ref), ("preg", preg_hbm, preg_ref), ("res", res_hbm, res),
            ("w", w_hbm, w), ("gate", gate_hbm.at[0], gate), ("up", up_hbm.at[0], up),
            ("down", down_hbm.at[0], down),
        ]
    ):
        loads[name] = pltpu.make_async_copy(src, dst, local_sem.at[i])
        loads[name].start()
    ex = Exchange(send_sem, recv_sem)

    lane = iota((GRID_W, HEAD_DIM), 1)

    def table(which):
        halves = []
        for part in range(2):
            row = table_ref[which, pl.ds(2 * (z * RING + x) + part, 1), :]
            halves.append(jnp.where(lane < 64, row, table_ref[which, 32 : 32 + GRID_W, :]))
        return jnp.concatenate(halves, axis=0)

    loads["table"].wait()
    cos, sin = table(0), table(1)
    for name in ("ids", "gw", "fs"):
        loads[name].wait()
    meta[0, 0:2, :] = ids_ref[...].astype(F32)
    meta[0, 2:3, :] = gw_ref[...]
    meta[0, 3:4, :] = fs_ref[...]
    meta[0, 4:8, :] = jnp.zeros((4, 128), F32)
    loads["k"].wait()
    loads["kg"].wait()
    for h in range(KV_HEADS):
        raw = k_raw[:, h * 128 : (h + 1) * 128].astype(F32)
        kv[h // 2, 0, 0, :, (h % 2) * 128 : (h % 2 + 1) * 128] = turn(raw, kg_ref[...], cos, sin)
    loads["v"].wait()
    for half in range(2):
        kv[half, 0, 0, :, 256:512] = v_raw[:, half * 256 : (half + 1) * 256]
    phase("barrier")
    pl.semaphore_wait(barrier, len(peers))

    phase("start")
    first = ("x", "z")
    second = ("z", "x")
    low, high = pl.ds(0, 64), pl.ds(64, 64)

    def both(p, kind, r=0):
        if kind == "own":
            peer = ring[first[p]]
            pairs = (kv.at[p, 0, 0], kv.at[p, 0, 3]), (kv.at[p, 0, 0], kv.at[p, 0, 1])
        elif kind == "relay":
            peer = ring[first[p]]
            pairs = (
                (kv.at[p, 0, 3, low], kv.at[p, 0, 2, low]),
                (kv.at[p, 0, 1, high], kv.at[p, 0, 2, high]),
            )
        elif kind == "far":
            peer = ring[second[p]]
            pairs = (kv.at[p, 0, r], kv.at[p, 3, r]), (kv.at[p, 0, r], kv.at[p, 1, r])
        else:
            peer = ring[second[p]]
            pairs = (
                (kv.at[p, 3, r, low], kv.at[p, 2, r, low]),
                (kv.at[p, 1, r, high], kv.at[p, 2, r, high]),
            )
        for (src, dst), to in zip(pairs, peer):
            ex.start(kind, (kind, p, r), src, dst, to)

    def got(p, kind, r=0):
        whole = kind in ("own", "far")
        ex.arrived((kind, p, r), kv.at[p, 0, pl.ds(0, 2 if whole else 1)])

    for p in range(2):
        both(p, "own")
    for p in range(2):
        both(p, "far", 0)
    for r in (1, 2, 3):
        ex.start("meta", "meta", meta.at[0], meta.at[4 - r], to_z[r])

    phase("qturn")
    loads["q"].wait()
    loads["qg"].wait()
    for h in range(HEADS):
        raw = q_raw[:, h * 128 : (h + 1) * 128].astype(F32)
        qt[h // 4, (h % 4) * 128 : (h % 4 + 1) * 128, :] = turn(raw, qg_ref[...], cos, sin)

    phase("own")
    for p in range(2):
        got(p, "own")
        both(p, "relay")
    for r in (3, 1):
        for p in range(2):
            both(p, "far", r)

    phase("tables")
    eye = iota((128, 128), 0) == iota((128, 128), 1)
    earlier = (iota((128, 128), 0) < iota((128, 128), 1)).astype(F32)

    def lay(column):
        return jnp.sum(jnp.where(eye, column, 0.0), axis=0, keepdims=True)

    def stand(row):
        return jnp.sum(jnp.where(eye, row, 0.0), axis=1, keepdims=True)

    def counted(members):
        return jnp.dot(members, earlier, preferred_element_type=F32)

    relative = ((meta[0, 0:1, :].astype(jnp.int32) >> 5) - z + 4) & 3
    members = (iota((8, 128), 0) == relative).astype(F32)
    rank = jnp.sum(members * counted(members), axis=0, keepdims=True)
    target = relative.astype(F32) * 32.0 + rank
    pack = (iota((128, 128), 0).astype(F32) == target).astype(BF16)
    home[...] = (iota((128, 128), 1).astype(F32) == stand(target)).astype(BF16)

    phase("relay")
    for p in range(2):
        got(p, "relay")
        both(p, "far", 2)
    for p in range(2):
        got(p, "far", 0)
        both(p, "last", 0)

    phase("tables2")
    ex.arrived("meta", meta.at[pl.ds(0, 3)])
    stacks = [[], [], [], []]
    for r in range(4):
        inside = (meta[r, 0:1, :].astype(jnp.int32) >> 5) == z
        members = jnp.broadcast_to(inside.astype(F32), (8, 128))
        places = jnp.where(inside, counted(members)[0:1], -1.0)
        taken = iota((32, 128), 0).astype(F32) == places
        for which in range(4):
            stacks[which].append(
                jnp.sum(
                    jnp.where(taken, meta[r, which : which + 1, :], 0.0), axis=1, keepdims=True
                )
            )
    expert1, expert2, group_share, first_share = [jnp.concatenate(s, axis=0) for s in stacks]

    def relative_expert(column):
        e = lay(column).astype(jnp.int32) & 31
        return (
            ((((e >> 3) - x + 4) & 3) << 3)
            + (((((e >> 1) & 3) - y + 4) & 3) << 1)
            + ((e & 1) ^ c)
        )

    rel1, rel2 = relative_expert(expert1), relative_expert(expert2)
    named1 = (iota((32, 128), 0) == rel1).astype(F32)
    named2 = (iota((32, 128), 0) == rel2).astype(F32)
    ahead = counted(named1 + named2)
    slot1 = rel1.astype(F32) * 16.0 + jnp.sum(named1 * ahead, axis=0, keepdims=True)
    slot2 = rel2.astype(F32) * 16.0 + jnp.sum(named2 * ahead, axis=0, keepdims=True)
    places = iota((512, 128), 0).astype(F32)
    spread[...] = ((places == slot1) | (places == slot2)).astype(BF16)
    places = iota((128, 512), 1).astype(F32)
    pick1[...] = (places == stand(slot1)).astype(BF16)
    pick2[...] = (places == stand(slot2)).astype(BF16)
    weight1 = group_share * first_share
    weight2 = group_share * (1.0 - first_share)

    scale = float(np.log2(np.e) / np.sqrt(HEAD_DIM))

    def attend(blocks, opening=False):
        def one(g, carry):
            p, h = g // 2, g % 2

            def part(offset):
                cols = pl.ds(pl.multiple_of(offset + h * 128, 128), 128)
                return jnp.concatenate([kv[p, a, b, :, cols] for a, b in blocks], axis=0)

            keys, values = part(0), part(256)
            scores = lax.dot_general(
                keys, qt[g], (((1,), (1,)), ((), ())), preferred_element_type=F32
            )
            peak = jnp.max(scores, axis=0, keepdims=True)
            if not opening:
                before = top[g]
                peak = jnp.maximum(peak, before)
            weights = jnp.exp2((scores - peak) * scale)
            summed = jnp.sum(weights, axis=0, keepdims=True)
            out = lax.dot_general(
                values, weights.astype(BF16), (((0,), (0,)), ((), ())),
                preferred_element_type=F32,
            )
            if not opening:
                shrink = jnp.exp2((before - peak) * scale)
                summed += total[g] * shrink
                out += acc[g] * shrink
            top[g] = peak
            total[g] = summed
            acc[g] = out
            return carry

        lax.fori_loop(0, KV_HEADS, one, 0, unroll=len(blocks) < 4 or 2)

    phase("att0")
    attend([(0, 0), (0, 1), (0, 2), (0, 3)], opening=True)

    def step_on(r, kind):
        for p in range(2):
            got(p, kind, r)
            if kind == "far":
                both(p, "last", r)

    phase("far3")
    step_on(3, "far")
    phase("att1")
    attend([(3, 0), (3, 3), (1, 0), (1, 3)])
    phase("far1")
    step_on(1, "far")
    phase("far2")
    step_on(2, "far")
    phase("att2")
    attend([(3, 1), (1, 1), (3, 2), (1, 2)])
    phase("last03")
    step_on(0, "last")
    step_on(3, "last")
    phase("att3")
    attend([(2, 0), (2, 3)])
    phase("last12")
    step_on(1, "last")
    phase("att4")
    attend([(2, 1)])
    phase("last2")
    step_on(2, "last")
    phase("att5")
    attend([(2, 2)])

    phase("div")
    for g in range(KV_HEADS):
        scaled = acc[g] / total[g]
        for h in range(4):
            head = g * 4 + h
            att[:, head * 128 : (head + 1) * 128] = (
                scaled[:, h * 128 : (h + 1) * 128].T.astype(BF16)
            )
    for name in ("postg", "preg", "res"):
        loads[name].wait()
    loads["w"].wait()
    phase("proj")

    def project(n, carry):
        cols = pl.ds(pl.multiple_of(n * 512, 512), 512)
        mixed[:, cols] = jnp.dot(att[...], w[:, cols], preferred_element_type=F32).astype(BF16)
        return carry

    lax.fori_loop(0, 4, project, 0, unroll=True)
    phase("norm")

    def norm(n, carry):
        at_rows = pl.ds(pl.multiple_of(n * 32, 32), 32)
        m = mixed[at_rows, :].astype(F32)
        m = m * lax.rsqrt(jnp.mean(m * m, axis=-1, keepdims=True) + EPSILON) * postg_ref[...]
        stream = (res[at_rows, :].astype(F32) + m).astype(BF16)
        res[at_rows, :] = stream
        s = stream.astype(F32)
        s = s * lax.rsqrt(jnp.mean(s * s, axis=-1, keepdims=True) + EPSILON) * preg_ref[...]
        normed[at_rows, :] = s.astype(BF16)
        return carry

    lax.fori_loop(0, 4, norm, 0, unroll=2)

    def begin_of(tag, i):
        return sum(SPANS[tag][:i])

    def span_of(tag, i):
        return pl.ds(begin_of(tag, i), SPANS[tag][i])

    def like(count, columns):
        return tally.at[pl.ds(0, count), pl.ds(0, columns)]

    def z_out(tag, i, src, dst):
        cols = span_of(tag, i)
        for r in (2, 1, 3):
            name = (tag, "z", i)
            ex.start(name, name, src.at[r, :, cols], dst.at[4 - r, :, cols], to_z[r])

    def z_in(tag, i):
        ex.arrived((tag, "z", i), like(96, SPANS[tag][i]))

    def swap(tag, i, src, mid, dst):
        step = SPANS[tag][i] // 2
        a, b = pl.ds(begin_of(tag, i), step), pl.ds(begin_of(tag, i) + step, step)

        def x_out(w, r, ref, to_ref, cols):
            ex.start(
                (tag, i), (tag, "x", r, i) if w == "a" else (tag, i),
                ref.at[r, :, :, :, cols], to_ref.at[4 - r, :, :, :, cols], to_x[r],
            )

        def x_in(r):
            ex.arrived((tag, "x", 4 - r, i), like(128, step))

        sides = [(2, 0), (2, 1), (1, 0), (3, 0), (1, 1), (3, 1), (0, 1)]

        def y_out(w, r, ref, to_ref, cols):
            for ry, rc in sides:
                ex.start(
                    (tag, i), (tag, "y", r, i) if w == "b" and r else (tag, i),
                    ref.at[r, ry, rc, :, cols], to_ref.at[r, (4 - ry) % 4, rc, :, cols],
                    to_y[ry, rc],
                )
            to_ref[r, 0, 0, :, cols] = ref[r, 0, 0, :, cols]

        def y_in(r):
            ex.arrived((tag, "y", r, i), like(112, step))

        for r in (2, 1, 3):
            x_out("a", r, src, mid, a)
        yield
        for r in (2, 3, 1):
            y_out("b", r, src, mid, b)
        y_out("a", 0, src, dst, a)
        y_out("b", 0, src, dst, b)
        yield
        y_in(2)
        x_out("b", 2, mid, dst, b)
        y_in(3)
        x_out("b", 3, mid, dst, b)
        x_in(2)
        y_out("a", 2, mid, dst, a)
        y_in(1)
        x_out("b", 1, mid, dst, b)
        x_in(3)
        y_out("a", 3, mid, dst, a)
        x_in(1)
        y_out("a", 1, mid, dst, a)
        yield
        ex.arrived((tag, i), like(5 * 112 + 3 * 128, step))

    def settle_swaps(tag):
        for i in range(ROUNDS):
            ex.settle((tag, "z", i), like(96, SPANS[tag][i]))
            ex.settle((tag, i), like(4 * 112 + 3 * 128, SPANS[tag][i]))

    def run(steps, count):
        for _ in range(count):
            next(steps, None)

    phase("pack")
    for i in range(ROUNDS):
        cols = span_of("d", i)
        packed = jnp.dot(pack, normed[:, cols], preferred_element_type=F32).astype(BF16)
        zs[:, :, cols] = packed.reshape(4, 32, SPANS["d"][i])
        rows[0, :, cols] = packed[0:32]
        z_out("d", i, zs, rows)

    def slots(i):
        cols = span_of("d", i)
        z_in("d", i)
        phase("slots%d" % i)
        spaced = jnp.dot(
            spread[...], rows[:, :, cols].reshape(128, SPANS["d"][i]), preferred_element_type=F32
        )
        xs[:, :, :, :, cols] = spaced.astype(BF16).reshape(4, 4, 2, 16, SPANS["d"][i])

    def lift(i, at_r, count):
        cols, at_rows = span_of("d", i), pl.ds(at_r * 128, count * 128)
        arrived = yr[at_r : at_r + count, :, :, :, cols].reshape(count * 128, SPANS["d"][i])
        for sums, weight in ((gates, gate), (lifts, up)):
            product = jnp.dot(arrived, weight[cols, :], preferred_element_type=F32)
            sums[at_rows, :] = product if i == 0 else sums[at_rows, :] + product

    def lower(i, half):
        step = SPANS["r"][i] // 2
        cols = pl.ds(begin_of("r", i) + half * step, step)
        produced = jnp.dot(hidden[...], down[:, cols], preferred_element_type=F32)
        made[:, :, :, :, cols] = produced.astype(BF16).reshape(4, 4, 2, 16, step)

    def combine(i):
        cols = span_of("r", i)
        returned = ret[:, :, :, :, cols].reshape(512, SPANS["r"][i])
        one = jnp.dot(pick1[...], returned, preferred_element_type=F32)
        two = jnp.dot(pick2[...], returned, preferred_element_type=F32)
        summed = (weight1 * one + weight2 * two).astype(BF16)
        comb[:, :, cols] = summed.reshape(4, 32, SPANS["r"][i])
        zret[0, :, cols] = summed[0:32]
        z_out("r", i, comb, zret)

    there = [swap("d", i, xs, xr, yr) for i in range(ROUNDS)]
    def begin(i):
        phase("zin%d" % i)
        slots(i)
        phase("d_start%d" % i)
        run(there[i], 2)

    def middle(i):
        phase("d_mid%d" % i)
        run(there[i], 1)

    def done(i):
        phase("d_in%d" % i)
        run(there[i], 1)
        phase("lift%d" % i)
        lift(i, 0, 4)

    begin(0)
    ex.settle("own", kv.at[0, 0])
    ex.settle("relay", kv.at[0, 0, pl.ds(0, 2)])
    ex.settle("far", kv.at[0])
    ex.settle("last", kv.at[0, pl.ds(0, 2)])
    ex.settle("meta", meta.at[pl.ds(0, 3)])
    begin(1)
    middle(0)
    begin(2)
    middle(1)
    loads["gate"].wait()
    loads["up"].wait()
    done(0)
    begin(3)
    middle(2)
    done(1)
    middle(3)
    done(2)
    phase("d_in3")
    run(there[3], 1)
    phase("lift3")
    for half in range(2):
        lift(3, 2 * half, 2)
        at_rows = pl.ds(256 * half, 256)
        g = gates[at_rows, :]
        hidden[at_rows, :] = (g / (1.0 + jnp.exp(-g)) * lifts[at_rows, :]).astype(BF16)
    loads["down"].wait()

    home_way = [swap("r", i, made, back, ret) for i in range(ROUNDS)]
    def begin(i):
        for half in range(2):
            phase("lower%d" % i)
            lower(i, half)
            phase("r_start%d" % i)
            run(home_way[i], 1)

    def middle(i):
        phase("r_mid%d" % i)
        run(home_way[i], 1)

    def end(i):
        phase("r_in%d" % i)
        run(home_way[i], 1)
        phase("combine%d" % i)
        combine(i)

    begin(0)
    begin(1)
    middle(0)
    begin(2)
    middle(1)
    settle_swaps("d")
    end(0)
    begin(3)
    middle(2)
    end(1)
    middle(3)
    end(2)
    end(3)

    def arrive(i):
        cols = span_of("r", i)
        z_in("r", i)
        added = jnp.dot(
            home[...], zret[:, :, cols].reshape(128, SPANS["r"][i]), preferred_element_type=F32
        )
        out_ref[:, cols] = (res[:, cols].astype(F32) + added).astype(BF16)

    for i in range(ROUNDS):
        phase("out%d" % i)
        arrive(i)
    phase("sent")
    settle_swaps("r")
    phase()


def layer(
    q, k, v, w, res, gate, up, down, query_gain, key_gain, post_gain, pre_gain, ids, gw, fs
):
    hbm = pl.BlockSpec(memory_space=pltpu.HBM)
    vmem = pl.BlockSpec(memory_space=pltpu.VMEM)
    tokens, width = q.shape
    _, _, ff = gate.shape
    slots = pltpu.VMEM((4, 4, 2, 16, width), BF16)
    z_block = pltpu.VMEM((4, 32, width), BF16)
    rows = pltpu.VMEM((tokens, width), BF16)
    return pl.pallas_call(
        layer_kernel,
        out_shape=pltpu.VMEM((tokens, width), BF16),
        in_specs=[hbm] * 16,
        out_specs=vmem,
        scratch_shapes=[
            pltpu.VMEM((2, 32 + GRID_W, HEAD_DIM), F32),
            pltpu.VMEM((1, HEAD_DIM), F32),
            pltpu.VMEM((1, HEAD_DIM), F32),
            pltpu.VMEM((1, width), F32),
            pltpu.VMEM((1, width), F32),
            pltpu.VMEM((2, tokens), jnp.int32),
            pltpu.VMEM((1, tokens), F32),
            pltpu.VMEM((1, tokens), F32),
            pltpu.VMEM((2, 4, 4, 128, 512), BF16),
            pltpu.VMEM((4, 512, 128), BF16),
            rows,
            pltpu.VMEM((tokens, 512), BF16),
            pltpu.VMEM((tokens, 512), BF16),
            pltpu.VMEM((width, width), BF16),
            rows,
            pltpu.VMEM((4, 1, 512), F32),
            pltpu.VMEM((4, 1, 512), F32),
            pltpu.VMEM((4, 128, 512), F32),
            rows,
            rows,
            rows,
            pltpu.VMEM((width, ff), BF16),
            pltpu.VMEM((width, ff), BF16),
            pltpu.VMEM((ff, width), BF16),
            pltpu.VMEM((4, 8, 128), F32),
            z_block, z_block, slots, slots, slots,
            pltpu.VMEM((512, ff), F32),
            pltpu.VMEM((512, ff), F32),
            pltpu.VMEM((512, ff), BF16),
            slots, slots, slots, z_block, z_block,
            pltpu.VMEM((512, 128), BF16),
            pltpu.VMEM((128, 512), BF16),
            pltpu.VMEM((128, 512), BF16),
            pltpu.VMEM((128, 128), BF16),
            pltpu.VMEM((5 * 112 + 3 * 128, 1024), BF16),
            pltpu.SemaphoreType.DMA((16,)),
            pltpu.SemaphoreType.DMA((SENT,)),
            pltpu.SemaphoreType.DMA((GOT,)),
        ],
        compiler_params=pltpu.CompilerParams(
            collective_id=0, has_side_effects=True, vmem_limit_bytes=60 * 1024 * 1024
        ),
        name="layer",
    )(
        q, k, v, w, res, gate, up, down, jnp.asarray(angle_tables()), query_gain.reshape(1, -1),
        key_gain.reshape(1, -1), post_gain.reshape(1, -1), pre_gain.reshape(1, -1), ids, gw, fs,
    )


def local(
    residual_in,
    query_proj,
    key_proj,
    value_proj,
    query_gain,
    key_gain,
    out_weight,
    post_gain,
    pre_gain,
    route_ids,
    group_weight,
    first_share,
    gate_weight,
    up_weight,
    down_weight,
):
    out = layer(
        query_proj[0], key_proj[0], value_proj[0], out_weight, residual_in[0],
        gate_weight, up_weight, down_weight, query_gain, key_gain, post_gain, pre_gain,
        route_ids[0].T, group_weight, first_share,
    )
    return out[None]


def solution(mesh):
    placed = (
        P("dp", "sp", None),
        P("dp", "sp", None),
        P("dp", "sp", None),
        P("dp", "sp", None),
        P(),
        P(),
        P(),
        P(),
        P(),
        P("dp", "sp", None),
        P("dp", "sp"),
        P("dp", "sp"),
        P(("sp", "dp"), None, None),
        P(("sp", "dp"), None, None),
        P(("sp", "dp"), None, None),
    )
    return jax.shard_map(
        local, mesh=mesh, in_specs=placed, out_specs=P("dp", "sp", None), check_vma=False
    )
```

```python
import jax
import jax.numpy as jnp
import numpy as np
from jax import lax
from jax.experimental import pallas as pl
from jax.experimental.pallas import tpu as pltpu
from jax.sharding import PartitionSpec as P

HEADS = 16
KV_HEADS = 4
HEAD_DIM = 128
GRID_W = 64
RING = 4
EPSILON = 1e-06
MESH = pl.DeviceIdType.MESH


class Phase:
    def __init__(self):
        self.scope = None

    def __call__(self, name=None):
        if self.scope is not None:
            self.scope.__exit__(None, None, None)
        self.scope = None
        if name is not None:
            self.scope = jax.named_scope(name)
            self.scope.__enter__()


F32 = jnp.float32
BF16 = jnp.bfloat16


def angle_tables():
    quarter = HEAD_DIM // 4
    inverse = (np.float32(10000.0) ** (-np.arange(quarter, dtype=np.float32) / quarter)).astype(
        np.float32
    )
    places = np.concatenate([np.arange(32), np.arange(GRID_W)]).astype(np.float32)
    angles = places[:, None] * np.tile(inverse, 4)[None, :]
    return np.stack([np.cos(angles), np.sin(angles)]).astype(np.float32)


def position():
    s = lax.axis_index("sp")
    d = lax.axis_index("dp")
    return s // RING, s % RING, d // 2, d % 2


def at(z, x, y, c):
    return (
        ((z + 2 * RING) % RING) * RING + (x + 2 * RING) % RING,
        ((y + 2 * RING) % RING) * 2 + c,
    )


def turn(heads, gain, cos, sin):
    normed = (
        heads * lax.rsqrt(jnp.mean(heads * heads, axis=-1, keepdims=True) + EPSILON) * gain
    )
    lane = lax.broadcasted_iota(jnp.int32, normed.shape, 1)
    turned = jnp.where(
        (lane // 32) % 2 == 0, -pltpu.roll(normed, 96, 1), pltpu.roll(normed, 32, 1)
    )
    return (normed * cos + turned * sin).astype(BF16)


class Exchange:
    def __init__(self, send_sem, recv_sem):
        self.send_sem, self.recv_sem = send_sem, recv_sem
        self.sent_at, self.got_at = {}, {}

    def start(self, sent, got, src, dst, peer):
        pltpu.make_async_remote_copy(
            src_ref=src,
            dst_ref=dst,
            send_sem=self.send_sem.at[self.sent_at.setdefault(sent, len(self.sent_at))],
            recv_sem=self.recv_sem.at[self.got_at.setdefault(got, len(self.got_at))],
            device_id=peer,
            device_id_type=MESH,
        ).start()

    def arrived(self, got, like):
        pltpu.make_async_copy(like, like, self.recv_sem.at[self.got_at[got]]).wait()

    def settle(self, sent, like):
        pltpu.make_async_copy(like, like, self.send_sem.at[self.sent_at[sent]]).wait()


SPANS = {"d": (256, 768, 768, 256), "r": (512, 768, 512, 256)}
ROUNDS = 4
SENT = 6
GOT = 11 + 2 * 8 * ROUNDS


def iota(shape, dim):
    return lax.broadcasted_iota(jnp.int32, shape, dim)


def layer_kernel(
    q_hbm, k_hbm, v_hbm, w_hbm, res_hbm, gate_hbm, up_hbm, down_hbm,
    table_hbm, qg_hbm, kg_hbm, postg_hbm, preg_hbm, ids_hbm, gw_hbm, fs_hbm,
    out_ref,
    table_ref, qg_ref, kg_ref, postg_ref, preg_ref, ids_ref, gw_ref, fs_ref,
    kv, qt, q_raw, k_raw, v_raw, w, res, top, total, acc, att, mixed, normed,
    gate, up, down, meta,
    zs, rows, xs, xr, yr, gates, lifts, hidden, made, back, ret, comb, zret,
    spread, pick1, pick2, home, tally,
    local_sem, send_sem, recv_sem,
):
    z, x, y, c = position()
    width = q_raw.shape[1]
    phase = Phase()
    phase("turn")
    to_z = {s: at(z + s, x, y, c) for s in (1, 2, 3)}
    to_x = {s: at(z, x + s, y, c) for s in (1, 2, 3)}
    to_y = {(s, o): at(z, x, y + s, c if o == 0 else 1 - c) for s in range(4) for o in (0, 1)}
    del to_y[0, 0]
    ring = {"z": (to_z[1], to_z[3]), "x": (to_x[1], to_x[3])}
    loads = {}

    def load(*items):
        for name, src, dst in items:
            loads[name] = pltpu.make_async_copy(src, dst, local_sem.at[len(loads)])
            loads[name].start()

    load(
        ("v", v_hbm, v_raw), ("k", k_hbm, k_raw), ("table", table_hbm, table_ref),
        ("kg", kg_hbm, kg_ref),
    )
    barrier = pltpu.get_barrier_semaphore()
    peers = [*to_z.values(), *to_x.values(), *to_y.values()]
    for peer in peers:
        pl.semaphore_signal(barrier, inc=1, device_id=peer, device_id_type=MESH)
    load(
        ("ids", ids_hbm, ids_ref), ("gw", gw_hbm, gw_ref),
        ("fs", fs_hbm, fs_ref), ("qg", qg_hbm, qg_ref), ("q", q_hbm, q_raw),
        ("postg", postg_hbm, postg_ref), ("preg", preg_hbm, preg_ref), ("res", res_hbm, res),
        ("w", w_hbm, w), ("gate", gate_hbm.at[0], gate), ("up", up_hbm.at[0], up),
        ("down", down_hbm.at[0], down),
    )
    ex = Exchange(send_sem, recv_sem)

    loads["v"].wait()
    for half in range(2):
        kv[half, 0, 0, :, 256:512] = v_raw[:, half * 256 : (half + 1) * 256]
    phase("barrier")
    pl.semaphore_wait(barrier, len(peers))

    phase("start")
    first = ("x", "z")
    second = ("z", "x")
    low, high = pl.ds(0, 64), pl.ds(64, 64)

    def both(p, kind, r=0, lanes=slice(None)):
        if kind == "own":
            peer = ring[first[p]]
            pairs = (kv.at[p, 0, 0], kv.at[p, 0, 3]), (kv.at[p, 0, 0], kv.at[p, 0, 1])
        elif kind == "relay":
            peer = ring[first[p]]
            pairs = (
                (kv.at[p, 0, 3, low], kv.at[p, 0, 2, low]),
                (kv.at[p, 0, 1, high], kv.at[p, 0, 2, high]),
            )
        elif kind == "far":
            peer = ring[second[p]]
            pairs = (kv.at[p, 0, r], kv.at[p, 3, r]), (kv.at[p, 0, r], kv.at[p, 1, r])
        else:
            peer = ring[second[p]]
            pairs = (
                (kv.at[p, 3, r, low], kv.at[p, 2, r, low]),
                (kv.at[p, 1, r, high], kv.at[p, 2, r, high]),
            )
        for (src, dst), to in zip(pairs, peer):
            ex.start("kv", (kind, r), src.at[:, lanes], dst.at[:, lanes], to)

    def got(kind, r=0):
        ex.arrived((kind, r), kv.at[0, 0, pl.ds(0, 4 if kind in ("own", "far") else 2)])

    def own(lanes):
        for kind in ("own", "far"):
            for p in range(2):
                both(p, kind, 0, lanes)

    own(pl.ds(256, 256))
    phase("kturn")
    lane = iota((GRID_W, HEAD_DIM), 1)

    def table(which):
        halves = []
        for part in range(2):
            row = table_ref[which, pl.ds(2 * (z * RING + x) + part, 1), :]
            halves.append(jnp.where(lane < 64, row, table_ref[which, 32 : 32 + GRID_W, :]))
        return jnp.concatenate(halves, axis=0)

    loads["table"].wait()
    cos, sin = table(0), table(1)
    for name in ("ids", "gw", "fs"):
        loads[name].wait()
    meta[0, 0:2, :] = ids_ref[...].astype(F32)
    meta[0, 2:3, :] = gw_ref[...]
    meta[0, 3:4, :] = fs_ref[...]
    meta[0, 4:8, :] = jnp.zeros((4, 128), F32)
    loads["k"].wait()
    loads["kg"].wait()
    for h in range(KV_HEADS):
        raw = k_raw[:, h * 128 : (h + 1) * 128].astype(F32)
        kv[h // 2, 0, 0, :, (h % 2) * 128 : (h % 2 + 1) * 128] = turn(raw, kg_ref[...], cos, sin)
    own(pl.ds(0, 256))
    for r in (1, 2, 3):
        ex.start("meta", "meta", meta.at[0], meta.at[4 - r], to_z[r])

    phase("qturn")
    loads["q"].wait()
    loads["qg"].wait()
    for h in range(HEADS):
        raw = q_raw[:, h * 128 : (h + 1) * 128].astype(F32)
        qt[h // 4, :, (h % 4) * 128 : (h % 4 + 1) * 128] = turn(raw, qg_ref[...], cos, sin).T

    phase("own")
    got("own")
    for p in range(2):
        both(p, "relay")
    for r in (3, 1):
        for p in range(2):
            both(p, "far", r)

    phase("tables")
    eye = iota((128, 128), 0) == iota((128, 128), 1)
    earlier = (iota((128, 128), 0) < iota((128, 128), 1)).astype(F32)

    def lay(column):
        return jnp.sum(jnp.where(eye, column, 0.0), axis=0, keepdims=True)

    def stand(row):
        return jnp.sum(jnp.where(eye, row, 0.0), axis=1, keepdims=True)

    def counted(members):
        return jnp.dot(members, earlier, preferred_element_type=F32)

    relative = ((meta[0, 0:1, :].astype(jnp.int32) >> 5) - z + 4) & 3
    members = (iota((8, 128), 0) == relative).astype(F32)
    rank = jnp.sum(members * counted(members), axis=0, keepdims=True)
    target = relative.astype(F32) * 32.0 + rank
    pack = (iota((128, 128), 0).astype(F32) == target).astype(BF16)
    home[...] = (iota((128, 128), 1).astype(F32) == stand(target)).astype(BF16)

    phase("relay")
    got("relay")
    for p in range(2):
        both(p, "far", 2)
    got("far", 0)
    for p in range(2):
        both(p, "last", 0)

    phase("tables2")
    ex.arrived("meta", meta.at[pl.ds(0, 3)])
    stacks = [[], [], [], []]
    for r in range(4):
        inside = (meta[r, 0:1, :].astype(jnp.int32) >> 5) == z
        members = jnp.broadcast_to(inside.astype(F32), (8, 128))
        places = jnp.where(inside, counted(members)[0:1], -1.0)
        taken = iota((32, 128), 0).astype(F32) == places
        for which in range(4):
            stacks[which].append(
                jnp.sum(
                    jnp.where(taken, meta[r, which : which + 1, :], 0.0), axis=1, keepdims=True
                )
            )
    expert1, expert2, group_share, first_share = [jnp.concatenate(s, axis=0) for s in stacks]

    def relative_expert(column):
        e = lay(column).astype(jnp.int32) & 31
        return (
            ((((e >> 3) - x + 4) & 3) << 3)
            + (((((e >> 1) & 3) - y + 4) & 3) << 1)
            + ((e & 1) ^ c)
        )

    rel1, rel2 = relative_expert(expert1), relative_expert(expert2)
    named1 = (iota((32, 128), 0) == rel1).astype(F32)
    named2 = (iota((32, 128), 0) == rel2).astype(F32)
    ahead = counted(named1 + named2)
    slot1 = rel1.astype(F32) * 16.0 + jnp.sum(named1 * ahead, axis=0, keepdims=True)
    slot2 = rel2.astype(F32) * 16.0 + jnp.sum(named2 * ahead, axis=0, keepdims=True)
    places = iota((512, 128), 0).astype(F32)
    spread[...] = ((places == slot1) | (places == slot2)).astype(BF16)
    places = iota((128, 512), 1).astype(F32)
    pick1[...] = (places == stand(slot1)).astype(BF16)
    pick2[...] = (places == stand(slot2)).astype(BF16)
    weight1 = group_share * first_share
    weight2 = group_share * (1.0 - first_share)

    scale = float(np.log2(np.e) / np.sqrt(HEAD_DIM))

    def attend(blocks, opening=False):
        def one(g, carry):
            p, h = g // 2, g % 2

            def part(offset):
                cols = pl.ds(pl.multiple_of(offset + h * 128, 128), 128)
                return jnp.concatenate([kv[p, a, b, :, cols] for a, b in blocks], axis=0)

            keys, values = part(0), part(256)
            scores = jnp.dot(keys, qt[g], preferred_element_type=F32)
            peak = jnp.max(scores, axis=0, keepdims=True)
            if not opening:
                before = top[g]
                peak = jnp.maximum(peak, before)
            weights = jnp.exp2((scores - peak) * scale)
            summed = jnp.sum(weights, axis=0, keepdims=True)
            out = lax.dot_general(
                values, weights.astype(BF16), (((0,), (0,)), ((), ())),
                preferred_element_type=F32,
            )
            if not opening:
                shrink = jnp.exp2((before - peak) * scale)
                summed += total[g] * shrink
                out += acc[g] * shrink
            top[g] = peak
            total[g] = summed
            acc[g] = out
            return carry

        lax.fori_loop(0, KV_HEADS, one, 0, unroll=len(blocks) < 4 or 2)

    phase("att0")
    attend([(0, 0), (0, 1), (0, 2), (0, 3)], opening=True)

    def step_on(r, kind):
        got(kind, r)
        if kind == "far":
            for p in range(2):
                both(p, "last", r)

    phase("far3")
    step_on(3, "far")
    phase("att1")
    attend([(3, 0), (3, 3), (1, 0), (1, 3)])
    phase("far1")
    step_on(1, "far")
    phase("far2")
    step_on(2, "far")
    phase("att2")
    attend([(3, 1), (1, 1), (3, 2), (1, 2)])
    phase("last03")
    step_on(0, "last")
    step_on(3, "last")
    phase("att3")
    attend([(2, 0), (2, 3)])
    phase("last12")
    step_on(1, "last")
    phase("att4")
    attend([(2, 1)])
    phase("last2")
    step_on(2, "last")
    phase("att5")
    attend([(2, 2)])

    phase("div")
    for g in range(KV_HEADS):
        scaled = acc[g] / total[g]
        for h in range(4):
            head = g * 4 + h
            att[:, head * 128 : (head + 1) * 128] = (
                scaled[:, h * 128 : (h + 1) * 128].T.astype(BF16)
            )
    for name in ("postg", "preg", "res"):
        loads[name].wait()
    loads["w"].wait()
    phase("proj")

    def project(n, carry):
        cols = pl.ds(pl.multiple_of(n * 512, 512), 512)
        mixed[:, cols] = jnp.dot(att[...], w[:, cols], preferred_element_type=F32).astype(BF16)
        return carry

    lax.fori_loop(0, 4, project, 0, unroll=True)
    phase("norm")

    def norm(n, carry):
        at_rows = pl.ds(pl.multiple_of(n * 32, 32), 32)
        m = mixed[at_rows, :].astype(F32)
        m = m * lax.rsqrt(jnp.mean(m * m, axis=-1, keepdims=True) + EPSILON) * postg_ref[...]
        stream = (res[at_rows, :].astype(F32) + m).astype(BF16)
        res[at_rows, :] = stream
        s = stream.astype(F32)
        s = s * lax.rsqrt(jnp.mean(s * s, axis=-1, keepdims=True) + EPSILON) * preg_ref[...]
        normed[at_rows, :] = s.astype(BF16)
        return carry

    lax.fori_loop(0, 4, norm, 0, unroll=2)

    def begin_of(tag, i):
        return sum(SPANS[tag][:i])

    def span_of(tag, i):
        return pl.ds(begin_of(tag, i), SPANS[tag][i])

    def like(count, columns):
        return tally.at[pl.ds(0, count), pl.ds(0, columns)]

    def z_out(tag, i, src, dst):
        cols = span_of(tag, i)
        for r in (2, 1, 3):
            ex.start((tag, "z"), (tag, "z", i), src.at[r, :, cols], dst.at[4 - r, :, cols], to_z[r])

    def z_in(tag, i):
        ex.arrived((tag, "z", i), like(96, SPANS[tag][i]))

    def swap(tag, i, src, mid, dst):
        step = SPANS[tag][i] // 2
        a, b = pl.ds(begin_of(tag, i), step), pl.ds(begin_of(tag, i) + step, step)

        def x_out(w, r, ref, to_ref, cols):
            ex.start(
                tag, (tag, "x", r, i) if w == "a" else (tag, i),
                ref.at[r, :, :, :, cols], to_ref.at[4 - r, :, :, :, cols], to_x[r],
            )

        def x_in(r):
            ex.arrived((tag, "x", 4 - r, i), like(128, step))

        sides = [(2, 0), (2, 1), (1, 0), (3, 0), (1, 1), (3, 1), (0, 1)]

        def y_out(w, r, ref, to_ref, cols):
            for ry, rc in sides:
                ex.start(
                    tag, (tag, "y", r, i) if w == "b" and r else (tag, i),
                    ref.at[r, ry, rc, :, cols], to_ref.at[r, (4 - ry) % 4, rc, :, cols],
                    to_y[ry, rc],
                )
            to_ref[r, 0, 0, :, cols] = ref[r, 0, 0, :, cols]

        def y_in(r):
            ex.arrived((tag, "y", r, i), like(112, step))

        for r in (2, 1, 3):
            x_out("a", r, src, mid, a)
        yield
        for r in (2, 3, 1):
            y_out("b", r, src, mid, b)
        y_out("a", 0, src, dst, a)
        y_out("b", 0, src, dst, b)
        yield
        y_in(2)
        x_out("b", 2, mid, dst, b)
        y_in(3)
        x_out("b", 3, mid, dst, b)
        x_in(2)
        y_out("a", 2, mid, dst, a)
        y_in(1)
        x_out("b", 1, mid, dst, b)
        x_in(3)
        y_out("a", 3, mid, dst, a)
        x_in(1)
        y_out("a", 1, mid, dst, a)
        yield
        ex.arrived((tag, i), like(5 * 112 + 3 * 128, step))

    def settle_swaps(tag):
        ex.settle((tag, "z"), like(96, width))
        ex.settle(tag, like(4 * 112 + 3 * 128, width))

    def run(steps, count):
        for _ in range(count):
            next(steps, None)

    phase("pack")
    for i in range(ROUNDS):
        cols = span_of("d", i)
        packed = jnp.dot(pack, normed[:, cols], preferred_element_type=F32).astype(BF16)
        zs[:, :, cols] = packed.reshape(4, 32, SPANS["d"][i])
        rows[0, :, cols] = packed[0:32]
        z_out("d", i, zs, rows)

    def slots(i):
        cols = span_of("d", i)
        z_in("d", i)
        phase("slots%d" % i)
        spaced = jnp.dot(
            spread[...], rows[:, :, cols].reshape(128, SPANS["d"][i]), preferred_element_type=F32
        )
        xs[:, :, :, :, cols] = spaced.astype(BF16).reshape(4, 4, 2, 16, SPANS["d"][i])

    def lift(i, at_r, count):
        cols, at_rows = span_of("d", i), pl.ds(at_r * 128, count * 128)
        arrived = yr[at_r : at_r + count, :, :, :, cols].reshape(count * 128, SPANS["d"][i])
        for sums, weight in ((gates, gate), (lifts, up)):
            product = jnp.dot(arrived, weight[cols, :], preferred_element_type=F32)
            sums[at_rows, :] = product if i == 0 else sums[at_rows, :] + product

    def lower(i, half):
        step = SPANS["r"][i] // 2
        cols = pl.ds(begin_of("r", i) + half * step, step)
        produced = jnp.dot(hidden[...], down[:, cols], preferred_element_type=F32)
        made[:, :, :, :, cols] = produced.astype(BF16).reshape(4, 4, 2, 16, step)

    def combine(i):
        cols = span_of("r", i)
        returned = ret[:, :, :, :, cols].reshape(512, SPANS["r"][i])
        one = jnp.dot(pick1[...], returned, preferred_element_type=F32)
        two = jnp.dot(pick2[...], returned, preferred_element_type=F32)
        summed = (weight1 * one + weight2 * two).astype(BF16)
        comb[:, :, cols] = summed.reshape(4, 32, SPANS["r"][i])
        zret[0, :, cols] = summed[0:32]
        z_out("r", i, comb, zret)

    there = [swap("d", i, xs, xr, yr) for i in range(ROUNDS)]
    def begin(i):
        phase("zin%d" % i)
        slots(i)
        phase("d_start%d" % i)
        run(there[i], 2)

    def middle(i):
        phase("d_mid%d" % i)
        run(there[i], 1)

    def done(i):
        phase("d_in%d" % i)
        run(there[i], 1)
        phase("lift%d" % i)
        lift(i, 0, 4)

    begin(0)
    ex.settle("kv", tally)
    ex.settle("meta", meta.at[pl.ds(0, 3)])
    begin(1)
    middle(0)
    begin(2)
    middle(1)
    loads["gate"].wait()
    loads["up"].wait()
    done(0)
    begin(3)
    middle(2)
    done(1)
    middle(3)
    done(2)
    phase("d_in3")
    run(there[3], 1)
    phase("lift3")
    for half in range(2):
        lift(3, 2 * half, 2)
        at_rows = pl.ds(256 * half, 256)
        g = gates[at_rows, :]
        hidden[at_rows, :] = (g / (1.0 + jnp.exp(-g)) * lifts[at_rows, :]).astype(BF16)
    loads["down"].wait()

    home_way = [swap("r", i, made, back, ret) for i in range(ROUNDS)]
    def begin(i):
        for half in range(2):
            phase("lower%d" % i)
            lower(i, half)
            phase("r_start%d" % i)
            run(home_way[i], 1)

    def middle(i):
        phase("r_mid%d" % i)
        run(home_way[i], 1)

    def end(i):
        phase("r_in%d" % i)
        run(home_way[i], 1)
        phase("combine%d" % i)
        combine(i)

    begin(0)
    begin(1)
    middle(0)
    begin(2)
    middle(1)
    settle_swaps("d")
    end(0)
    begin(3)
    middle(2)
    middle(3)
    end(1)
    end(2)
    end(3)

    def arrive(i):
        cols = span_of("r", i)
        z_in("r", i)
        added = jnp.dot(
            home[...], zret[:, :, cols].reshape(128, SPANS["r"][i]), preferred_element_type=F32
        )
        out_ref[:, cols] = (res[:, cols].astype(F32) + added).astype(BF16)

    for i in range(ROUNDS):
        phase("out%d" % i)
        arrive(i)
    phase("sent")
    settle_swaps("r")
    phase()


def layer(
    q, k, v, w, res, gate, up, down, query_gain, key_gain, post_gain, pre_gain, ids, gw, fs
):
    hbm = pl.BlockSpec(memory_space=pltpu.HBM)
    vmem = pl.BlockSpec(memory_space=pltpu.VMEM)
    tokens, width = q.shape
    _, _, ff = gate.shape
    slots = pltpu.VMEM((4, 4, 2, 16, width), BF16)
    z_block = pltpu.VMEM((4, 32, width), BF16)
    rows = pltpu.VMEM((tokens, width), BF16)
    return pl.pallas_call(
        layer_kernel,
        out_shape=pltpu.VMEM((tokens, width), BF16),
        in_specs=[hbm] * 16,
        out_specs=vmem,
        scratch_shapes=[
            pltpu.VMEM((2, 32 + GRID_W, HEAD_DIM), F32),
            pltpu.VMEM((1, HEAD_DIM), F32),
            pltpu.VMEM((1, HEAD_DIM), F32),
            pltpu.VMEM((1, width), F32),
            pltpu.VMEM((1, width), F32),
            pltpu.VMEM((2, tokens), jnp.int32),
            pltpu.VMEM((1, tokens), F32),
            pltpu.VMEM((1, tokens), F32),
            pltpu.VMEM((2, 4, 4, 128, 512), BF16),
            pltpu.VMEM((4, 128, 512), BF16),
            rows,
            pltpu.VMEM((tokens, 512), BF16),
            pltpu.VMEM((tokens, 512), BF16),
            pltpu.VMEM((width, width), BF16),
            rows,
            pltpu.VMEM((4, 1, 512), F32),
            pltpu.VMEM((4, 1, 512), F32),
            pltpu.VMEM((4, 128, 512), F32),
            rows,
            rows,
            rows,
            pltpu.VMEM((width, ff), BF16),
            pltpu.VMEM((width, ff), BF16),
            pltpu.VMEM((ff, width), BF16),
            pltpu.VMEM((4, 8, 128), F32),
            z_block, z_block, slots, slots, slots,
            pltpu.VMEM((512, ff), F32),
            pltpu.VMEM((512, ff), F32),
            pltpu.VMEM((512, ff), BF16),
            slots, slots, slots, z_block, z_block,
            pltpu.VMEM((512, 128), BF16),
            pltpu.VMEM((128, 512), BF16),
            pltpu.VMEM((128, 512), BF16),
            pltpu.VMEM((128, 128), BF16),
            pltpu.VMEM((960, width), BF16),
            pltpu.SemaphoreType.DMA((16,)),
            pltpu.SemaphoreType.DMA((SENT,)),
            pltpu.SemaphoreType.DMA((GOT,)),
        ],
        compiler_params=pltpu.CompilerParams(
            collective_id=0, has_side_effects=True, vmem_limit_bytes=60 * 1024 * 1024
        ),
        name="layer",
    )(
        q, k, v, w, res, gate, up, down, jnp.asarray(angle_tables()), query_gain.reshape(1, -1),
        key_gain.reshape(1, -1), post_gain.reshape(1, -1), pre_gain.reshape(1, -1), ids, gw, fs,
    )


def local(
    residual_in,
    query_proj,
    key_proj,
    value_proj,
    query_gain,
    key_gain,
    out_weight,
    post_gain,
    pre_gain,
    route_ids,
    group_weight,
    first_share,
    gate_weight,
    up_weight,
    down_weight,
):
    out = layer(
        query_proj[0], key_proj[0], value_proj[0], out_weight, residual_in[0],
        gate_weight, up_weight, down_weight, query_gain, key_gain, post_gain, pre_gain,
        route_ids[0].T, group_weight, first_share,
    )
    return out[None]


def solution(mesh):
    placed = (
        P("dp", "sp", None),
        P("dp", "sp", None),
        P("dp", "sp", None),
        P("dp", "sp", None),
        P(),
        P(),
        P(),
        P(),
        P(),
        P("dp", "sp", None),
        P("dp", "sp"),
        P("dp", "sp"),
        P(("sp", "dp"), None, None),
        P(("sp", "dp"), None, None),
        P(("sp", "dp"), None, None),
    )
    return jax.shard_map(
        local, mesh=mesh, in_specs=placed, out_specs=P("dp", "sp", None), check_vma=False
    )
```

```python
import jax
import jax.numpy as jnp
import numpy as np
from jax import lax
from jax.experimental import pallas as pl
from jax.experimental.pallas import tpu as pltpu
from jax.sharding import PartitionSpec as P

HEADS = 16
KV_HEADS = 4
HEAD_DIM = 128
GRID_W = 64
RING = 4
EPSILON = 1e-06
MESH = pl.DeviceIdType.MESH


class Phase:
    def __init__(self):
        self.scope = None

    def __call__(self, name=None):
        if self.scope is not None:
            self.scope.__exit__(None, None, None)
        self.scope = None
        if name is not None:
            self.scope = jax.named_scope(name)
            self.scope.__enter__()


F32 = jnp.float32
BF16 = jnp.bfloat16


def angle_tables():
    quarter = HEAD_DIM // 4
    inverse = (np.float32(10000.0) ** (-np.arange(quarter, dtype=np.float32) / quarter)).astype(
        np.float32
    )
    places = np.concatenate([np.arange(32), np.arange(GRID_W)]).astype(np.float32)
    angles = places[:, None] * np.tile(inverse, 4)[None, :]
    return np.stack([np.cos(angles), np.sin(angles)]).astype(np.float32)


def position():
    s = lax.axis_index("sp")
    d = lax.axis_index("dp")
    return s // RING, s % RING, d // 2, d % 2


def at(z, x, y, c):
    return (
        ((z + 2 * RING) % RING) * RING + (x + 2 * RING) % RING,
        ((y + 2 * RING) % RING) * 2 + c,
    )


def turn(heads, gain, cos, sin):
    normed = (
        heads * lax.rsqrt(jnp.mean(heads * heads, axis=-1, keepdims=True) + EPSILON) * gain
    )
    lane = lax.broadcasted_iota(jnp.int32, normed.shape, 1)
    turned = jnp.where(
        (lane // 32) % 2 == 0, -pltpu.roll(normed, 96, 1), pltpu.roll(normed, 32, 1)
    )
    return (normed * cos + turned * sin).astype(BF16)


class Exchange:
    def __init__(self, send_sem, recv_sem):
        self.send_sem, self.recv_sem = send_sem, recv_sem
        self.sent_at, self.got_at = {}, {}

    def start(self, sent, got, src, dst, peer):
        pltpu.make_async_remote_copy(
            src_ref=src,
            dst_ref=dst,
            send_sem=self.send_sem.at[self.sent_at.setdefault(sent, len(self.sent_at))],
            recv_sem=self.recv_sem.at[self.got_at.setdefault(got, len(self.got_at))],
            device_id=peer,
            device_id_type=MESH,
        ).start()

    def arrived(self, got, like):
        pltpu.make_async_copy(like, like, self.recv_sem.at[self.got_at[got]]).wait()

    def settle(self, sent, like):
        pltpu.make_async_copy(like, like, self.send_sem.at[self.sent_at[sent]]).wait()


SPANS = {"d": (256, 768, 768, 256), "r": (512, 768, 512, 256)}
ROUNDS = 4
SENT = 6
GOT = 11 + 2 * 8 * ROUNDS


def iota(shape, dim):
    return lax.broadcasted_iota(jnp.int32, shape, dim)


def layer_kernel(
    q_hbm, k_hbm, v_hbm, w_hbm, res_hbm, gate_hbm, up_hbm, down_hbm,
    table_hbm, qg_hbm, kg_hbm, postg_hbm, preg_hbm, ids_hbm, gw_hbm, fs_hbm,
    out_ref,
    table_ref, qg_ref, kg_ref, postg_ref, preg_ref, ids_ref, gw_ref, fs_ref,
    kv, qt, q_raw, k_raw, v_raw, w, res, top, total, acc, att, mixed, normed,
    gate, up, down, meta,
    zs, rows, xs, xr, yr, gates, lifts, hidden, made, back, ret, comb, zret,
    spread, pick1, pick2, home, tally,
    local_sem, send_sem, recv_sem,
):
    z, x, y, c = position()
    width = q_raw.shape[1]
    phase = Phase()
    phase("turn")
    to_z = {s: at(z + s, x, y, c) for s in (1, 2, 3)}
    to_x = {s: at(z, x + s, y, c) for s in (1, 2, 3)}
    to_y = {(s, o): at(z, x, y + s, c if o == 0 else 1 - c) for s in range(4) for o in (0, 1)}
    del to_y[0, 0]
    ring = {"z": (to_z[1], to_z[3]), "x": (to_x[1], to_x[3])}
    loads = {}

    def load(*items):
        for name, src, dst in items:
            loads[name] = pltpu.make_async_copy(src, dst, local_sem.at[len(loads)])
            loads[name].start()

    load(
        ("v", v_hbm, v_raw), ("k", k_hbm, k_raw), ("table", table_hbm, table_ref),
        ("kg", kg_hbm, kg_ref),
    )
    barrier = pltpu.get_barrier_semaphore()
    peers = [*to_z.values(), *to_x.values(), *to_y.values()]
    for peer in peers:
        pl.semaphore_signal(barrier, inc=1, device_id=peer, device_id_type=MESH)
    load(
        ("ids", ids_hbm, ids_ref), ("gw", gw_hbm, gw_ref),
        ("fs", fs_hbm, fs_ref), ("qg", qg_hbm, qg_ref), ("q", q_hbm, q_raw),
        ("postg", postg_hbm, postg_ref), ("preg", preg_hbm, preg_ref), ("res", res_hbm, res),
        ("w", w_hbm, w), ("gate", gate_hbm.at[0], gate), ("up", up_hbm.at[0], up),
        ("down", down_hbm.at[0], down),
    )
    ex = Exchange(send_sem, recv_sem)

    loads["v"].wait()
    for half in range(2):
        kv[half, 0, 0, :, 256:512] = v_raw[:, half * 256 : (half + 1) * 256]
    phase("barrier")
    pl.semaphore_wait(barrier, len(peers))

    phase("start")
    first = ("x", "z")
    second = ("z", "x")
    low, high = pl.ds(0, 64), pl.ds(64, 64)

    def both(p, kind, r=0, lanes=slice(None)):
        if kind == "own":
            peer = ring[first[p]]
            pairs = (kv.at[p, 0, 0], kv.at[p, 0, 3]), (kv.at[p, 0, 0], kv.at[p, 0, 1])
        elif kind == "relay":
            peer = ring[first[p]]
            pairs = (
                (kv.at[p, 0, 3, low], kv.at[p, 0, 2, low]),
                (kv.at[p, 0, 1, high], kv.at[p, 0, 2, high]),
            )
        elif kind == "far":
            peer = ring[second[p]]
            pairs = (kv.at[p, 0, r], kv.at[p, 3, r]), (kv.at[p, 0, r], kv.at[p, 1, r])
        else:
            peer = ring[second[p]]
            pairs = (
                (kv.at[p, 3, r, low], kv.at[p, 2, r, low]),
                (kv.at[p, 1, r, high], kv.at[p, 2, r, high]),
            )
        for (src, dst), to in zip(pairs, peer):
            ex.start("kv", (kind, r), src.at[:, lanes], dst.at[:, lanes], to)

    def got(kind, r=0):
        ex.arrived((kind, r), kv.at[0, 0, pl.ds(0, 4 if kind in ("own", "far") else 2)])

    for p in range(2):
        both(p, "own", 0, pl.ds(256, 256))
    phase("kturn")
    lane = iota((GRID_W, HEAD_DIM), 1)

    def table(which):
        halves = []
        for part in range(2):
            row = table_ref[which, pl.ds(2 * (z * RING + x) + part, 1), :]
            halves.append(jnp.where(lane < 64, row, table_ref[which, 32 : 32 + GRID_W, :]))
        return jnp.concatenate(halves, axis=0)

    loads["table"].wait()
    cos, sin = table(0), table(1)
    for name in ("ids", "gw", "fs"):
        loads[name].wait()
    meta[0, 0:2, :] = ids_ref[...].astype(F32)
    meta[0, 2:3, :] = gw_ref[...]
    meta[0, 3:4, :] = fs_ref[...]
    meta[0, 4:8, :] = jnp.zeros((4, 128), F32)
    loads["k"].wait()
    loads["kg"].wait()
    for h in range(KV_HEADS):
        raw = k_raw[:, h * 128 : (h + 1) * 128].astype(F32)
        kv[h // 2, 0, 0, :, (h % 2) * 128 : (h % 2 + 1) * 128] = turn(raw, kg_ref[...], cos, sin)
    for p in range(2):
        both(p, "own", 0, pl.ds(0, 256))
    for p in range(2):
        both(p, "far", 0)
    for r in (1, 2, 3):
        ex.start("meta", "meta", meta.at[0], meta.at[4 - r], to_z[r])

    phase("qturn")
    loads["q"].wait()
    loads["qg"].wait()
    for h in range(HEADS):
        raw = q_raw[:, h * 128 : (h + 1) * 128].astype(F32)
        qt[h // 4, :, (h % 4) * 128 : (h % 4 + 1) * 128] = turn(raw, qg_ref[...], cos, sin).T

    phase("own")
    got("own")
    for p in range(2):
        both(p, "relay")
    for r in (3, 1):
        for p in range(2):
            both(p, "far", r)

    phase("tables")
    eye = iota((128, 128), 0) == iota((128, 128), 1)
    earlier = (iota((128, 128), 0) < iota((128, 128), 1)).astype(F32)

    def lay(column):
        return jnp.sum(jnp.where(eye, column, 0.0), axis=0, keepdims=True)

    def stand(row):
        return jnp.sum(jnp.where(eye, row, 0.0), axis=1, keepdims=True)

    def counted(members):
        return jnp.dot(members, earlier, preferred_element_type=F32)

    relative = ((meta[0, 0:1, :].astype(jnp.int32) >> 5) - z + 4) & 3
    members = (iota((8, 128), 0) == relative).astype(F32)
    rank = jnp.sum(members * counted(members), axis=0, keepdims=True)
    target = relative.astype(F32) * 32.0 + rank
    pack = (iota((128, 128), 0).astype(F32) == target).astype(BF16)
    home[...] = (iota((128, 128), 1).astype(F32) == stand(target)).astype(BF16)

    phase("relay")
    got("relay")
    for p in range(2):
        both(p, "far", 2)
    got("far", 0)
    for p in range(2):
        both(p, "last", 0)

    phase("tables2")
    ex.arrived("meta", meta.at[pl.ds(0, 3)])
    stacks = [[], [], [], []]
    for r in range(4):
        inside = (meta[r, 0:1, :].astype(jnp.int32) >> 5) == z
        members = jnp.broadcast_to(inside.astype(F32), (8, 128))
        places = jnp.where(inside, counted(members)[0:1], -1.0)
        taken = iota((32, 128), 0).astype(F32) == places
        for which in range(4):
            stacks[which].append(
                jnp.sum(
                    jnp.where(taken, meta[r, which : which + 1, :], 0.0), axis=1, keepdims=True
                )
            )
    expert1, expert2, group_share, first_share = [jnp.concatenate(s, axis=0) for s in stacks]

    def relative_expert(column):
        e = lay(column).astype(jnp.int32) & 31
        return (
            ((((e >> 3) - x + 4) & 3) << 3)
            + (((((e >> 1) & 3) - y + 4) & 3) << 1)
            + ((e & 1) ^ c)
        )

    rel1, rel2 = relative_expert(expert1), relative_expert(expert2)
    named1 = (iota((32, 128), 0) == rel1).astype(F32)
    named2 = (iota((32, 128), 0) == rel2).astype(F32)
    ahead = counted(named1 + named2)
    slot1 = rel1.astype(F32) * 16.0 + jnp.sum(named1 * ahead, axis=0, keepdims=True)
    slot2 = rel2.astype(F32) * 16.0 + jnp.sum(named2 * ahead, axis=0, keepdims=True)
    places = iota((512, 128), 0).astype(F32)
    spread[...] = ((places == slot1) | (places == slot2)).astype(BF16)
    places = iota((128, 512), 1).astype(F32)
    pick1[...] = (places == stand(slot1)).astype(BF16)
    pick2[...] = (places == stand(slot2)).astype(BF16)
    weight1 = group_share * first_share
    weight2 = group_share * (1.0 - first_share)

    scale = float(np.log2(np.e) / np.sqrt(HEAD_DIM))

    def attend(blocks, opening=False):
        def one(g, carry):
            p, h = g // 2, g % 2

            def part(offset):
                cols = pl.ds(pl.multiple_of(offset + h * 128, 128), 128)
                return jnp.concatenate([kv[p, a, b, :, cols] for a, b in blocks], axis=0)

            keys, values = part(0), part(256)
            scores = jnp.dot(keys, qt[g], preferred_element_type=F32)
            peak = jnp.max(scores, axis=0, keepdims=True)
            if not opening:
                before = top[g]
                peak = jnp.maximum(peak, before)
            weights = jnp.exp2((scores - peak) * scale)
            summed = jnp.sum(weights, axis=0, keepdims=True)
            out = lax.dot_general(
                values, weights.astype(BF16), (((0,), (0,)), ((), ())),
                preferred_element_type=F32,
            )
            if not opening:
                shrink = jnp.exp2((before - peak) * scale)
                summed += total[g] * shrink
                out += acc[g] * shrink
            top[g] = peak
            total[g] = summed
            acc[g] = out
            return carry

        lax.fori_loop(0, KV_HEADS, one, 0, unroll=len(blocks) < 4 or 2)

    phase("att0")
    attend([(0, 0), (0, 1), (0, 2), (0, 3)], opening=True)

    def step_on(r, kind):
        got(kind, r)
        if kind == "far":
            for p in range(2):
                both(p, "last", r)

    phase("far3")
    step_on(3, "far")
    phase("att1")
    attend([(3, 0), (3, 3), (1, 0), (1, 3)])
    phase("far1")
    step_on(1, "far")
    phase("far2")
    step_on(2, "far")
    phase("att2")
    attend([(3, 1), (1, 1), (3, 2), (1, 2)])
    phase("last03")
    step_on(0, "last")
    step_on(3, "last")
    phase("att3")
    attend([(2, 0), (2, 3)])
    phase("last12")
    step_on(1, "last")
    phase("att4")
    attend([(2, 1)])
    phase("last2")
    step_on(2, "last")
    phase("att5")
    attend([(2, 2)])

    phase("div")
    for g in range(KV_HEADS):
        scaled = acc[g] / total[g]
        for h in range(4):
            head = g * 4 + h
            att[:, head * 128 : (head + 1) * 128] = (
                scaled[:, h * 128 : (h + 1) * 128].T.astype(BF16)
            )
    for name in ("postg", "preg", "res"):
        loads[name].wait()
    loads["w"].wait()
    phase("proj")

    def project(n, carry):
        cols = pl.ds(pl.multiple_of(n * 512, 512), 512)
        mixed[:, cols] = jnp.dot(att[...], w[:, cols], preferred_element_type=F32).astype(BF16)
        return carry

    lax.fori_loop(0, 4, project, 0, unroll=True)
    phase("norm")

    def norm(n, carry):
        at_rows = pl.ds(pl.multiple_of(n * 32, 32), 32)
        m = mixed[at_rows, :].astype(F32)
        m = m * lax.rsqrt(jnp.mean(m * m, axis=-1, keepdims=True) + EPSILON) * postg_ref[...]
        stream = (res[at_rows, :].astype(F32) + m).astype(BF16)
        res[at_rows, :] = stream
        s = stream.astype(F32)
        s = s * lax.rsqrt(jnp.mean(s * s, axis=-1, keepdims=True) + EPSILON) * preg_ref[...]
        normed[at_rows, :] = s.astype(BF16)
        return carry

    lax.fori_loop(0, 4, norm, 0, unroll=2)

    def begin_of(tag, i):
        return sum(SPANS[tag][:i])

    def span_of(tag, i):
        return pl.ds(begin_of(tag, i), SPANS[tag][i])

    def like(count, columns):
        return tally.at[pl.ds(0, count), pl.ds(0, columns)]

    def z_out(tag, i, src, dst):
        cols = span_of(tag, i)
        for r in (2, 1, 3):
            ex.start((tag, "z"), (tag, "z", i), src.at[r, :, cols], dst.at[4 - r, :, cols], to_z[r])

    def z_in(tag, i):
        ex.arrived((tag, "z", i), like(96, SPANS[tag][i]))

    def swap(tag, i, src, mid, dst):
        step = SPANS[tag][i] // 2
        a, b = pl.ds(begin_of(tag, i), step), pl.ds(begin_of(tag, i) + step, step)

        def x_out(w, r, ref, to_ref, cols):
            ex.start(
                tag, (tag, "x", r, i) if w == "a" else (tag, i),
                ref.at[r, :, :, :, cols], to_ref.at[4 - r, :, :, :, cols], to_x[r],
            )

        def x_in(r):
            ex.arrived((tag, "x", 4 - r, i), like(128, step))

        sides = [(2, 0), (2, 1), (1, 0), (3, 0), (1, 1), (3, 1), (0, 1)]

        def y_out(w, r, ref, to_ref, cols):
            for ry, rc in sides:
                ex.start(
                    tag, (tag, "y", r, i) if w == "b" and r else (tag, i),
                    ref.at[r, ry, rc, :, cols], to_ref.at[r, (4 - ry) % 4, rc, :, cols],
                    to_y[ry, rc],
                )
            to_ref[r, 0, 0, :, cols] = ref[r, 0, 0, :, cols]

        def y_in(r):
            ex.arrived((tag, "y", r, i), like(112, step))

        for r in (2, 1, 3):
            x_out("a", r, src, mid, a)
        yield
        for r in (2, 3, 1):
            y_out("b", r, src, mid, b)
        y_out("a", 0, src, dst, a)
        y_out("b", 0, src, dst, b)
        yield
        y_in(2)
        x_out("b", 2, mid, dst, b)
        y_in(3)
        x_out("b", 3, mid, dst, b)
        x_in(2)
        y_out("a", 2, mid, dst, a)
        y_in(1)
        x_out("b", 1, mid, dst, b)
        x_in(3)
        y_out("a", 3, mid, dst, a)
        x_in(1)
        y_out("a", 1, mid, dst, a)
        yield
        ex.arrived((tag, i), like(5 * 112 + 3 * 128, step))

    def settle_swaps(tag):
        ex.settle((tag, "z"), like(96, width))
        ex.settle(tag, like(4 * 112 + 3 * 128, width))

    def run(steps, count):
        for _ in range(count):
            next(steps, None)

    phase("pack")
    for i in range(ROUNDS):
        cols = span_of("d", i)
        packed = jnp.dot(pack, normed[:, cols], preferred_element_type=F32).astype(BF16)
        zs[:, :, cols] = packed.reshape(4, 32, SPANS["d"][i])
        rows[0, :, cols] = packed[0:32]
        z_out("d", i, zs, rows)

    def slots(i):
        cols = span_of("d", i)
        z_in("d", i)
        phase("slots%d" % i)
        spaced = jnp.dot(
            spread[...], rows[:, :, cols].reshape(128, SPANS["d"][i]), preferred_element_type=F32
        )
        xs[:, :, :, :, cols] = spaced.astype(BF16).reshape(4, 4, 2, 16, SPANS["d"][i])

    def lift(i, at_r, count):
        cols, at_rows = span_of("d", i), pl.ds(at_r * 128, count * 128)
        arrived = yr[at_r : at_r + count, :, :, :, cols].reshape(count * 128, SPANS["d"][i])
        for sums, weight in ((gates, gate), (lifts, up)):
            product = jnp.dot(arrived, weight[cols, :], preferred_element_type=F32)
            sums[at_rows, :] = product if i == 0 else sums[at_rows, :] + product

    def lower(i, half):
        step = SPANS["r"][i] // 2
        cols = pl.ds(begin_of("r", i) + half * step, step)
        produced = jnp.dot(hidden[...], down[:, cols], preferred_element_type=F32)
        made[:, :, :, :, cols] = produced.astype(BF16).reshape(4, 4, 2, 16, step)

    def combine(i):
        cols = span_of("r", i)
        returned = ret[:, :, :, :, cols].reshape(512, SPANS["r"][i])
        one = jnp.dot(pick1[...], returned, preferred_element_type=F32)
        two = jnp.dot(pick2[...], returned, preferred_element_type=F32)
        summed = (weight1 * one + weight2 * two).astype(BF16)
        comb[:, :, cols] = summed.reshape(4, 32, SPANS["r"][i])
        zret[0, :, cols] = summed[0:32]
        z_out("r", i, comb, zret)

    there = [swap("d", i, xs, xr, yr) for i in range(ROUNDS)]
    def begin(i):
        phase("zin%d" % i)
        slots(i)
        phase("d_start%d" % i)
        run(there[i], 2)

    def middle(i):
        phase("d_mid%d" % i)
        run(there[i], 1)

    def done(i):
        phase("d_in%d" % i)
        run(there[i], 1)
        phase("lift%d" % i)
        lift(i, 0, 4)

    begin(0)
    ex.settle("kv", tally)
    ex.settle("meta", meta.at[pl.ds(0, 3)])
    begin(1)
    middle(0)
    begin(2)
    middle(1)
    loads["gate"].wait()
    loads["up"].wait()
    done(0)
    begin(3)
    middle(2)
    done(1)
    middle(3)
    done(2)
    phase("d_in3")
    run(there[3], 1)
    phase("lift3")
    for half in range(2):
        lift(3, 2 * half, 2)
        at_rows = pl.ds(256 * half, 256)
        g = gates[at_rows, :]
        hidden[at_rows, :] = (g / (1.0 + jnp.exp(-g)) * lifts[at_rows, :]).astype(BF16)
    loads["down"].wait()

    home_way = [swap("r", i, made, back, ret) for i in range(ROUNDS)]
    def begin(i):
        for half in range(2):
            phase("lower%d" % i)
            lower(i, half)
            phase("r_start%d" % i)
            run(home_way[i], 1)

    def middle(i):
        phase("r_mid%d" % i)
        run(home_way[i], 1)

    def end(i):
        phase("r_in%d" % i)
        run(home_way[i], 1)
        phase("combine%d" % i)
        combine(i)

    begin(0)
    begin(1)
    middle(0)
    begin(2)
    middle(1)
    settle_swaps("d")
    end(0)
    begin(3)
    middle(2)
    middle(3)
    end(1)
    end(2)
    end(3)

    def arrive(i):
        cols = span_of("r", i)
        z_in("r", i)
        added = jnp.dot(
            home[...], zret[:, :, cols].reshape(128, SPANS["r"][i]), preferred_element_type=F32
        )
        out_ref[:, cols] = (res[:, cols].astype(F32) + added).astype(BF16)

    for i in range(ROUNDS):
        phase("out%d" % i)
        arrive(i)
    phase("sent")
    settle_swaps("r")
    phase()


def layer(
    q, k, v, w, res, gate, up, down, query_gain, key_gain, post_gain, pre_gain, ids, gw, fs
):
    hbm = pl.BlockSpec(memory_space=pltpu.HBM)
    vmem = pl.BlockSpec(memory_space=pltpu.VMEM)
    tokens, width = q.shape
    _, _, ff = gate.shape
    slots = pltpu.VMEM((4, 4, 2, 16, width), BF16)
    z_block = pltpu.VMEM((4, 32, width), BF16)
    rows = pltpu.VMEM((tokens, width), BF16)
    return pl.pallas_call(
        layer_kernel,
        out_shape=pltpu.VMEM((tokens, width), BF16),
        in_specs=[hbm] * 16,
        out_specs=vmem,
        scratch_shapes=[
            pltpu.VMEM((2, 32 + GRID_W, HEAD_DIM), F32),
            pltpu.VMEM((1, HEAD_DIM), F32),
            pltpu.VMEM((1, HEAD_DIM), F32),
            pltpu.VMEM((1, width), F32),
            pltpu.VMEM((1, width), F32),
            pltpu.VMEM((2, tokens), jnp.int32),
            pltpu.VMEM((1, tokens), F32),
            pltpu.VMEM((1, tokens), F32),
            pltpu.VMEM((2, 4, 4, 128, 512), BF16),
            pltpu.VMEM((4, 128, 512), BF16),
            rows,
            pltpu.VMEM((tokens, 512), BF16),
            pltpu.VMEM((tokens, 512), BF16),
            pltpu.VMEM((width, width), BF16),
            rows,
            pltpu.VMEM((4, 1, 512), F32),
            pltpu.VMEM((4, 1, 512), F32),
            pltpu.VMEM((4, 128, 512), F32),
            rows,
            rows,
            rows,
            pltpu.VMEM((width, ff), BF16),
            pltpu.VMEM((width, ff), BF16),
            pltpu.VMEM((ff, width), BF16),
            pltpu.VMEM((4, 8, 128), F32),
            z_block, z_block, slots, slots, slots,
            pltpu.VMEM((512, ff), F32),
            pltpu.VMEM((512, ff), F32),
            pltpu.VMEM((512, ff), BF16),
            slots, slots, slots, z_block, z_block,
            pltpu.VMEM((512, 128), BF16),
            pltpu.VMEM((128, 512), BF16),
            pltpu.VMEM((128, 512), BF16),
            pltpu.VMEM((128, 128), BF16),
            pltpu.VMEM((960, width), BF16),
            pltpu.SemaphoreType.DMA((16,)),
            pltpu.SemaphoreType.DMA((SENT,)),
            pltpu.SemaphoreType.DMA((GOT,)),
        ],
        compiler_params=pltpu.CompilerParams(
            collective_id=0, has_side_effects=True, vmem_limit_bytes=60 * 1024 * 1024
        ),
        name="layer",
    )(
        q, k, v, w, res, gate, up, down, jnp.asarray(angle_tables()), query_gain.reshape(1, -1),
        key_gain.reshape(1, -1), post_gain.reshape(1, -1), pre_gain.reshape(1, -1), ids, gw, fs,
    )


def local(
    residual_in,
    query_proj,
    key_proj,
    value_proj,
    query_gain,
    key_gain,
    out_weight,
    post_gain,
    pre_gain,
    route_ids,
    group_weight,
    first_share,
    gate_weight,
    up_weight,
    down_weight,
):
    out = layer(
        query_proj[0], key_proj[0], value_proj[0], out_weight, residual_in[0],
        gate_weight, up_weight, down_weight, query_gain, key_gain, post_gain, pre_gain,
        route_ids[0].T, group_weight, first_share,
    )
    return out[None]


def solution(mesh):
    placed = (
        P("dp", "sp", None),
        P("dp", "sp", None),
        P("dp", "sp", None),
        P("dp", "sp", None),
        P(),
        P(),
        P(),
        P(),
        P(),
        P("dp", "sp", None),
        P("dp", "sp"),
        P("dp", "sp"),
        P(("sp", "dp"), None, None),
        P(("sp", "dp"), None, None),
        P(("sp", "dp"), None, None),
    )
    return jax.shard_map(
        local, mesh=mesh, in_specs=placed, out_specs=P("dp", "sp", None), check_vma=False
    )
```
